32 devices in a mesh: sp: 4 (over z), fs: 4 (over y, x), tp: 2 (over core).
Axes of the slice: x: 2, y: 2, z: 4, core: 2. Of those that a mesh axis runs over, the one named last changes fastest.
Arguments:
- tokens: bfloat16 [4, 1024, 2048], P('fs', 'sp', 'tp'), may hold values from -6 to 6
- norm_gain: float32 [2048], replicated, may hold values from 0.1 to 1.9
- ret_query: bfloat16 [2048, 1024], P('sp', 'tp'), may hold values from -0.125 to 0.125
- ret_key: bfloat16 [2048, 1024], P('sp', 'tp'), may hold values from -0.125 to 0.125
- ret_value: bfloat16 [2048, 1024], P('sp', 'tp'), may hold values from -0.125 to 0.125
- att_query: bfloat16 [2048, 1024], P('sp', 'tp'), may hold values from -0.125 to 0.125
- att_key: bfloat16 [2048, 256], P('sp', 'tp'), may hold values from -0.125 to 0.125
- att_value: bfloat16 [2048, 256], P('sp', 'tp'), may hold values from -0.125 to 0.125
- log_decay: float32 [4, 4, 1024], P('fs', 'tp', 'sp'), may hold values from -1 to 0
- start_state: float32 [4, 4, 256, 256], P('fs', 'tp'), may hold values from -12 to 12
- ret_gain: float32 [1024], P('tp'), may hold values from 0.1 to 1.9
- sink_logits: float32 [16], P('tp'), may hold values from 1 to 5
- ret_out: bfloat16 [1024, 2048], P('tp', 'fs'), may hold values from -0.1875 to 0.1875
- att_out: bfloat16 [1024, 2048], P('tp', 'fs'), may hold values from -1.5 to 1.5
Outputs:
- mixed: bfloat16 [4, 1024, 2048], P('fs', 'sp', 'tp')
The draws below stay inside these ranges and needn't reach their ends.
All inputs are finite; a program needn't handle non-finite values.
Results may differ from the reference program's by a relative error of at most 0.015.
Values may be sent and summed in bfloat16 or wider, within the bound.
A program may use at most 128 MiB of HBM per device.

```python
import jax
import jax.numpy as jnp
from jax import lax

D = 2048
RETENTION_HEADS = 4
DK = 256
DV = 256
AQH = 16
AKH = 4
HD = 64
WINDOW = 128
BLOCK = 128
TOK_DEV = 256
SEQUENCE_COUNT = 4
SEQUENCE_LENGTH = 1024
N_TP = 2


def draw_log_decay(key, part):
    random_subkeys = jax.random.split(jax.random.fold_in(key, 17), 5)
    blocks = SEQUENCE_LENGTH // TOK_DEV
    ranking = jax.vmap(lambda inner: jax.random.permutation(inner, RETENTION_HEADS))(jax.random.split(random_subkeys[0], SEQUENCE_COUNT))
    fast_heads = (ranking < RETENTION_HEADS // 2).astype(jnp.float32)
    baseline_decay = fast_heads * (3.0 / BLOCK) + (1.0 - fast_heads) * (1.0 / SEQUENCE_LENGTH)
    noise_spread = jax.random.uniform(random_subkeys[1], (SEQUENCE_COUNT, RETENTION_HEADS, blocks), jnp.float32, 0.4, 1.2)
    noise_spread = jnp.repeat(noise_spread, TOK_DEV, axis=-1)
    random_noise = jax.random.uniform(random_subkeys[2], (SEQUENCE_COUNT, RETENTION_HEADS, SEQUENCE_LENGTH), jnp.float32, 0.5, 1.5)
    spike_position = jax.random.randint(random_subkeys[3], (SEQUENCE_COUNT, RETENTION_HEADS, 2), 0, SEQUENCE_LENGTH)
    spike_magnitude = jax.random.uniform(random_subkeys[4], (SEQUENCE_COUNT, RETENTION_HEADS, 2), jnp.float32, 0.2, 0.4)
    position_list = jnp.arange(SEQUENCE_LENGTH, dtype=jnp.int32)
    spike_events = jnp.sum(jnp.where(position_list[None, None, None, :] == spike_position[..., None], jnp.log(1.0 - spike_magnitude)[..., None], 0.0), axis=2)
    return (-baseline_decay[..., None] * noise_spread * random_noise + spike_events).astype(jnp.float32)


def levels(rng, dims, cuts, smallest, high):
    level, own = 1.0, jax.random.fold_in(rng, 6)
    for axis_at, blocks in cuts:
        heights = jnp.exp(jax.random.uniform(jax.random.fold_in(own, axis_at), (blocks,), jnp.float32, smallest / len(cuts), high / len(cuts)))
        level = level * jnp.repeat(heights, dims[axis_at] // blocks).reshape([-1 if axis == axis_at else 1 for axis in range(len(dims))])
    return level


def gaussian(stream_key, dims, deviation, bound, cuts=(), kind=jnp.bfloat16):
    drawn = jax.random.normal(stream_key, dims, jnp.float32) * deviation
    if len(cuts) > 0:
        drawn = levels(stream_key, dims, cuts, -0.22, 0.18) * drawn
    return jnp.clip(drawn, min=-bound, max=bound).astype(kind)


def setup_inputs(seed: int = 0) -> dict:
    key_of = jax.random.split(jax.random.key(seed), 15)
    return {
        "tokens": gaussian(key_of[0], (SEQUENCE_COUNT, SEQUENCE_LENGTH, D), 1.0, 6.0, ((0, 4), (1, 4), (2, 2))),
        "norm_gain": jnp.clip(1.0 + 0.18 * jax.random.normal(key_of[1], (D,), jnp.float32), 0.1, 1.9),
        "ret_query": gaussian(key_of[2], (D, RETENTION_HEADS * DK), D ** -0.5, 0.125, ((0, 4), (1, 2))),
        "ret_key": gaussian(key_of[3], (D, RETENTION_HEADS * DK), D ** -0.5, 0.125, ((0, 4), (1, 2))),
        "ret_value": gaussian(key_of[4], (D, RETENTION_HEADS * DV), D ** -0.5, 0.125, ((0, 4), (1, 2))),
        "att_query": gaussian(key_of[5], (D, AQH * HD), D ** -0.5, 0.125, ((0, 4), (1, 2))),
        "att_key": gaussian(key_of[6], (D, AKH * HD), D ** -0.5, 0.125, ((0, 4), (1, 2))),
        "att_value": gaussian(key_of[7], (D, AKH * HD), D ** -0.5, 0.125, ((0, 4), (1, 2))),
        "log_decay": draw_log_decay(jax.random.fold_in(key_of[14], 71), 0),
        "start_state": gaussian(key_of[9], (SEQUENCE_COUNT, RETENTION_HEADS, DK, DV), (2 * (TOK_DEV // DK) ** 0.5), 12.0, ((0, 4), (1, 2)), jnp.float32),
        "ret_gain": jnp.clip(1.0 + 0.18 * jax.random.normal(key_of[10], (RETENTION_HEADS * DV,), jnp.float32), 0.1, 1.9),
        "sink_logits": jnp.clip(1.0 + 4.0 * jax.random.uniform(key_of[11], (AQH,), jnp.float32) ** levels(key_of[11], (AQH,), ((0, 2),), -0.2, 0.2), 1.0, 5.0),
        "ret_out": gaussian(key_of[12], (RETENTION_HEADS * DV, D), (RETENTION_HEADS * DV) ** -0.5, 0.1875, ((0, 2), (1, 4))),
        "att_out": gaussian(key_of[13], (AQH * HD, D), (AQH * HD // 64) ** -0.5, 1.5, ((0, 2), (1, 4))),
    }


epsilon = 1e-06
exact_result = lax.Precision.HIGHEST

def rotate(values, positions):
    half_dim = values.shape[-1] // 2
    inverse = 1.0 / 10000.0 ** (jnp.arange(half_dim, dtype=jnp.float32) / half_dim)
    angles = positions.astype(jnp.float32)[:, None] * inverse[None, :]
    cosine = jnp.cos(angles)[:, None, :]
    sine_table = jnp.sin(angles)[:, None, :]
    front_half = values[..., :half_dim]
    back_half = values[..., half_dim:]
    return jnp.concatenate([front_half * cosine - back_half * sine_table, front_half * sine_table + back_half * cosine], axis=-1)

def block_step(memory_state, inputs):
    queries, key_matrix_rows, value_matrix_rows, log_rates = inputs
    length_here = log_rates.shape[-1]
    causal = jnp.arange(length_here)[:, None] >= jnp.arange(length_here)[None, :]
    running_totals = jnp.cumsum(log_rates, axis=-1)
    relative = running_totals[:, :, None] - running_totals[:, None, :]
    weight = jnp.where(causal[None], jnp.exp(jnp.where(causal[None], relative, 0.0)), 0.0)
    score_matrix = jnp.einsum('hqd,hkd->hqk', queries, key_matrix_rows, precision=exact_result) * weight
    carried_state = jnp.einsum('hqd,hdv->hqv', queries * jnp.exp(running_totals)[:, :, None], memory_state, precision=exact_result)
    output_rows = jnp.einsum('arf,afu->aru', score_matrix, value_matrix_rows, precision=exact_result) + carried_state
    decay_factors = jnp.exp(running_totals[:, -1:] - running_totals)
    memory_state = memory_state * jnp.exp(running_totals[:, -1])[:, None, None] + jnp.einsum('iwj,iwe->ije', key_matrix_rows * decay_factors[:, :, None], value_matrix_rows, precision=exact_result)
    return (memory_state, output_rows)

def reference(tokens, norm_gain, ret_query, ret_key, ret_value, att_query, att_key, att_value, log_decay, start_state, ret_gain, sink_logits, ret_out, att_out):

    def one_sequence(inputs):
        rows_in, decay_rows, initial = inputs
        as_float = rows_in.astype(jnp.float32)
        normed = (as_float * lax.rsqrt(lax.optimization_barrier(jnp.mean(as_float * as_float, axis=-1, keepdims=True)) + epsilon) * norm_gain).astype(jnp.bfloat16)

        def project(weights):
            return jnp.dot(normed, weights, preferred_element_type=jnp.float32).astype(jnp.bfloat16)
        ret_queries = project(ret_query)
        ret_keys = project(ret_key)
        ret_values = project(ret_value)
        att_queries = project(att_query)
        att_keys = project(att_key)
        att_values = project(att_value)
        positions = jnp.arange(SEQUENCE_LENGTH, dtype=jnp.int32)
        queries = rotate(ret_queries.astype(jnp.float32).reshape(SEQUENCE_LENGTH, RETENTION_HEADS, DK), positions)
        keys_rot = rotate(ret_keys.astype(jnp.float32).reshape(SEQUENCE_LENGTH, RETENTION_HEADS, DK), positions) * DK ** (-0.5)
        values_f = ret_values.astype(jnp.float32).reshape(SEQUENCE_LENGTH, RETENTION_HEADS, DV)
        count = SEQUENCE_LENGTH // BLOCK

        def blocked(array):
            return array.reshape(count, BLOCK, RETENTION_HEADS, array.shape[-1]).transpose(0, 2, 1, 3)
        log_rates = decay_rows.reshape(RETENTION_HEADS, count, BLOCK).transpose(1, 0, 2)
        _, pieces = lax.scan(block_step, initial, (blocked(queries), blocked(keys_rot), blocked(values_f), log_rates))
        retained = pieces.transpose(0, 2, 1, 3).reshape(SEQUENCE_LENGTH, RETENTION_HEADS, DV)
        centred = retained - lax.optimization_barrier(jnp.mean(retained, axis=-1, keepdims=True))
        variance = lax.optimization_barrier(jnp.mean(centred * centred, axis=-1, keepdims=True))
        ret_hidden = ((centred * lax.rsqrt(variance + epsilon)).reshape(SEQUENCE_LENGTH, RETENTION_HEADS * DV) * ret_gain).astype(jnp.bfloat16)
        windows = SEQUENCE_LENGTH // WINDOW
        groups = AQH // AKH
        grouped_q = att_queries.reshape(windows, WINDOW, AKH, groups, HD).astype(jnp.float32)

        def banded(array):
            blocks_now = array.reshape(windows, WINDOW, AKH, HD)
            earlier = jnp.concatenate([jnp.zeros((1, WINDOW, AKH, HD), array.dtype), blocks_now[:-1]], axis=0)
            return jnp.concatenate([earlier, blocks_now], axis=1).astype(jnp.float32)
        key_band = banded(att_keys)
        value_band = banded(att_values)
        score_matrix = jnp.einsum('nqhgd,nkhd->nhgqk', grouped_q, key_band) * HD ** (-0.5)
        query_index = WINDOW + jnp.arange(WINDOW)
        key_index = jnp.arange(2 * WINDOW)
        allowed = (key_index[None, :] <= query_index[:, None]) & (query_index[:, None] - key_index[None, :] < WINDOW)
        present = (jnp.arange(windows)[:, None] > 0) | (key_index >= WINDOW)[None, :]
        visible = (allowed[None] & present[:, None, :])[:, None, None]
        expo = jnp.exp(jnp.where(visible, score_matrix, -1e+30))
        summed = lax.optimization_barrier(jnp.sum(expo, axis=-1, keepdims=True)) + jnp.exp(sink_logits).reshape(1, AKH, groups, 1, 1)
        probs = (expo / summed).astype(jnp.bfloat16)
        att_hidden = jnp.einsum('nhgqk,nkhd->nqhgd', probs.astype(jnp.float32), value_band).astype(jnp.bfloat16).reshape(SEQUENCE_LENGTH, AQH * HD)
        ret_cols = RETENTION_HEADS * DV // N_TP
        att_cols = AQH * HD // N_TP
        mixed = jnp.zeros((SEQUENCE_LENGTH, D), jnp.float32)
        for group_index in range(N_TP):
            partial_value = jnp.dot(ret_hidden[:, group_index * ret_cols:(group_index + 1) * ret_cols], ret_out[group_index * ret_cols:(group_index + 1) * ret_cols], preferred_element_type=jnp.float32)
            partial_value = partial_value + jnp.dot(att_hidden[:, group_index * att_cols:(group_index + 1) * att_cols], att_out[group_index * att_cols:(group_index + 1) * att_cols], preferred_element_type=jnp.float32)
            rounded = lax.optimization_barrier(partial_value.astype(jnp.bfloat16))
            mixed = mixed + rounded.astype(jnp.float32)
        return mixed.astype(jnp.bfloat16)
    return lax.map(one_sequence, (tokens, log_decay, start_state))
```

```python
import functools

import jax
import jax.numpy as jnp
import numpy as np
from jax import lax
from jax.experimental import pallas as pl
from jax.experimental.pallas import tpu as pltpu
from jax.sharding import PartitionSpec as P

DK = 256
DV = 256
HD = 64
WINDOW = 128
BLOCK = 128


epsilon = 1e-06
exact_result = lax.Precision.HIGHEST


def carried_in(array, axis, combine, identity):
    peers, mine = (lax.axis_size(axis), lax.axis_index(axis))
    everything = jax.tree.map(
        lambda part, kind: lax.all_gather(part.astype(kind), axis),
        array,
        (jnp.bfloat16, jnp.bfloat16),
    )
    start = jax.tree.map(
        lambda part, zero: jnp.broadcast_to(jnp.asarray(zero, part.dtype), part.shape),
        array,
        identity,
    )

    def hop(k, before):
        reached = k < mine
        new = combine(
            before, jax.tree.map(lambda part, own: part[k].astype(own.dtype), everything, array)
        )
        return jax.tree.map(lambda a, b: jnp.where(reached, a, b), new, before)

    return lax.fori_loop(0, peers, hop, start)


def passed_along(block, axis, distance):
    devices = range(lax.axis_size(axis))
    route = [(i - distance, i) for i in devices if i - distance in devices]
    return lax.ppermute(block, axis, route)


def rotate(values, positions):
    half_dim = values.shape[-1] // 2
    inverse = 1.0 / 10000.0 ** (jnp.arange(half_dim, dtype=jnp.float32) / half_dim)
    angles = positions.astype(jnp.float32)[:, None] * inverse[None, :]
    cosine = jnp.cos(angles)[:, None, :]
    sine_table = jnp.sin(angles)[:, None, :]
    front_half = values[..., :half_dim]
    back_half = values[..., half_dim:]
    return jnp.concatenate(
        [
            front_half * cosine - back_half * sine_table,
            front_half * sine_table + back_half * cosine,
        ],
        axis=-1,
    )


def block_step(memory_state, inputs):
    queries, key_matrix_rows, value_matrix_rows, log_rates = inputs
    length_here = log_rates.shape[-1]
    causal = jnp.arange(length_here)[:, None] >= jnp.arange(length_here)[None, :]
    running_totals = jnp.cumsum(log_rates, axis=-1)
    relative = running_totals[:, :, None] - running_totals[:, None, :]
    weight = jnp.where(causal[None], jnp.exp(jnp.where(causal[None], relative, 0.0)), 0.0)
    score_matrix = (
        jnp.einsum("hqd,hkd->hqk", queries, key_matrix_rows, precision=exact_result) * weight
    )
    carried_state = jnp.einsum(
        "hqd,hdv->hqv",
        queries * jnp.exp(running_totals)[:, :, None],
        memory_state,
        precision=exact_result,
    )
    output_rows = (
        jnp.einsum("arf,afu->aru", score_matrix, value_matrix_rows, precision=exact_result)
        + carried_state
    )
    decay_factors = jnp.exp(running_totals[:, -1:] - running_totals)
    memory_state = memory_state * jnp.exp(running_totals[:, -1])[:, None, None] + jnp.einsum(
        "iwj,iwe->ije",
        key_matrix_rows * decay_factors[:, :, None],
        value_matrix_rows,
        precision=exact_result,
    )
    return (memory_state, output_rows)


def chain(earlier, later):
    return (earlier[0] * later[0], earlier[1] * later[0][:, None, None] + later[1])


def shards(
    tokens,
    norm_gain,
    ret_query,
    ret_key,
    ret_value,
    att_query,
    att_key,
    att_value,
    log_decay,
    start_state,
    ret_gain,
    sink_logits,
    ret_out,
    att_out,
):
    gathered = lax.all_gather(tokens[0], "tp", axis=1, tiled=True)
    row_count = gathered.shape[0]
    as_float = gathered.astype(jnp.float32)
    normed = (
        as_float
        * lax.rsqrt(jnp.mean(as_float * as_float, axis=-1, keepdims=True) + epsilon)
        * norm_gain
    ).astype(jnp.bfloat16)
    offset = lax.axis_index("sp") * row_count
    positions = offset + jnp.arange(row_count, dtype=jnp.int32)
    weights = (ret_query, ret_key, ret_value, att_query, att_key, att_value)
    pieces = (
        lax.all_gather(weights[0], "sp", axis=0, tiled=True),
        lax.all_gather(weights[1], "sp", axis=0, tiled=True),
        lax.all_gather(weights[2], "sp", axis=0, tiled=True),
        lax.all_gather(weights[3], "sp", axis=0, tiled=True),
        lax.all_gather(weights[4], "sp", axis=0, tiled=True),
        lax.all_gather(weights[5], "sp", axis=0, tiled=True),
    )
    projected = tuple(
        (jnp.dot(normed, piece, preferred_element_type=jnp.float32) for piece in pieces)
    )
    rounded = tuple((product_f.astype(jnp.bfloat16) for product_f in projected))
    projected = rounded[:3]
    head_count = projected[0].shape[1] // DK
    queries = rotate(projected[0].astype(jnp.float32).reshape(row_count, head_count, DK), positions)
    keys_rot = rotate(
        projected[1].astype(jnp.float32).reshape(row_count, head_count, DK), positions
    ) * DK ** (-0.5)
    values_f = projected[2].astype(jnp.float32).reshape(row_count, head_count, DV)
    log_rates = log_decay[0]
    count = row_count // BLOCK

    def blocked(array):
        return array.reshape(count, BLOCK, head_count, array.shape[-1]).transpose(0, 2, 1, 3)

    rates_blocked = log_rates.reshape(head_count, count, BLOCK).transpose(1, 0, 2)
    local_state, pieces = lax.scan(
        block_step,
        jnp.zeros((head_count, DK, DV), jnp.float32),
        (blocked(queries), blocked(keys_rot), blocked(values_f), rates_blocked),
    )
    local_out = pieces.transpose(0, 2, 1, 3).reshape(row_count, head_count, DV)
    running_totals = jnp.cumsum(log_rates, axis=-1)
    device_decay = jnp.exp(running_totals[:, -1])
    identity = (jnp.ones((head_count,), jnp.float32), jnp.zeros((head_count, DK, DV), jnp.float32))
    prior_decay, prior_state = carried_in((device_decay, local_state), "sp", chain, identity)
    incoming = prior_state + prior_decay[:, None, None] * start_state[0]
    retained = local_out + jnp.einsum(
        "thd,hdv->thv",
        queries * jnp.exp(running_totals).T[:, :, None],
        incoming,
        precision=exact_result,
    )
    centred = retained - jnp.mean(retained, axis=-1, keepdims=True)
    variance = jnp.mean(centred * centred, axis=-1, keepdims=True)
    ret_hidden = (
        (centred * lax.rsqrt(variance + epsilon)).reshape(row_count, head_count * DV) * ret_gain
    ).astype(jnp.bfloat16)
    att_queries, att_keys, att_values = rounded[3:]
    kv_heads = att_keys.shape[1] // HD
    groups = att_queries.shape[1] // HD // kv_heads
    earlier_keys, earlier_values = passed_along(
        (att_keys[row_count - WINDOW :], att_values[row_count - WINDOW :]), "sp", 1
    )
    extended_keys = jnp.concatenate([earlier_keys, att_keys], axis=0)
    extended_values = jnp.concatenate([earlier_values, att_values], axis=0)
    windows = row_count // WINDOW

    def banded(array):
        earlier = array[:row_count].reshape(windows, WINDOW, kv_heads, HD)
        current = array[WINDOW:].reshape(windows, WINDOW, kv_heads, HD)
        return jnp.concatenate([earlier, current], axis=1)

    key_band = banded(extended_keys)
    value_band = banded(extended_values)
    grouped_q = att_queries.reshape(windows, WINDOW, kv_heads, groups, HD)
    score_matrix = jnp.einsum(
        "nqhgd,nkhd->nhgqk", grouped_q, key_band, preferred_element_type=jnp.float32
    ) * HD ** (-0.5)
    query_index = WINDOW + jnp.arange(WINDOW)
    key_index = jnp.arange(2 * WINDOW)
    allowed = (key_index[None, :] <= query_index[:, None]) & (
        query_index[:, None] - key_index[None, :] < WINDOW
    )
    key_place = offset - WINDOW + jnp.arange(windows)[:, None] * WINDOW + key_index[None, :]
    visible = (allowed[None] & (key_place >= 0)[:, None, :])[:, None, None]
    expo = jnp.exp(jnp.where(visible, score_matrix, -1e30))
    summed = jnp.sum(expo, axis=-1, keepdims=True) + jnp.exp(sink_logits).reshape(
        1, kv_heads, groups, 1, 1
    )
    probs = (expo / summed).astype(jnp.bfloat16)
    attended = jnp.einsum(
        "nhgqk,nkhd->nqhgd", probs, value_band, preferred_element_type=jnp.float32
    )
    att_hidden = attended.astype(jnp.bfloat16).reshape(row_count, kv_heads * groups * HD)
    ret_width = ret_hidden.shape[1]
    joined = jnp.concatenate([ret_hidden, att_hidden], axis=1)[None]
    piece = lax.all_gather(joined, "fs", axis=0, tiled=True)
    product = jnp.einsum(
        "srh,hd->srd", piece[:, :, :ret_width], ret_out, preferred_element_type=jnp.float32
    )
    product = product + jnp.einsum(
        "srh,hd->srd", piece[:, :, ret_width:], att_out, preferred_element_type=jnp.float32
    )
    partial_rows = product.astype(jnp.bfloat16)
    regrouped = lax.all_to_all(partial_rows, "fs", split_axis=0, concat_axis=2, tiled=True)
    mixed = lax.psum_scatter(
        regrouped[0].astype(jnp.float32).astype(jnp.bfloat16), "tp", scatter_dimension=1, tiled=True
    )
    return mixed[None]


MESH = pl.DeviceIdType.MESH
F32 = jnp.float32
BF16 = jnp.bfloat16
GAIN_ROW = 0
DECAY_ROW = 1
SINK_ROW = 2
K_AT, V_AT, KV_AT, Q_AT, A_AT = 0, 256, 512, 640, 896


def dot(a, b):
    return jnp.dot(a, b, preferred_element_type=F32)


def dot_t(a, b):
    return lax.dot_general(a, b, (((1,), (1,)), ((), ())), preferred_element_type=F32)


def dot_l(a, b):
    return lax.dot_general(a, b, (((0,), (0,)), ((), ())), preferred_element_type=F32)


def fused(
    tok_in, ngain_in, rq, rk, rv, aq, ak, av, gain_in, decay_in, sink_in, start, ro, ao, cos_in, sin_in, out,
    ngain, gain_v, decay_v, sink_v, ak_v, av_v, cos, sin, insem,
    small, sm, traw, xn, akp, w, wo, s0, local_state, sbuf, states, kbuf, vbuf, qbuf, aqbuf, kvp, inner, hid, hin,
    total, ob,
    send, smsem, tsem, ownsem, zsem, ysem, psem, wosem, ssem, stsem, halosem, hsem, outsem,
):
    z, f, c = lax.axis_index("sp"), lax.axis_index("fs"), lax.axis_index("tp")
    y, x = f // 2, lax.rem(f, 2)
    zh, zb = z // 2, lax.rem(z, 2)
    peer = 1 - c
    fx, fy = 2 * y + 1 - x, 2 * (1 - y) + x
    zp, z2, z3 = z + 1 - 2 * zb, lax.rem(z + 2, 4), 3 - z
    head = 2 * zb + x
    rows, half = tok_in.shape
    depth = rq.shape[0]
    part = depth // 4
    mid = jnp.logical_or(z == 1, z == 2)
    near, far = jnp.where(mid, z3, z2), jnp.where(mid, z2, z3)
    order = (zp, near, far)
    first, second = zh == 0, zh == 1

    loads = [
        (ngain_in, ngain), (gain_in, gain_v), (decay_in, decay_v), (sink_in, sink_v), (ak, ak_v), (av, av_v),
        (cos_in.at[pl.ds(pl.multiple_of(zh * 2 * rows, 2 * rows), 2 * rows)], cos),
        (sin_in.at[pl.ds(pl.multiple_of(zh * 2 * rows, 2 * rows), 2 * rows)], sin),
    ]
    inputs = [pltpu.make_async_copy(src, dst, insem.at[i]) for i, (src, dst) in enumerate(loads)]
    for copy in inputs:
        copy.start()

    barrier = pltpu.get_barrier_semaphore()
    greeted = [{"tp": peer}, {"fs": fy}]
    for t in range(2):
        core = jnp.int32(t)
        greeted += [{"sp": zs, "tp": core} for zs in order]
        greeted += [{"fs": fx, "tp": core}, {"sp": zp, "fs": fx, "tp": core}]
    for where in greeted:
        pl.semaphore_signal(barrier, inc=1, device_id=where, device_id_type=MESH)
    pl.semaphore_wait(barrier, len(greeted))

    sent = []
    slots = iter(range(send.shape[0]))

    def both(a, b):
        if a is None:
            return b
        return a if b is None else jnp.logical_and(a, b)

    def remote(cond, src, dst, rsem, **where):
        copy = pltpu.make_async_remote_copy(
            src_ref=src, dst_ref=dst, send_sem=send.at[next(slots)], recv_sem=rsem,
            device_id=where, device_id_type=MESH,
        )
        sent.append((cond, copy))
        if cond is None:
            copy.start()
        else:
            pl.when(cond)(copy.start)

    def local(cond, src, dst, sem):
        copy = pltpu.make_async_copy(src, dst, sem)
        if cond is None:
            copy.start()
        else:
            pl.when(cond)(copy.start)

    def arrived(dst, sem):
        pltpu.make_async_copy(dst, dst, sem).wait()

    mine = traw.at[zb, c]
    local(c == x, tok_in, mine, tsem.at[zb, c])
    remote(c != x, tok_in, mine, tsem.at[zb, c], tp=peer)
    remote(None, tok_in, mine, tsem.at[zb, c], sp=zp, tp=x)
    remote(None, tok_in, mine, tsem.at[zb, c], fs=fx, tp=x)

    pieces = ((K_AT, 512), (KV_AT, 128), (Q_AT, 256), (A_AT, 256))

    def rows_of(zs, ys, cs):
        return pl.ds(pl.multiple_of(zs * depth + ys * 2 * part + cs * part, part), part)

    to_a = jnp.where(zb == c, z2, zp)
    column = pl.ds(pl.multiple_of(x * DK, DK), DK)

    def send_weights(p):
        arrays = {0: ((rk, K_AT, DK), (rv, V_AT, DK)), 1: ((akp, KV_AT, 128),), 2: ((rq, Q_AT, DK),),
                  3: ((aq, A_AT, DK),)}[p]
        for a, at, width in arrays:
            cols = pl.ds(0, width) if a is akp else column
            for cond, to in ((None, to_a), (zb != c, z3)):
                for t in range(2):
                    src = a.at[pl.ds(pl.multiple_of(y * 2 * part + t * part, part), part), cols]
                    remote(cond, src, w.at[rows_of(z, y, t), pl.ds(at, width)], zsem.at[p, z], sp=to, tp=jnp.int32(t))
        for a, at, width in arrays:
            cols = pl.ds(0, width) if a is akp else column
            dst = w.at[pl.ds(pl.multiple_of(z * depth, depth), depth), pl.ds(at, width)]
            local(c == zb, a.at[:, cols], dst, ownsem.at[p])
            remote(c == zb, a.at[:, cols], dst, ownsem.at[p], tp=peer)

    send_weights(0)

    out_rows, out_cols = ro.shape

    def out_block(kind, ys, cs):
        return wo.at[kind, ys, pl.ds(pl.multiple_of(cs * out_rows, out_rows), out_rows)], wosem.at[kind, ys, cs]

    def send_out(kind):
        a = (ro, ao)[kind]
        block, sem = out_block(kind, y, c)
        remote(None, a, block, sem, fs=fy)
        remote(None, a, block, sem, tp=peer)
        local(None, a, block, sem)

    def pass_out(kind):
        block, sem = out_block(kind, 1 - y, c)
        arrived(block, sem)
        remote(None, block, block, sem, tp=peer)

    def wait_out(kind):
        for ys, cs in ((y, c), (y, peer), (1 - y, peer)):
            arrived(*out_block(kind, ys, cs))

    send_out(0)

    for i in (1, 2, 3):
        inputs[i].wait()
    small[...] = jnp.zeros_like(small)
    small[pl.ds(GAIN_ROW, 1), :] = gain_v[...]
    for j in range(2):
        small[pl.ds(DECAY_ROW, 1), pl.ds(j * rows, rows)] = decay_v[pl.ds(j, 1), :]
    small[pl.ds(SINK_ROW, 1), pl.ds(0, sink_v.shape[1])] = sink_v[...]
    inputs[4].wait()
    inputs[5].wait()
    packed = [
        jnp.concatenate([ak_v[:, j * HD : (j + 1) * HD], av_v[:, j * HD : (j + 1) * HD]], axis=1) for j in range(2)
    ]
    akp[...] = jnp.where(x == 0, packed[0], packed[1])

    for xs in range(2):
        dx = x if xs == 0 else 1 - x
        fd = f if xs == 0 else fx
        here = jnp.logical_and(zb == c, c == x) if xs == 0 else None
        away = jnp.logical_not(here) if xs == 0 else None
        if xs == 0:
            local(here, small, sm.at[zb], smsem.at[zb])
        remote(away, small, sm.at[zb], smsem.at[zb], sp=2 * zh + c, fs=fd, tp=x)
        gives = jnp.logical_and(first, zb == c)
        src = start.at[dx]
        if xs == 0:
            local(both(gives, c == x), src, s0, ssem)
            remote(both(gives, c != x), src, s0, ssem, tp=peer)
        else:
            remote(gives, src, s0, ssem, fs=fd, tp=x)

    send_weights(1)
    send_weights(2)
    send_weights(3)

    for t in range(2):
        block = traw.at[1 - zb, t]

        @pl.when(c == x)
        def _():
            arrived(block, tsem.at[1 - zb, t])

        remote(c == x, block, block, tsem.at[1 - zb, t], fs=fx)

    def take(p):
        at, width = pieces[p]
        cols = pl.ds(at, width)
        for zs in order:
            block = w.at[rows_of(zs, y, c), cols]
            arrived(block, zsem.at[p, zs])
            remote(None, block, block, ysem.at[p, zs], fs=fy)
            remote(None, block, block, psem.at[p], tp=peer)

    def spread(p):
        at, width = pieces[p]
        cols = pl.ds(at, width)
        for zs in order:
            block = w.at[rows_of(zs, 1 - y, c), cols]
            arrived(block, ysem.at[p, zs])
            remote(None, block, block, psem.at[p], tp=peer)

    def complete(p):
        at, width = pieces[p]
        cols = pl.ds(at, width)
        arrived(w.at[pl.ds(0, depth), cols], ownsem.at[p])
        arrived(w.at[pl.ds(0, 6 * part), cols], psem.at[p])

    inputs[0].wait()

    def normalize(b):
        @pl.loop(0, rows // 32)
        def _(i):
            at = pl.ds(pl.multiple_of(i * 32, 32), 32)
            to = pl.ds(pl.multiple_of(b * rows + i * 32, 32), 32)
            h0, h1 = traw[b, 0, at, :].astype(F32), traw[b, 1, at, :].astype(F32)
            squares = jnp.sum(h0 * h0, axis=-1, keepdims=True) + jnp.sum(h1 * h1, axis=-1, keepdims=True)
            scale = lax.rsqrt(squares / (2 * half) + epsilon)
            xn[to, pl.ds(0, half)] = (h0 * scale * ngain[:, pl.ds(0, half)]).astype(BF16)
            xn[to, pl.ds(half, half)] = (h1 * scale * ngain[:, pl.ds(half, half)]).astype(BF16)

    def token_wait(b):
        for t in range(2):
            block, sem = traw.at[b, t], tsem.at[b, t]
            if b is other:
                pl.when(c != x)(functools.partial(arrived, block, sem))
            else:
                arrived(block, sem)

    own, other = zb, 1 - zb
    token_wait(own)
    normalize(own)
    take(0)
    send_out(1)
    spread(0)
    token_wait(other)
    normalize(other)
    inputs[6].wait()
    inputs[7].wait()
    for b in range(2):
        arrived(sm.at[b], smsem.at[b])
    complete(0)

    def block_at(b):
        return pl.ds(pl.multiple_of(b * rows, rows), rows)

    def tile(b, at, width):
        return dot(xn[block_at(b), :], w[:, pl.ds(at, width)])

    h = DK // 2

    def turn(a, b, factor):
        co, si = cos[block_at(b), :], sin[block_at(b), :]
        lo, hi = a[:, :h], a[:, h:]
        return jnp.concatenate([(lo * co - hi * si) * factor, (lo * si + hi * co) * factor], axis=1).astype(BF16)

    lane = lax.broadcasted_iota(jnp.int32, (rows, rows), 1)
    row = lax.broadcasted_iota(jnp.int32, (rows, rows), 0)

    def rates(b):
        l = sm[b, pl.ds(DECAY_ROW, 1), pl.ds(pl.multiple_of(x * rows, rows), rows)]
        cum = jnp.sum(jnp.where(lane <= row, l, 0.0), axis=1, keepdims=True)
        return cum, jnp.sum(l, axis=1, keepdims=True)

    @pl.loop(0, 2)
    def _(b):
        at = block_at(b)
        k = turn(tile(b, K_AT, DK).astype(BF16).astype(F32), b, DK ** (-0.5))
        kbuf[at, :] = k
        v = tile(b, V_AT, DV).astype(BF16)
        vbuf[at, :] = v
        cum, whole = rates(b)
        kd = (k.astype(F32) * jnp.exp(whole - cum)).astype(BF16)
        local_state[b] = dot_l(kd, v)

    def decay_of(b):
        return jnp.exp(rates(b)[1])

    @pl.when(first)
    def _():
        arrived(s0, ssem)
        states[0] = s0[...].astype(BF16)
        after = s0[...] * decay_of(0) + local_state[0]
        states[1] = after.astype(BF16)
        sbuf[...] = (after * decay_of(1) + local_state[1]).astype(BF16)

    remote(first, sbuf, states.at[0], stsem, sp=z2)

    take(1)
    spread(1)
    take(2)
    complete(1)

    @pl.when(first)
    def _():
        kvp[pl.ds(0, WINDOW), :] = jnp.zeros((WINDOW, kvp.shape[1]), BF16)

    @pl.loop(0, 2)
    def _(b):
        to = pl.ds(pl.multiple_of(WINDOW + b * rows, WINDOW), rows)
        kvp[to, :] = tile(b, KV_AT, 128).astype(BF16)

    remote(first, kvp.at[pl.ds(2 * rows, WINDOW)], kvp.at[pl.ds(0, WINDOW)], halosem, sp=z2)
    pass_out(0)
    spread(2)
    take(3)
    complete(2)

    @pl.loop(0, 2)
    def _(b):
        at = block_at(b)
        q = turn(tile(b, Q_AT, DK).astype(BF16).astype(F32), b, 1.0)
        qbuf[at, :] = q
        cum, _ = rates(b)
        cum_row = jnp.sum(jnp.where(lane == row, cum, 0.0), axis=0, keepdims=True)
        weight = jnp.where(lane <= row, jnp.exp(jnp.where(lane <= row, cum - cum_row, 0.0)), 0.0)
        scores = (dot_t(q, kbuf[at, :]) * weight).astype(BF16)
        inner[at, :] = dot(scores, vbuf[at, :])

    spread(3)

    @pl.when(second)
    def _():
        arrived(states.at[0], stsem)
        states[1] = (states[0].astype(F32) * decay_of(0) + local_state[0]).astype(BF16)

    def hand_on(kind, b):
        if b is other:
            remote(None, hid.at[kind, other], hin.at[kind, head], hsem.at[kind, head], sp=zp)
            remote(None, hid.at[kind, other], hin.at[kind, head], hsem.at[kind, head], sp=zp, fs=fx)
        else:
            remote(None, hid.at[kind, own], hin.at[kind, head], hsem.at[kind, head], fs=fx)
            local(None, hid.at[kind, own], hin.at[kind, head], hsem.at[kind, head])

    gain_at = pl.ds(pl.multiple_of(x * DV, DV), DV)
    for b in (other, own):
        at = block_at(b)
        cum, _ = rates(b)
        o = inner[at, :] + dot((qbuf[at, :].astype(F32) * jnp.exp(cum)).astype(BF16), states[b])
        centred = o - jnp.mean(o, axis=-1, keepdims=True)
        var = jnp.mean(centred * centred, axis=-1, keepdims=True)
        hid[0, b] = (centred * lax.rsqrt(var + epsilon) * sm[0, pl.ds(GAIN_ROW, 1), gain_at]).astype(BF16)
        hand_on(0, b)

    complete(3)

    @pl.loop(0, 2)
    def _(b):
        aqbuf[block_at(b), :] = tile(b, A_AT, DK).astype(BF16)

    lane2 = lax.broadcasted_iota(jnp.int32, (WINDOW, 2 * WINDOW), 1)
    row2 = lax.broadcasted_iota(jnp.int32, (WINDOW, 2 * WINDOW), 0)
    per = rows // WINDOW
    groups = DK // HD
    pl.when(second)(functools.partial(arrived, kvp.at[pl.ds(0, WINDOW)], halosem))
    sink_row = sm[0, pl.ds(SINK_ROW, 1), pl.ds(0, 128)]
    sink_lane = lax.broadcasted_iota(jnp.int32, (1, 128), 1)
    sinks = [
        jnp.exp(jnp.sum(jnp.where(sink_lane == x * groups + i, sink_row, 0.0), axis=1, keepdims=True))
        for i in range(groups)
    ]

    for b in (other, own):
        @pl.loop(0, per)
        def _(i):
            n = b * per + i
            at = pl.ds(pl.multiple_of(n * WINDOW, WINDOW), WINDOW)
            band = kvp[pl.ds(pl.multiple_of(n * WINDOW, WINDOW), 2 * WINDOW), :]
            k, v = band[:, :HD], band[:, HD:]
            seen = (lane2 <= row2 + WINDOW) & (lane2 > row2)
            visible = seen & (lane2 + n * WINDOW + zh * 2 * rows >= WINDOW)
            res = []
            for g in range(groups):
                q = aqbuf[at, pl.ds(g * HD, HD)]
                e = jnp.exp(jnp.where(visible, dot_t(q, k) * HD ** (-0.5), -1e30))
                norm = jnp.sum(e, axis=-1, keepdims=True) + sinks[g]
                res.append(dot((e / norm).astype(BF16), v))
            hid[1, b, pl.ds(pl.multiple_of(i * WINDOW, WINDOW), WINDOW), :] = jnp.concatenate(res, axis=1).astype(BF16)

        hand_on(1, b)

    pass_out(1)
    wait_out(0)
    for kind in range(2):
        if kind == 1:
            wait_out(1)
        for hz, hx in ((zb, x), (1 - zb, x), (zb, 1 - x), (1 - zb, 1 - x)):
            arrived(hin.at[kind, 2 * hz + hx], hsem.at[kind, 2 * hz + hx])
        for t in range(4):
            cols = pl.ds(t % 2 * 256, 256)
            acc = None
            for n in range(4):
                term = dot(hin[kind, n], wo[kind, t // 2, pl.ds(n * DV, DV), cols])
                acc = term if acc is None else acc + term
            if kind == 0:
                total[:, pl.ds(t * 256, 256)] = acc
                continue
            ob[t] = (total[:, pl.ds(t * 256, 256)] + acc).astype(BF16)
            yq = t // 2
            dst = out.at[:, pl.ds(pl.multiple_of(x * out_cols + t % 2 * 256, 256), 256)]
            home = c == x
            local(both(home, c == yq), ob.at[t], dst, outsem)
            remote(both(home, c != yq), ob.at[t], dst, outsem, tp=peer)
            remote(jnp.logical_not(home), ob.at[t], dst, outsem, fs=fx, tp=jnp.int32(yq))

    arrived(out, outsem)
    for cond, copy in sent:
        if cond is None:
            copy.wait_send()
        else:
            pl.when(cond)(copy.wait_send)


def layer(mesh, *args):
    (tokens, norm_gain, ret_query, ret_key, ret_value, att_query, att_key, att_value,
     log_decay, start_state, ret_gain, sink_logits, ret_out, att_out) = args
    n_sp, n_fs, n_tp = mesh.shape["sp"], mesh.shape["fs"], mesh.shape["tp"]
    heads = ret_query.shape[1] // DK
    kv_heads = att_key.shape[1] // HD
    rows, half = tokens.shape[1:]
    depth = ret_query.shape[0]
    square = (
        n_tp == 2 and n_fs == 4 and n_sp == 4 and heads == 2 and kv_heads == 2
        and att_query.shape[1] == ret_query.shape[1] and rows == DK and tokens.shape[0] == 1
        and 2 * half == n_sp * depth and ret_out.shape == att_out.shape
        and ret_out.shape == (heads * DV, half // 2) and half == 4 * DK
    )
    if not square:
        return shards(*args)
    h = DK // 2
    length = n_sp * rows
    inverse = np.float32(1.0) / np.float32(10000.0) ** (np.arange(h, dtype=np.float32) / np.float32(h))
    angles = np.arange(length, dtype=np.float32)[:, None] * inverse[None, :]
    cos = jnp.asarray(np.cos(angles), F32)
    sin = jnp.asarray(np.sin(angles), F32)
    wide = heads * rows
    hbm = pl.BlockSpec(memory_space=pl.ANY)
    dma = pltpu.SemaphoreType.DMA
    v = pltpu.VMEM
    res = pl.pallas_call(
        fused,
        out_shape=jax.ShapeDtypeStruct((rows, half), BF16),
        in_specs=[hbm] * 16,
        out_specs=hbm,
        scratch_shapes=[
            v((1, norm_gain.shape[0]), F32),
            v((1, ret_gain.shape[0]), F32),
            v((heads, rows), F32),
            v((1, sink_logits.shape[0]), F32),
            v(att_key.shape, BF16),
            v(att_value.shape, BF16),
            v((2 * rows, h), F32),
            v((2 * rows, h), F32),
            dma((8,)),
            v((8, wide), F32),
            v((2, 8, wide), F32),
            v((2, 2, rows, half), BF16),
            v((2 * rows, 2 * half), BF16),
            v((depth, 128), BF16),
            v((n_sp * depth, A_AT + DK), BF16),
            v((2, 2, 2 * ret_out.shape[0], ret_out.shape[1]), BF16),
            v((DK, DV), F32),
            v((2, DK, DV), F32),
            v((DK, DV), BF16),
            v((2, DK, DV), BF16),
            v((2 * rows, DK), BF16),
            v((2 * rows, DV), BF16),
            v((2 * rows, DK), BF16),
            v((2 * rows, DK), BF16),
            v((WINDOW + 2 * rows, 128), BF16),
            v((2 * rows, DV), F32),
            v((2, 2, rows, DV), BF16),
            v((2, 4, rows, DV), BF16),
            v((rows, half), F32),
            v((4, rows, 256), BF16),
            dma((128,)),
            dma((2,)),
            dma((2, 2)),
            dma((4,)),
            dma((4, n_sp)),
            dma((4, n_sp)),
            dma((4,)),
            dma((2, 2, 2)),
            dma,
            dma,
            dma,
            dma((2, 4)),
            dma,
        ],
        compiler_params=pltpu.CompilerParams(
            collective_id=0, has_side_effects=True, vmem_limit_bytes=67043328
        ),
    )(
        tokens[0], norm_gain[None], ret_query, ret_key, ret_value, att_query, att_key, att_value,
        ret_gain[None], log_decay[0], sink_logits[None], start_state[0], ret_out, att_out, cos, sin,
    )
    return res[None]


def solution(mesh):
    placed = (
        P("fs", "sp", "tp"),
        P(),
        P("sp", "tp"),
        P("sp", "tp"),
        P("sp", "tp"),
        P("sp", "tp"),
        P("sp", "tp"),
        P("sp", "tp"),
        P("fs", "tp", "sp"),
        P("fs", "tp", None, None),
        P("tp"),
        P("tp"),
        P("tp", "fs"),
        P("tp", "fs"),
    )
    return jax.shard_map(
        functools.partial(layer, mesh), mesh=mesh, in_specs=placed, out_specs=P("fs", "sp", "tp"), check_vma=False
    )
```

```python
import functools

import jax
import jax.numpy as jnp
import numpy as np
from jax import lax
from jax.experimental import pallas as pl
from jax.experimental.pallas import tpu as pltpu
from jax.sharding import PartitionSpec as P

DK = 256
DV = 256
HD = 64
WINDOW = 128
BLOCK = 128


epsilon = 1e-06
exact_result = lax.Precision.HIGHEST


def carried_in(array, axis, combine, identity):
    peers, mine = (lax.axis_size(axis), lax.axis_index(axis))
    everything = jax.tree.map(
        lambda part, kind: lax.all_gather(part.astype(kind), axis),
        array,
        (jnp.bfloat16, jnp.bfloat16),
    )
    start = jax.tree.map(
        lambda part, zero: jnp.broadcast_to(jnp.asarray(zero, part.dtype), part.shape),
        array,
        identity,
    )

    def hop(k, before):
        reached = k < mine
        new = combine(
            before, jax.tree.map(lambda part, own: part[k].astype(own.dtype), everything, array)
        )
        return jax.tree.map(lambda a, b: jnp.where(reached, a, b), new, before)

    return lax.fori_loop(0, peers, hop, start)


def passed_along(block, axis, distance):
    devices = range(lax.axis_size(axis))
    route = [(i - distance, i) for i in devices if i - distance in devices]
    return lax.ppermute(block, axis, route)


def rotate(values, positions):
    half_dim = values.shape[-1] // 2
    inverse = 1.0 / 10000.0 ** (jnp.arange(half_dim, dtype=jnp.float32) / half_dim)
    angles = positions.astype(jnp.float32)[:, None] * inverse[None, :]
    cosine = jnp.cos(angles)[:, None, :]
    sine_table = jnp.sin(angles)[:, None, :]
    front_half = values[..., :half_dim]
    back_half = values[..., half_dim:]
    return jnp.concatenate(
        [
            front_half * cosine - back_half * sine_table,
            front_half * sine_table + back_half * cosine,
        ],
        axis=-1,
    )


def block_step(memory_state, inputs):
    queries, key_matrix_rows, value_matrix_rows, log_rates = inputs
    length_here = log_rates.shape[-1]
    causal = jnp.arange(length_here)[:, None] >= jnp.arange(length_here)[None, :]
    running_totals = jnp.cumsum(log_rates, axis=-1)
    relative = running_totals[:, :, None] - running_totals[:, None, :]
    weight = jnp.where(causal[None], jnp.exp(jnp.where(causal[None], relative, 0.0)), 0.0)
    score_matrix = (
        jnp.einsum("hqd,hkd->hqk", queries, key_matrix_rows, precision=exact_result) * weight
    )
    carried_state = jnp.einsum(
        "hqd,hdv->hqv",
        queries * jnp.exp(running_totals)[:, :, None],
        memory_state,
        precision=exact_result,
    )
    output_rows = (
        jnp.einsum("arf,afu->aru", score_matrix, value_matrix_rows, precision=exact_result)
        + carried_state
    )
    decay_factors = jnp.exp(running_totals[:, -1:] - running_totals)
    memory_state = memory_state * jnp.exp(running_totals[:, -1])[:, None, None] + jnp.einsum(
        "iwj,iwe->ije",
        key_matrix_rows * decay_factors[:, :, None],
        value_matrix_rows,
        precision=exact_result,
    )
    return (memory_state, output_rows)


def chain(earlier, later):
    return (earlier[0] * later[0], earlier[1] * later[0][:, None, None] + later[1])


def shards(
    tokens,
    norm_gain,
    ret_query,
    ret_key,
    ret_value,
    att_query,
    att_key,
    att_value,
    log_decay,
    start_state,
    ret_gain,
    sink_logits,
    ret_out,
    att_out,
):
    gathered = lax.all_gather(tokens[0], "tp", axis=1, tiled=True)
    row_count = gathered.shape[0]
    as_float = gathered.astype(jnp.float32)
    normed = (
        as_float
        * lax.rsqrt(jnp.mean(as_float * as_float, axis=-1, keepdims=True) + epsilon)
        * norm_gain
    ).astype(jnp.bfloat16)
    offset = lax.axis_index("sp") * row_count
    positions = offset + jnp.arange(row_count, dtype=jnp.int32)
    weights = (ret_query, ret_key, ret_value, att_query, att_key, att_value)
    pieces = (
        lax.all_gather(weights[0], "sp", axis=0, tiled=True),
        lax.all_gather(weights[1], "sp", axis=0, tiled=True),
        lax.all_gather(weights[2], "sp", axis=0, tiled=True),
        lax.all_gather(weights[3], "sp", axis=0, tiled=True),
        lax.all_gather(weights[4], "sp", axis=0, tiled=True),
        lax.all_gather(weights[5], "sp", axis=0, tiled=True),
    )
    projected = tuple(
        (jnp.dot(normed, piece, preferred_element_type=jnp.float32) for piece in pieces)
    )
    rounded = tuple((product_f.astype(jnp.bfloat16) for product_f in projected))
    projected = rounded[:3]
    head_count = projected[0].shape[1] // DK
    queries = rotate(projected[0].astype(jnp.float32).reshape(row_count, head_count, DK), positions)
    keys_rot = rotate(
        projected[1].astype(jnp.float32).reshape(row_count, head_count, DK), positions
    ) * DK ** (-0.5)
    values_f = projected[2].astype(jnp.float32).reshape(row_count, head_count, DV)
    log_rates = log_decay[0]
    count = row_count // BLOCK

    def blocked(array):
        return array.reshape(count, BLOCK, head_count, array.shape[-1]).transpose(0, 2, 1, 3)

    rates_blocked = log_rates.reshape(head_count, count, BLOCK).transpose(1, 0, 2)
    local_state, pieces = lax.scan(
        block_step,
        jnp.zeros((head_count, DK, DV), jnp.float32),
        (blocked(queries), blocked(keys_rot), blocked(values_f), rates_blocked),
    )
    local_out = pieces.transpose(0, 2, 1, 3).reshape(row_count, head_count, DV)
    running_totals = jnp.cumsum(log_rates, axis=-1)
    device_decay = jnp.exp(running_totals[:, -1])
    identity = (jnp.ones((head_count,), jnp.float32), jnp.zeros((head_count, DK, DV), jnp.float32))
    prior_decay, prior_state = carried_in((device_decay, local_state), "sp", chain, identity)
    incoming = prior_state + prior_decay[:, None, None] * start_state[0]
    retained = local_out + jnp.einsum(
        "thd,hdv->thv",
        queries * jnp.exp(running_totals).T[:, :, None],
        incoming,
        precision=exact_result,
    )
    centred = retained - jnp.mean(retained, axis=-1, keepdims=True)
    variance = jnp.mean(centred * centred, axis=-1, keepdims=True)
    ret_hidden = (
        (centred * lax.rsqrt(variance + epsilon)).reshape(row_count, head_count * DV) * ret_gain
    ).astype(jnp.bfloat16)
    att_queries, att_keys, att_values = rounded[3:]
    kv_heads = att_keys.shape[1] // HD
    groups = att_queries.shape[1] // HD // kv_heads
    earlier_keys, earlier_values = passed_along(
        (att_keys[row_count - WINDOW :], att_values[row_count - WINDOW :]), "sp", 1
    )
    extended_keys = jnp.concatenate([earlier_keys, att_keys], axis=0)
    extended_values = jnp.concatenate([earlier_values, att_values], axis=0)
    windows = row_count // WINDOW

    def banded(array):
        earlier = array[:row_count].reshape(windows, WINDOW, kv_heads, HD)
        current = array[WINDOW:].reshape(windows, WINDOW, kv_heads, HD)
        return jnp.concatenate([earlier, current], axis=1)

    key_band = banded(extended_keys)
    value_band = banded(extended_values)
    grouped_q = att_queries.reshape(windows, WINDOW, kv_heads, groups, HD)
    score_matrix = jnp.einsum(
        "nqhgd,nkhd->nhgqk", grouped_q, key_band, preferred_element_type=jnp.float32
    ) * HD ** (-0.5)
    query_index = WINDOW + jnp.arange(WINDOW)
    key_index = jnp.arange(2 * WINDOW)
    allowed = (key_index[None, :] <= query_index[:, None]) & (
        query_index[:, None] - key_index[None, :] < WINDOW
    )
    key_place = offset - WINDOW + jnp.arange(windows)[:, None] * WINDOW + key_index[None, :]
    visible = (allowed[None] & (key_place >= 0)[:, None, :])[:, None, None]
    expo = jnp.exp(jnp.where(visible, score_matrix, -1e30))
    summed = jnp.sum(expo, axis=-1, keepdims=True) + jnp.exp(sink_logits).reshape(
        1, kv_heads, groups, 1, 1
    )
    probs = (expo / summed).astype(jnp.bfloat16)
    attended = jnp.einsum(
        "nhgqk,nkhd->nqhgd", probs, value_band, preferred_element_type=jnp.float32
    )
    att_hidden = attended.astype(jnp.bfloat16).reshape(row_count, kv_heads * groups * HD)
    ret_width = ret_hidden.shape[1]
    joined = jnp.concatenate([ret_hidden, att_hidden], axis=1)[None]
    piece = lax.all_gather(joined, "fs", axis=0, tiled=True)
    product = jnp.einsum(
        "srh,hd->srd", piece[:, :, :ret_width], ret_out, preferred_element_type=jnp.float32
    )
    product = product + jnp.einsum(
        "srh,hd->srd", piece[:, :, ret_width:], att_out, preferred_element_type=jnp.float32
    )
    partial_rows = product.astype(jnp.bfloat16)
    regrouped = lax.all_to_all(partial_rows, "fs", split_axis=0, concat_axis=2, tiled=True)
    mixed = lax.psum_scatter(
        regrouped[0].astype(jnp.float32).astype(jnp.bfloat16), "tp", scatter_dimension=1, tiled=True
    )
    return mixed[None]


MESH = pl.DeviceIdType.MESH
F32 = jnp.float32
BF16 = jnp.bfloat16
GAIN_ROW = 0
DECAY_ROW = 1
SINK_ROW = 2
K_AT, V_AT, KV_AT, Q_AT, A_AT = 0, 256, 512, 640, 896


def dot(a, b):
    return jnp.dot(a, b, preferred_element_type=F32)


def dot_t(a, b):
    return lax.dot_general(a, b, (((1,), (1,)), ((), ())), preferred_element_type=F32)


def dot_l(a, b):
    return lax.dot_general(a, b, (((0,), (0,)), ((), ())), preferred_element_type=F32)


def fused(
    tok_in, ngain_in, rq, rk, rv, aq, ak, av, gain_in, decay_in, sink_in, start, ro, ao, cos_in, sin_in, out,
    ngain, gain_v, decay_v, sink_v, ak_v, av_v, cos, sin, insem,
    small, sm, traw, xn, akp, w, wo, s0, local_state, sbuf, states, kbuf, vbuf, qbuf, aqbuf, kvp, inner, hid, hin,
    total, ob,
    send, smsem, tsem, ownsem, zsem, ysem, psem, wosem, ssem, stsem, halosem, hsem, outsem,
):
    z, f, c = lax.axis_index("sp"), lax.axis_index("fs"), lax.axis_index("tp")
    y, x = f // 2, lax.rem(f, 2)
    zh, zb = z // 2, lax.rem(z, 2)
    peer = 1 - c
    fx, fy = 2 * y + 1 - x, 2 * (1 - y) + x
    zp, z2, z3 = z + 1 - 2 * zb, lax.rem(z + 2, 4), 3 - z
    head = 2 * zb + x
    rows, half = tok_in.shape
    depth = rq.shape[0]
    part = depth // 4
    mid = jnp.logical_or(z == 1, z == 2)
    near, far = jnp.where(mid, z3, z2), jnp.where(mid, z2, z3)
    order = (zp, near, far)
    first, second = zh == 0, zh == 1

    loads = [
        (ngain_in, ngain), (gain_in, gain_v), (decay_in, decay_v), (sink_in, sink_v), (ak, ak_v), (av, av_v),
        (cos_in.at[pl.ds(pl.multiple_of(zh * 2 * rows, 2 * rows), 2 * rows)], cos),
        (sin_in.at[pl.ds(pl.multiple_of(zh * 2 * rows, 2 * rows), 2 * rows)], sin),
    ]
    inputs = [pltpu.make_async_copy(src, dst, insem.at[i]) for i, (src, dst) in enumerate(loads)]
    for copy in inputs:
        copy.start()

    barrier = pltpu.get_barrier_semaphore()
    greeted = [{"tp": peer}, {"fs": fy}]
    for t in range(2):
        core = jnp.int32(t)
        greeted += [{"sp": zs, "tp": core} for zs in order]
        greeted += [{"fs": fx, "tp": core}, {"sp": zp, "fs": fx, "tp": core}]
    for where in greeted:
        pl.semaphore_signal(barrier, inc=1, device_id=where, device_id_type=MESH)
    pl.semaphore_wait(barrier, len(greeted))

    sent = []
    slots = iter(range(send.shape[0]))

    def both(a, b):
        if a is None:
            return b
        return a if b is None else jnp.logical_and(a, b)

    def remote(cond, src, dst, rsem, **where):
        copy = pltpu.make_async_remote_copy(
            src_ref=src, dst_ref=dst, send_sem=send.at[next(slots)], recv_sem=rsem,
            device_id=where, device_id_type=MESH,
        )
        sent.append((cond, copy))
        if cond is None:
            copy.start()
        else:
            pl.when(cond)(copy.start)
        return copy

    def local(cond, src, dst, sem):
        copy = pltpu.make_async_copy(src, dst, sem)
        if cond is None:
            copy.start()
        else:
            pl.when(cond)(copy.start)

    def arrived(dst, sem):
        pltpu.make_async_copy(dst, dst, sem).wait()

    mine = traw.at[zb, c]
    local(c == x, tok_in, mine, tsem.at[zb, c])
    remote(c != x, tok_in, mine, tsem.at[zb, c], tp=peer)
    ahead = remote(None, tok_in, mine, tsem.at[zb, c], sp=zp, tp=x)
    remote(None, tok_in, mine, tsem.at[zb, c], fs=fx, tp=x)

    pieces = ((K_AT, DK), (V_AT, DV), (KV_AT, 128), (Q_AT, DK), (A_AT, 128), (A_AT + 128, 128))
    sources = (rk, rv, akp, rq, aq, aq)
    halved = 4

    def rows_of(zs, ys, cs):
        return pl.ds(pl.multiple_of(zs * depth + ys * 2 * part + cs * part, part), part)

    def rows_whole(zs, cs):
        return pl.ds(pl.multiple_of(zs * depth + cs * 2 * part, 2 * part), 2 * part)

    def weight(p):
        a, (at, width) = sources[p], pieces[p]
        offset = x * DK + (128 if p == 5 else 0)
        return a, pl.ds(0, width) if a is akp else pl.ds(pl.multiple_of(offset, 128), width), pl.ds(at, width)

    def send_weights(p, cond, to):
        a, cols, at = weight(p)
        for t in range(2):
            if p < halved:
                src = a.at[pl.ds(pl.multiple_of(y * 2 * part + t * part, part), part), cols]
                dst = w.at[rows_of(z, y, t), at]
            else:
                src = a.at[pl.ds(t * 2 * part, 2 * part), cols]
                dst = w.at[rows_whole(z, t), at]
            remote(cond, src, dst, zsem.at[p, z], sp=to, tp=jnp.int32(t))

    def keep_weights(p):
        a, cols, at = weight(p)
        dst = w.at[pl.ds(pl.multiple_of(z * depth, depth), depth), at]
        local(c == zb, a.at[:, cols], dst, ownsem.at[p])
        remote(c == zb, a.at[:, cols], dst, ownsem.at[p], tp=peer)

    to_a = jnp.where(zb == c, z2, zp)
    early = jnp.logical_and(zb != c, mid)
    late = jnp.logical_and(zb != c, jnp.logical_not(mid))
    for p in (0, 1, 3, 4, 5):
        send_weights(p, early, z3)
    for p in (0, 1, 3, 4, 5):
        keep_weights(p)

    out_rows, out_cols = ro.shape

    shares = ((0, 0, out_rows), (1, 0, out_rows // 2), (1, out_rows // 2, out_rows // 2))

    def out_block(share, ys, cs):
        kind, at, n = shares[share]
        rows_at = pl.ds(pl.multiple_of(cs * out_rows + at, n), n)
        return wo.at[kind, ys, rows_at], wosem.at[share, ys, cs]

    def send_out(share):
        kind, at, n = shares[share]
        a = (ro, ao)[kind].at[pl.ds(at, n)]
        block, sem = out_block(share, y, c)
        remote(None, a, block, sem, fs=fy)
        remote(None, a, block, sem, tp=peer)
        local(None, a, block, sem)

    def pass_out(share):
        block, sem = out_block(share, 1 - y, c)
        arrived(block, sem)
        remote(None, block, block, sem, tp=peer)

    def wait_out(kind):
        for share in ((0,), (1, 2))[kind]:
            for ys, cs in ((y, c), (y, peer), (1 - y, peer)):
                arrived(*out_block(share, ys, cs))

    send_out(0)
    send_out(1)

    for i in (1, 2, 3):
        inputs[i].wait()
    small[...] = jnp.zeros_like(small)
    small[pl.ds(GAIN_ROW, 1), :] = gain_v[...]
    for j in range(2):
        small[pl.ds(DECAY_ROW, 1), pl.ds(j * rows, rows)] = decay_v[pl.ds(j, 1), :]
    small[pl.ds(SINK_ROW, 1), pl.ds(0, sink_v.shape[1])] = sink_v[...]
    inputs[4].wait()
    inputs[5].wait()
    packed = [
        jnp.concatenate([ak_v[:, j * HD : (j + 1) * HD], av_v[:, j * HD : (j + 1) * HD]], axis=1) for j in range(2)
    ]
    akp[...] = jnp.where(x == 0, packed[0], packed[1])

    send_weights(2, early, z3)
    keep_weights(2)
    here = jnp.logical_and(zb == c, c == x)
    to_square = 2 * zh + c
    local(here, small, sm.at[zb], smsem.at[zb])
    remote(jnp.logical_not(here), small, sm.at[zb], smsem.at[zb], sp=to_square, tp=x)
    remote(None, small, sm.at[zb], smsem.at[zb], sp=to_square, fs=fx, tp=x)
    gives = jnp.logical_and(first, zb == c)
    local(both(gives, c == x), start.at[x], s0, ssem)
    remote(both(gives, c != x), start.at[x], s0, ssem, tp=peer)

    ahead.wait_send()
    for p in range(len(pieces)):
        send_weights(p, None, to_a)
        send_weights(p, late, z3)

    for t in range(2):
        block = traw.at[1 - zb, t]

        @pl.when(c == x)
        def _():
            arrived(block, tsem.at[1 - zb, t])

        remote(c == x, block, block, tsem.at[1 - zb, t], fs=fx)

    remote(gives, start.at[1 - x], s0, ssem, fs=fx, tp=x)

    def take(p):
        at, width = pieces[p]
        cols = pl.ds(at, width)
        for zs in order:
            block = w.at[rows_of(zs, y, c) if p < halved else rows_whole(zs, c), cols]
            arrived(block, zsem.at[p, zs])
            if p < halved:
                remote(None, block, block, ysem.at[p, zs], fs=fy)
            remote(None, block, block, psem.at[p], tp=peer)

    def spread(p):
        at, width = pieces[p]
        cols = pl.ds(at, width)
        for zs in order:
            block = w.at[rows_of(zs, 1 - y, c), cols]
            arrived(block, ysem.at[p, zs])
            remote(None, block, block, psem.at[p], tp=peer)

    def complete(p):
        at, width = pieces[p]
        cols = pl.ds(at, width)
        arrived(w.at[pl.ds(0, depth), cols], ownsem.at[p])
        arrived(w.at[pl.ds(0, 6 * part), cols], psem.at[p])

    inputs[0].wait()

    def normalize(b):
        @pl.loop(0, rows // 32)
        def _(i):
            at = pl.ds(pl.multiple_of(i * 32, 32), 32)
            to = pl.ds(pl.multiple_of(b * rows + i * 32, 32), 32)
            h0, h1 = traw[b, 0, at, :].astype(F32), traw[b, 1, at, :].astype(F32)
            squares = jnp.sum(h0 * h0, axis=-1, keepdims=True) + jnp.sum(h1 * h1, axis=-1, keepdims=True)
            scale = lax.rsqrt(squares / (2 * half) + epsilon)
            xn[to, pl.ds(0, half)] = (h0 * scale * ngain[:, pl.ds(0, half)]).astype(BF16)
            xn[to, pl.ds(half, half)] = (h1 * scale * ngain[:, pl.ds(half, half)]).astype(BF16)

    def token_wait(b):
        for t in range(2):
            block, sem = traw.at[b, t], tsem.at[b, t]
            if b is other:
                pl.when(c != x)(functools.partial(arrived, block, sem))
            else:
                arrived(block, sem)

    own, other = zb, 1 - zb
    token_wait(own)
    normalize(own)
    take(0)
    take(1)
    spread(0)
    take(2)
    spread(1)
    take(3)
    send_out(2)
    token_wait(other)
    normalize(other)
    inputs[6].wait()
    inputs[7].wait()
    for b in range(2):
        arrived(sm.at[b], smsem.at[b])
    complete(0)
    complete(1)

    def block_at(b):
        return pl.ds(pl.multiple_of(b * rows, rows), rows)

    def tile(b, at, width):
        return dot(xn[block_at(b), :], w[:, pl.ds(at, width)])

    h = DK // 2

    def turn(a, b, factor):
        co, si = cos[block_at(b), :], sin[block_at(b), :]
        lo, hi = a[:, :h], a[:, h:]
        return jnp.concatenate([(lo * co - hi * si) * factor, (lo * si + hi * co) * factor], axis=1).astype(BF16)

    lane = lax.broadcasted_iota(jnp.int32, (rows, rows), 1)
    row = lax.broadcasted_iota(jnp.int32, (rows, rows), 0)

    def rates(b):
        l = sm[b, pl.ds(DECAY_ROW, 1), pl.ds(pl.multiple_of(x * rows, rows), rows)]
        cum = jnp.sum(jnp.where(lane <= row, l, 0.0), axis=1, keepdims=True)
        return cum, jnp.sum(l, axis=1, keepdims=True)

    @pl.loop(0, 2)
    def _(b):
        at = block_at(b)
        k = turn(tile(b, K_AT, DK).astype(BF16).astype(F32), b, DK ** (-0.5))
        kbuf[at, :] = k
        v = tile(b, V_AT, DV).astype(BF16)
        vbuf[at, :] = v
        cum, whole = rates(b)
        kd = (k.astype(F32) * jnp.exp(whole - cum)).astype(BF16)
        local_state[b] = dot_l(kd, v)

    def decay_of(b):
        return jnp.exp(rates(b)[1])

    @pl.when(first)
    def _():
        arrived(s0, ssem)
        states[0] = s0[...].astype(BF16)
        after = s0[...] * decay_of(0) + local_state[0]
        states[1] = after.astype(BF16)
        sbuf[...] = (after * decay_of(1) + local_state[1]).astype(BF16)

    remote(first, sbuf, states.at[0], stsem, sp=z2)

    spread(2)
    spread(3)
    pass_out(0)
    pass_out(1)
    take(4)
    complete(2)

    @pl.when(first)
    def _():
        kvp[pl.ds(0, WINDOW), :] = jnp.zeros((WINDOW, kvp.shape[1]), BF16)

    @pl.loop(0, 2)
    def _(b):
        to = pl.ds(pl.multiple_of(WINDOW + b * rows, WINDOW), rows)
        kvp[to, :] = tile(b, KV_AT, 128).astype(BF16)

    remote(first, kvp.at[pl.ds(2 * rows, WINDOW)], kvp.at[pl.ds(0, WINDOW)], halosem, sp=z2)
    complete(3)

    def hand_on(kind, b, cols=None):
        sem = kind if cols is None else kind + cols
        at = pl.ds(0, DV) if cols is None else pl.ds(cols * 128, 128)
        src, dst, sem = hid.at[kind, b, :, at], hin.at[kind, head, :, at], hsem.at[sem, head]
        if b is other:
            remote(None, src, dst, sem, sp=zp)
            remote(None, src, dst, sem, sp=zp, fs=fx)
        else:
            remote(None, src, dst, sem, fs=fx)
            local(None, src, dst, sem)

    @pl.loop(0, 2)
    def _(b):
        at = block_at(b)
        q = turn(tile(b, Q_AT, DK).astype(BF16).astype(F32), b, 1.0)
        qbuf[at, :] = q
        cum, _ = rates(b)
        cum_row = jnp.sum(jnp.where(lane == row, cum, 0.0), axis=0, keepdims=True)
        weight = jnp.where(lane <= row, jnp.exp(jnp.where(lane <= row, cum - cum_row, 0.0)), 0.0)
        scores = (dot_t(q, kbuf[at, :]) * weight).astype(BF16)
        inner[at, :] = dot(scores, vbuf[at, :])

    @pl.when(second)
    def _():
        arrived(states.at[0], stsem)
        states[1] = (states[0].astype(F32) * decay_of(0) + local_state[0]).astype(BF16)

    gain_at = pl.ds(pl.multiple_of(x * DV, DV), DV)
    for b in (other, own):
        at = block_at(b)
        cum, _ = rates(b)
        o = inner[at, :] + dot((qbuf[at, :].astype(F32) * jnp.exp(cum)).astype(BF16), states[b])
        centred = o - jnp.mean(o, axis=-1, keepdims=True)
        var = jnp.mean(centred * centred, axis=-1, keepdims=True)
        hid[0, b] = (centred * lax.rsqrt(var + epsilon) * sm[0, pl.ds(GAIN_ROW, 1), gain_at]).astype(BF16)
        hand_on(0, b)

    lane2 = lax.broadcasted_iota(jnp.int32, (WINDOW, 2 * WINDOW), 1)
    row2 = lax.broadcasted_iota(jnp.int32, (WINDOW, 2 * WINDOW), 0)
    per = rows // WINDOW
    groups = DK // HD
    pl.when(second)(functools.partial(arrived, kvp.at[pl.ds(0, WINDOW)], halosem))
    sink_row = sm[0, pl.ds(SINK_ROW, 1), pl.ds(0, 128)]
    sink_lane = lax.broadcasted_iota(jnp.int32, (1, 128), 1)
    sinks = [
        jnp.exp(jnp.sum(jnp.where(sink_lane == x * groups + i, sink_row, 0.0), axis=1, keepdims=True))
        for i in range(groups)
    ]

    take(5)
    def attend(part_at, b):
        cols = pl.ds(part_at * 128, 128)
        aqbuf[block_at(b), cols] = tile(b, A_AT + part_at * 128, 128).astype(BF16)
        for i in range(per):
            n = b * per + i
            at = pl.ds(pl.multiple_of(n * WINDOW, WINDOW), WINDOW)
            band = kvp[pl.ds(pl.multiple_of(n * WINDOW, WINDOW), 2 * WINDOW), :]
            k, v = band[:, :HD], band[:, HD:]
            seen = (lane2 <= row2 + WINDOW) & (lane2 > row2)
            visible = seen & (lane2 + n * WINDOW + zh * 2 * rows >= WINDOW)
            q = aqbuf[at, cols]
            score = dot_t(jnp.concatenate([q[:, :HD], q[:, HD:]], axis=0), k) * HD ** (-0.5)
            probs = []
            for g in range(2):
                e = jnp.exp(jnp.where(visible, score[g * WINDOW : (g + 1) * WINDOW], -1e30))
                norm = 1.0 / (jnp.sum(e, axis=-1, keepdims=True) + sinks[part_at * 2 + g])
                probs.append((e * norm).astype(BF16))
            res = dot(jnp.concatenate(probs, axis=0), v)
            to = pl.ds(i * WINDOW, WINDOW)
            hid[1, b, to, cols] = jnp.concatenate([res[:WINDOW], res[WINDOW:]], axis=1).astype(BF16)

    for part_at in range(2):
        complete(4 + part_at)
        for b in (other, own):
            attend(part_at, b)
            hand_on(1, b, part_at)

    pass_out(2)
    for kind in range(2):
        wait_out(kind)
        for hz, hx in ((zb, x), (1 - zb, x), (zb, 1 - x), (1 - zb, 1 - x)):
            n = 2 * hz + hx
            if kind == 0:
                arrived(hin.at[0, n], hsem.at[0, n])
            else:
                for i in range(2):
                    arrived(hin.at[1, n, :, pl.ds(i * 128, 128)], hsem.at[1 + i, n])
        for t in range(4):
            cols = pl.ds(t % 2 * 256, 256)
            acc = None
            for n in range(4):
                term = dot(hin[kind, n], wo[kind, t // 2, pl.ds(n * DV, DV), cols])
                acc = term if acc is None else acc + term
            if kind == 0:
                total[:, pl.ds(t * 256, 256)] = acc
                continue
            ob[t] = (total[:, pl.ds(t * 256, 256)] + acc).astype(BF16)
            yq = t // 2
            dst = out.at[:, pl.ds(pl.multiple_of(x * out_cols + t % 2 * 256, 256), 256)]
            home = c == x
            local(both(home, c == yq), ob.at[t], dst, outsem)
            remote(both(home, c != yq), ob.at[t], dst, outsem, tp=peer)
            remote(jnp.logical_not(home), ob.at[t], dst, outsem, fs=fx, tp=jnp.int32(yq))

    arrived(out, outsem)
    for cond, copy in sent:
        if copy is ahead:
            continue
        if cond is None:
            copy.wait_send()
        else:
            pl.when(cond)(copy.wait_send)


def layer(mesh, *args):
    (tokens, norm_gain, ret_query, ret_key, ret_value, att_query, att_key, att_value,
     log_decay, start_state, ret_gain, sink_logits, ret_out, att_out) = args
    n_sp, n_fs, n_tp = mesh.shape["sp"], mesh.shape["fs"], mesh.shape["tp"]
    heads = ret_query.shape[1] // DK
    kv_heads = att_key.shape[1] // HD
    rows, half = tokens.shape[1:]
    depth = ret_query.shape[0]
    square = (
        n_tp == 2 and n_fs == 4 and n_sp == 4 and heads == 2 and kv_heads == 2
        and att_query.shape[1] == ret_query.shape[1] and rows == DK and tokens.shape[0] == 1
        and 2 * half == n_sp * depth and ret_out.shape == att_out.shape
        and ret_out.shape == (heads * DV, half // 2) and half == 4 * DK
    )
    if not square:
        return shards(*args)
    h = DK // 2
    length = n_sp * rows
    inverse = np.float32(1.0) / np.float32(10000.0) ** (np.arange(h, dtype=np.float32) / np.float32(h))
    angles = np.arange(length, dtype=np.float32)[:, None] * inverse[None, :]
    cos = jnp.asarray(np.cos(angles), F32)
    sin = jnp.asarray(np.sin(angles), F32)
    wide = heads * rows
    hbm = pl.BlockSpec(memory_space=pl.ANY)
    dma = pltpu.SemaphoreType.DMA
    v = pltpu.VMEM
    res = pl.pallas_call(
        fused,
        out_shape=jax.ShapeDtypeStruct((rows, half), BF16),
        in_specs=[hbm] * 16,
        out_specs=hbm,
        scratch_shapes=[
            v((1, norm_gain.shape[0]), F32),
            v((1, ret_gain.shape[0]), F32),
            v((heads, rows), F32),
            v((1, sink_logits.shape[0]), F32),
            v(att_key.shape, BF16),
            v(att_value.shape, BF16),
            v((2 * rows, h), F32),
            v((2 * rows, h), F32),
            dma((8,)),
            v((8, wide), F32),
            v((2, 8, wide), F32),
            v((2, 2, rows, half), BF16),
            v((2 * rows, 2 * half), BF16),
            v((depth, 128), BF16),
            v((n_sp * depth, A_AT + DK), BF16),
            v((2, 2, 2 * ret_out.shape[0], ret_out.shape[1]), BF16),
            v((DK, DV), F32),
            v((2, DK, DV), F32),
            v((DK, DV), BF16),
            v((2, DK, DV), BF16),
            v((2 * rows, DK), BF16),
            v((2 * rows, DV), BF16),
            v((2 * rows, DK), BF16),
            v((2 * rows, DK), BF16),
            v((WINDOW + 2 * rows, 128), BF16),
            v((2 * rows, DV), F32),
            v((2, 2, rows, DV), BF16),
            v((2, 4, rows, DV), BF16),
            v((rows, half), F32),
            v((4, rows, 256), BF16),
            dma((128,)),
            dma((2,)),
            dma((2, 2)),
            dma((6,)),
            dma((6, n_sp)),
            dma((6, n_sp)),
            dma((6,)),
            dma((3, 2, 2)),
            dma,
            dma,
            dma,
            dma((3, 4)),
            dma,
        ],
        compiler_params=pltpu.CompilerParams(
            collective_id=0, has_side_effects=True, vmem_limit_bytes=67043328
        ),
    )(
        tokens[0], norm_gain[None], ret_query, ret_key, ret_value, att_query, att_key, att_value,
        ret_gain[None], log_decay[0], sink_logits[None], start_state[0], ret_out, att_out, cos, sin,
    )
    return res[None]


def solution(mesh):
    placed = (
        P("fs", "sp", "tp"),
        P(),
        P("sp", "tp"),
        P("sp", "tp"),
        P("sp", "tp"),
        P("sp", "tp"),
        P("sp", "tp"),
        P("sp", "tp"),
        P("fs", "tp", "sp"),
        P("fs", "tp", None, None),
        P("tp"),
        P("tp"),
        P("tp", "fs"),
        P("tp", "fs"),
    )
    return jax.shard_map(
        functools.partial(layer, mesh), mesh=mesh, in_specs=placed, out_specs=P("fs", "sp", "tp"), check_vma=False
    )
```

```python
import functools

import jax
import jax.numpy as jnp
import numpy as np
from jax import lax
from jax.experimental import pallas as pl
from jax.experimental.pallas import tpu as pltpu
from jax.sharding import PartitionSpec as P

DK = 256
DV = 256
HD = 64
WINDOW = 128
BLOCK = 128


epsilon = 1e-06
exact_result = lax.Precision.HIGHEST


def carried_in(array, axis, combine, identity):
    peers, mine = (lax.axis_size(axis), lax.axis_index(axis))
    everything = jax.tree.map(
        lambda part, kind: lax.all_gather(part.astype(kind), axis),
        array,
        (jnp.bfloat16, jnp.bfloat16),
    )
    start = jax.tree.map(
        lambda part, zero: jnp.broadcast_to(jnp.asarray(zero, part.dtype), part.shape),
        array,
        identity,
    )

    def hop(k, before):
        reached = k < mine
        new = combine(
            before, jax.tree.map(lambda part, own: part[k].astype(own.dtype), everything, array)
        )
        return jax.tree.map(lambda a, b: jnp.where(reached, a, b), new, before)

    return lax.fori_loop(0, peers, hop, start)


def passed_along(block, axis, distance):
    devices = range(lax.axis_size(axis))
    route = [(i - distance, i) for i in devices if i - distance in devices]
    return lax.ppermute(block, axis, route)


def rotate(values, positions):
    half_dim = values.shape[-1] // 2
    inverse = 1.0 / 10000.0 ** (jnp.arange(half_dim, dtype=jnp.float32) / half_dim)
    angles = positions.astype(jnp.float32)[:, None] * inverse[None, :]
    cosine = jnp.cos(angles)[:, None, :]
    sine_table = jnp.sin(angles)[:, None, :]
    front_half = values[..., :half_dim]
    back_half = values[..., half_dim:]
    return jnp.concatenate(
        [
            front_half * cosine - back_half * sine_table,
            front_half * sine_table + back_half * cosine,
        ],
        axis=-1,
    )


def block_step(memory_state, inputs):
    queries, key_matrix_rows, value_matrix_rows, log_rates = inputs
    length_here = log_rates.shape[-1]
    causal = jnp.arange(length_here)[:, None] >= jnp.arange(length_here)[None, :]
    running_totals = jnp.cumsum(log_rates, axis=-1)
    relative = running_totals[:, :, None] - running_totals[:, None, :]
    weight = jnp.where(causal[None], jnp.exp(jnp.where(causal[None], relative, 0.0)), 0.0)
    score_matrix = (
        jnp.einsum("hqd,hkd->hqk", queries, key_matrix_rows, precision=exact_result) * weight
    )
    carried_state = jnp.einsum(
        "hqd,hdv->hqv",
        queries * jnp.exp(running_totals)[:, :, None],
        memory_state,
        precision=exact_result,
    )
    output_rows = (
        jnp.einsum("arf,afu->aru", score_matrix, value_matrix_rows, precision=exact_result)
        + carried_state
    )
    decay_factors = jnp.exp(running_totals[:, -1:] - running_totals)
    memory_state = memory_state * jnp.exp(running_totals[:, -1])[:, None, None] + jnp.einsum(
        "iwj,iwe->ije",
        key_matrix_rows * decay_factors[:, :, None],
        value_matrix_rows,
        precision=exact_result,
    )
    return (memory_state, output_rows)


def chain(earlier, later):
    return (earlier[0] * later[0], earlier[1] * later[0][:, None, None] + later[1])


def shards(
    tokens,
    norm_gain,
    ret_query,
    ret_key,
    ret_value,
    att_query,
    att_key,
    att_value,
    log_decay,
    start_state,
    ret_gain,
    sink_logits,
    ret_out,
    att_out,
):
    gathered = lax.all_gather(tokens[0], "tp", axis=1, tiled=True)
    row_count = gathered.shape[0]
    as_float = gathered.astype(jnp.float32)
    normed = (
        as_float
        * lax.rsqrt(jnp.mean(as_float * as_float, axis=-1, keepdims=True) + epsilon)
        * norm_gain
    ).astype(jnp.bfloat16)
    offset = lax.axis_index("sp") * row_count
    positions = offset + jnp.arange(row_count, dtype=jnp.int32)
    weights = (ret_query, ret_key, ret_value, att_query, att_key, att_value)
    pieces = (
        lax.all_gather(weights[0], "sp", axis=0, tiled=True),
        lax.all_gather(weights[1], "sp", axis=0, tiled=True),
        lax.all_gather(weights[2], "sp", axis=0, tiled=True),
        lax.all_gather(weights[3], "sp", axis=0, tiled=True),
        lax.all_gather(weights[4], "sp", axis=0, tiled=True),
        lax.all_gather(weights[5], "sp", axis=0, tiled=True),
    )
    projected = tuple(
        (jnp.dot(normed, piece, preferred_element_type=jnp.float32) for piece in pieces)
    )
    rounded = tuple((product_f.astype(jnp.bfloat16) for product_f in projected))
    projected = rounded[:3]
    head_count = projected[0].shape[1] // DK
    queries = rotate(projected[0].astype(jnp.float32).reshape(row_count, head_count, DK), positions)
    keys_rot = rotate(
        projected[1].astype(jnp.float32).reshape(row_count, head_count, DK), positions
    ) * DK ** (-0.5)
    values_f = projected[2].astype(jnp.float32).reshape(row_count, head_count, DV)
    log_rates = log_decay[0]
    count = row_count // BLOCK

    def blocked(array):
        return array.reshape(count, BLOCK, head_count, array.shape[-1]).transpose(0, 2, 1, 3)

    rates_blocked = log_rates.reshape(head_count, count, BLOCK).transpose(1, 0, 2)
    local_state, pieces = lax.scan(
        block_step,
        jnp.zeros((head_count, DK, DV), jnp.float32),
        (blocked(queries), blocked(keys_rot), blocked(values_f), rates_blocked),
    )
    local_out = pieces.transpose(0, 2, 1, 3).reshape(row_count, head_count, DV)
    running_totals = jnp.cumsum(log_rates, axis=-1)
    device_decay = jnp.exp(running_totals[:, -1])
    identity = (jnp.ones((head_count,), jnp.float32), jnp.zeros((head_count, DK, DV), jnp.float32))
    prior_decay, prior_state = carried_in((device_decay, local_state), "sp", chain, identity)
    incoming = prior_state + prior_decay[:, None, None] * start_state[0]
    retained = local_out + jnp.einsum(
        "thd,hdv->thv",
        queries * jnp.exp(running_totals).T[:, :, None],
        incoming,
        precision=exact_result,
    )
    centred = retained - jnp.mean(retained, axis=-1, keepdims=True)
    variance = jnp.mean(centred * centred, axis=-1, keepdims=True)
    ret_hidden = (
        (centred * lax.rsqrt(variance + epsilon)).reshape(row_count, head_count * DV) * ret_gain
    ).astype(jnp.bfloat16)
    att_queries, att_keys, att_values = rounded[3:]
    kv_heads = att_keys.shape[1] // HD
    groups = att_queries.shape[1] // HD // kv_heads
    earlier_keys, earlier_values = passed_along(
        (att_keys[row_count - WINDOW :], att_values[row_count - WINDOW :]), "sp", 1
    )
    extended_keys = jnp.concatenate([earlier_keys, att_keys], axis=0)
    extended_values = jnp.concatenate([earlier_values, att_values], axis=0)
    windows = row_count // WINDOW

    def banded(array):
        earlier = array[:row_count].reshape(windows, WINDOW, kv_heads, HD)
        current = array[WINDOW:].reshape(windows, WINDOW, kv_heads, HD)
        return jnp.concatenate([earlier, current], axis=1)

    key_band = banded(extended_keys)
    value_band = banded(extended_values)
    grouped_q = att_queries.reshape(windows, WINDOW, kv_heads, groups, HD)
    score_matrix = jnp.einsum(
        "nqhgd,nkhd->nhgqk", grouped_q, key_band, preferred_element_type=jnp.float32
    ) * HD ** (-0.5)
    query_index = WINDOW + jnp.arange(WINDOW)
    key_index = jnp.arange(2 * WINDOW)
    allowed = (key_index[None, :] <= query_index[:, None]) & (
        query_index[:, None] - key_index[None, :] < WINDOW
    )
    key_place = offset - WINDOW + jnp.arange(windows)[:, None] * WINDOW + key_index[None, :]
    visible = (allowed[None] & (key_place >= 0)[:, None, :])[:, None, None]
    expo = jnp.exp(jnp.where(visible, score_matrix, -1e30))
    summed = jnp.sum(expo, axis=-1, keepdims=True) + jnp.exp(sink_logits).reshape(
        1, kv_heads, groups, 1, 1
    )
    probs = (expo / summed).astype(jnp.bfloat16)
    attended = jnp.einsum(
        "nhgqk,nkhd->nqhgd", probs, value_band, preferred_element_type=jnp.float32
    )
    att_hidden = attended.astype(jnp.bfloat16).reshape(row_count, kv_heads * groups * HD)
    ret_width = ret_hidden.shape[1]
    joined = jnp.concatenate([ret_hidden, att_hidden], axis=1)[None]
    piece = lax.all_gather(joined, "fs", axis=0, tiled=True)
    product = jnp.einsum(
        "srh,hd->srd", piece[:, :, :ret_width], ret_out, preferred_element_type=jnp.float32
    )
    product = product + jnp.einsum(
        "srh,hd->srd", piece[:, :, ret_width:], att_out, preferred_element_type=jnp.float32
    )
    partial_rows = product.astype(jnp.bfloat16)
    regrouped = lax.all_to_all(partial_rows, "fs", split_axis=0, concat_axis=2, tiled=True)
    mixed = lax.psum_scatter(
        regrouped[0].astype(jnp.float32).astype(jnp.bfloat16), "tp", scatter_dimension=1, tiled=True
    )
    return mixed[None]


MESH = pl.DeviceIdType.MESH
F32 = jnp.float32
BF16 = jnp.bfloat16
GAIN_ROW = 0
DECAY_ROW = 1
SINK_ROW = 2
K_AT, V_AT, KV_AT, Q_AT, A_AT = 0, 256, 512, 640, 896


def dot(a, b):
    return jnp.dot(a, b, preferred_element_type=F32)


def dot_t(a, b):
    return lax.dot_general(a, b, (((1,), (1,)), ((), ())), preferred_element_type=F32)


def dot_l(a, b):
    return lax.dot_general(a, b, (((0,), (0,)), ((), ())), preferred_element_type=F32)


def fused(
    tok_in, ngain_in, rq, rk, rv, aq, ak, av, gain_in, decay_in, sink_in, start, ro, ao, cos_in, sin_in, out,
    ngain, gain_v, decay_v, sink_v, ak_v, av_v, cos, sin, insem,
    small, sm, traw, xn, akp, w, wo, s0, local_state, sbuf, states, kbuf, vbuf, qbuf, kvp, inner, hid, hin,
    total, ob, fade, since, until,
    send, smsem, tsem, ownsem, zsem, ysem, psem, wosem, ssem, stsem, halosem, hsem, outsem,
):
    z, f, c = lax.axis_index("sp"), lax.axis_index("fs"), lax.axis_index("tp")
    y, x = f // 2, lax.rem(f, 2)
    zh, zb = z // 2, lax.rem(z, 2)
    peer = 1 - c
    fx, fy = 2 * y + 1 - x, 2 * (1 - y) + x
    zp, z2, z3 = z + 1 - 2 * zb, lax.rem(z + 2, 4), 3 - z
    head = 2 * zb + x
    rows, half = tok_in.shape
    depth = rq.shape[0]
    part = depth // 4
    mid = jnp.logical_or(z == 1, z == 2)
    near, far = jnp.where(mid, z3, z2), jnp.where(mid, z2, z3)
    order = (zp, near, far)
    first, second = zh == 0, zh == 1

    loads = [
        (ngain_in, ngain), (gain_in, gain_v), (decay_in, decay_v), (sink_in, sink_v), (ak, ak_v), (av, av_v),
        (cos_in.at[pl.ds(pl.multiple_of(zh * 2 * rows, 2 * rows), 2 * rows)], cos),
        (sin_in.at[pl.ds(pl.multiple_of(zh * 2 * rows, 2 * rows), 2 * rows)], sin),
    ]
    inputs = [pltpu.make_async_copy(src, dst, insem.at[i]) for i, (src, dst) in enumerate(loads)]
    for copy in inputs:
        copy.start()

    barrier = pltpu.get_barrier_semaphore()
    greeted = [{"tp": peer}, {"fs": fy}]
    for t in range(2):
        core = jnp.int32(t)
        greeted += [{"sp": zs, "tp": core} for zs in order]
        greeted += [{"fs": fx, "tp": core}, {"sp": zp, "fs": fx, "tp": core}]
    for where in greeted:
        pl.semaphore_signal(barrier, inc=1, device_id=where, device_id_type=MESH)
    pl.semaphore_wait(barrier, len(greeted))

    sent = []
    slots = iter(range(send.shape[0]))

    def both(a, b):
        if a is None:
            return b
        return a if b is None else jnp.logical_and(a, b)

    def remote(cond, src, dst, rsem, **where):
        copy = pltpu.make_async_remote_copy(
            src_ref=src, dst_ref=dst, send_sem=send.at[next(slots)], recv_sem=rsem,
            device_id=where, device_id_type=MESH,
        )
        sent.append((cond, copy))
        if cond is None:
            copy.start()
        else:
            pl.when(cond)(copy.start)
        return copy

    def local(cond, src, dst, sem):
        copy = pltpu.make_async_copy(src, dst, sem)
        if cond is None:
            copy.start()
        else:
            pl.when(cond)(copy.start)

    def arrived(dst, sem):
        pltpu.make_async_copy(dst, dst, sem).wait()

    mine = traw.at[zb, c]
    local(c == x, tok_in, mine, tsem.at[zb, c])
    remote(c != x, tok_in, mine, tsem.at[zb, c], tp=peer)
    ahead = remote(None, tok_in, mine, tsem.at[zb, c], sp=zp, tp=x)
    remote(None, tok_in, mine, tsem.at[zb, c], fs=fx, tp=x)

    pieces = ((K_AT, DK), (V_AT, DV), (KV_AT, 128), (A_AT, DK), (Q_AT, DK))
    sources = (rk, rv, akp, aq, rq)
    whole = (4,)

    def rows_of(zs, ys, cs):
        return pl.ds(pl.multiple_of(zs * depth + ys * 2 * part + cs * part, part), part)

    def rows_whole(zs, cs):
        return pl.ds(pl.multiple_of(zs * depth + cs * 2 * part, 2 * part), 2 * part)

    def weight(p):
        a, (at, width) = sources[p], pieces[p]
        return a, pl.ds(0, width) if a is akp else pl.ds(pl.multiple_of(x * DK, DK), width), pl.ds(at, width)

    def send_weights(p, cond, to):
        a, cols, at = weight(p)
        for t in range(2):
            if p in whole:
                src = a.at[pl.ds(t * 2 * part, 2 * part), cols]
                dst = w.at[rows_whole(z, t), at]
            else:
                src = a.at[pl.ds(pl.multiple_of(y * 2 * part + t * part, part), part), cols]
                dst = w.at[rows_of(z, y, t), at]
            remote(cond, src, dst, zsem.at[p, z], sp=to, tp=jnp.int32(t))

    def keep_weights(p):
        a, cols, at = weight(p)
        dst = w.at[pl.ds(pl.multiple_of(z * depth, depth), depth), at]
        local(c == zb, a.at[:, cols], dst, ownsem.at[p])
        remote(c == zb, a.at[:, cols], dst, ownsem.at[p], tp=peer)

    to_a = jnp.where(zb == c, z2, zp)
    early = jnp.logical_and(zb != c, mid)
    late = jnp.logical_and(zb != c, jnp.logical_not(mid))
    for p in (0, 1, 3, 4):
        send_weights(p, early, z3)
    for p in (0, 1, 3, 4):
        keep_weights(p)

    out_rows, out_cols = ro.shape

    shares = ((0, 0, out_rows), (1, 0, out_rows // 2), (1, out_rows // 2, out_rows // 2))

    def out_block(share, ys, cs):
        kind, at, n = shares[share]
        rows_at = pl.ds(pl.multiple_of(cs * out_rows + at, n), n)
        return wo.at[kind, ys, rows_at], wosem.at[share, ys, cs]

    def send_out(share):
        kind, at, n = shares[share]
        a = (ro, ao)[kind].at[pl.ds(at, n)]
        block, sem = out_block(share, y, c)
        remote(None, a, block, sem, fs=fy)
        remote(None, a, block, sem, tp=peer)
        local(None, a, block, sem)

    def pass_out(share):
        block, sem = out_block(share, 1 - y, c)
        arrived(block, sem)
        remote(None, block, block, sem, tp=peer)

    def wait_out(kind):
        for share in ((0,), (1, 2))[kind]:
            for ys, cs in ((y, c), (y, peer), (1 - y, peer)):
                arrived(*out_block(share, ys, cs))

    send_out(0)
    send_out(1)

    for i in (1, 2, 3):
        inputs[i].wait()
    small[...] = jnp.zeros_like(small)
    small[pl.ds(GAIN_ROW, 1), :] = gain_v[...]
    for j in range(2):
        small[pl.ds(DECAY_ROW, 1), pl.ds(j * rows, rows)] = decay_v[pl.ds(j, 1), :]
    small[pl.ds(SINK_ROW, 1), pl.ds(0, sink_v.shape[1])] = sink_v[...]
    inputs[4].wait()
    inputs[5].wait()
    packed = [
        jnp.concatenate([ak_v[:, j * HD : (j + 1) * HD], av_v[:, j * HD : (j + 1) * HD]], axis=1) for j in range(2)
    ]
    akp[...] = jnp.where(x == 0, packed[0], packed[1])

    send_weights(2, early, z3)
    keep_weights(2)
    here = jnp.logical_and(zb == c, c == x)
    to_square = 2 * zh + c
    local(here, small, sm.at[zb], smsem.at[zb])
    remote(jnp.logical_not(here), small, sm.at[zb], smsem.at[zb], sp=to_square, tp=x)
    remote(None, small, sm.at[zb], smsem.at[zb], sp=to_square, fs=fx, tp=x)
    gives = jnp.logical_and(first, zb == c)
    local(both(gives, c == x), start.at[x], s0, ssem)
    remote(both(gives, c != x), start.at[x], s0, ssem, tp=peer)

    ahead.wait_send()
    for p in (2, 0, 1, 3, 4):
        send_weights(p, None, to_a)
        send_weights(p, late, z3)

    for t in range(2):
        block = traw.at[1 - zb, t]

        @pl.when(c == x)
        def _():
            arrived(block, tsem.at[1 - zb, t])

        remote(c == x, block, block, tsem.at[1 - zb, t], fs=fx)

    remote(gives, start.at[1 - x], s0, ssem, fs=fx, tp=x)

    def take(p):
        at, width = pieces[p]
        cols = pl.ds(at, width)
        for zs in order:
            block = w.at[rows_whole(zs, c) if p in whole else rows_of(zs, y, c), cols]
            arrived(block, zsem.at[p, zs])
            if p not in whole:
                remote(None, block, block, ysem.at[p, zs], fs=fy)
            remote(None, block, block, psem.at[p], tp=peer)

    def spread(p):
        at, width = pieces[p]
        cols = pl.ds(at, width)
        for zs in order:
            block = w.at[rows_of(zs, 1 - y, c), cols]
            arrived(block, ysem.at[p, zs])
            remote(None, block, block, psem.at[p], tp=peer)

    def complete(p):
        at, width = pieces[p]
        cols = pl.ds(at, width)
        arrived(w.at[pl.ds(0, depth), cols], ownsem.at[p])
        arrived(w.at[pl.ds(0, 6 * part), cols], psem.at[p])

    inputs[0].wait()

    def normalize(b):
        @pl.loop(0, rows // 32)
        def _(i):
            at = pl.ds(pl.multiple_of(i * 32, 32), 32)
            to = pl.ds(pl.multiple_of(b * rows + i * 32, 32), 32)
            h0, h1 = traw[b, 0, at, :].astype(F32), traw[b, 1, at, :].astype(F32)
            squares = jnp.sum(h0 * h0, axis=-1, keepdims=True) + jnp.sum(h1 * h1, axis=-1, keepdims=True)
            scale = lax.rsqrt(squares / (2 * half) + epsilon)
            xn[to, pl.ds(0, half)] = (h0 * scale * ngain[:, pl.ds(0, half)]).astype(BF16)
            xn[to, pl.ds(half, half)] = (h1 * scale * ngain[:, pl.ds(half, half)]).astype(BF16)

    def token_wait(b):
        for t in range(2):
            block, sem = traw.at[b, t], tsem.at[b, t]
            if b is other:
                pl.when(c != x)(functools.partial(arrived, block, sem))
            else:
                arrived(block, sem)

    own, other = zb, 1 - zb
    token_wait(own)
    normalize(own)
    pl.when(c == x)(functools.partial(normalize, other))
    for b in range(2):
        arrived(sm.at[b], smsem.at[b])
    lane = lax.broadcasted_iota(jnp.int32, (rows, rows), 1)
    row = lax.broadcasted_iota(jnp.int32, (rows, rows), 0)

    def rates(b):
        return sm[b, pl.ds(DECAY_ROW, 1), pl.ds(pl.multiple_of(x * rows, rows), rows)]

    @pl.loop(0, 2)
    def _(b):
        at = pl.ds(pl.multiple_of(b * rows, rows), rows)
        l = rates(b)
        cum = jnp.sum(jnp.where(lane <= row, l, 0.0), axis=1, keepdims=True)
        cum_row = jnp.sum(jnp.where(lane == row, cum, 0.0), axis=0, keepdims=True)
        fade[b] = jnp.where(lane <= row, jnp.exp(jnp.where(lane <= row, cum - cum_row, 0.0)), 0.0)
        since[at, :] = jnp.exp(cum)
        until[at, :] = jnp.exp(jnp.sum(l, axis=1, keepdims=True) - cum)

    pass_out(0)
    take(2)
    take(0)
    spread(2)
    take(1)
    pass_out(1)
    spread(0)
    spread(1)
    take(3)
    send_out(2)
    token_wait(other)
    pl.when(c != x)(functools.partial(normalize, other))
    inputs[6].wait()
    inputs[7].wait()
    complete(2)

    def block_at(b):
        return pl.ds(pl.multiple_of(b * rows, rows), rows)

    def tile(b, at, width):
        return dot(xn[block_at(b), :], w[:, pl.ds(at, width)])

    h = DK // 2

    def turn(a, b, factor):
        co, si = cos[block_at(b), :], sin[block_at(b), :]
        lo, hi = a[:, :h], a[:, h:]
        return jnp.concatenate([(lo * co - hi * si) * factor, (lo * si + hi * co) * factor], axis=1).astype(BF16)

    @pl.when(first)
    def _():
        kvp[pl.ds(0, WINDOW), :] = jnp.zeros((WINDOW, kvp.shape[1]), BF16)

    @pl.loop(0, 2)
    def _(b):
        to = pl.ds(pl.multiple_of(WINDOW + b * rows, WINDOW), rows)
        kvp[to, :] = tile(b, KV_AT, 128).astype(BF16)

    remote(first, kvp.at[pl.ds(2 * rows, WINDOW)], kvp.at[pl.ds(0, WINDOW)], halosem, sp=z2)
    complete(0)
    complete(1)
    @pl.loop(0, 2)
    def _(b):
        at = block_at(b)
        k = turn(tile(b, K_AT, DK).astype(BF16).astype(F32), b, DK ** (-0.5))
        kbuf[at, :] = k
        v = tile(b, V_AT, DV).astype(BF16)
        vbuf[at, :] = v
        kd = (k.astype(F32) * until[at, :]).astype(BF16)
        local_state[b] = dot_l(kd, v)

    def decay_of(b):
        return jnp.exp(jnp.sum(rates(b), axis=1, keepdims=True))

    @pl.when(first)
    def _():
        arrived(s0, ssem)
        states[0] = s0[...].astype(BF16)
        after = s0[...] * decay_of(0) + local_state[0]
        states[1] = after.astype(BF16)
        sbuf[...] = (after * decay_of(1) + local_state[1]).astype(BF16)

    remote(first, sbuf, states.at[0], stsem, sp=z2)

    def hand_on(kind, b, away=None, part_at=None):
        at = pl.ds(0, rows) if part_at is None else pl.ds(part_at * (rows // 2), rows // 2)
        sem = hsem.at[2 if kind else part_at, head]
        src, dst = hid.at[kind, b, at], hin.at[kind, head, at]
        leaves, stays = (zb != b, zb == b) if away is None else (None, None)
        if away is not False:
            remote(leaves, src, dst, sem, sp=zp)
            remote(leaves, src, dst, sem, sp=zp, fs=fx)
        if away is not True:
            remote(stays, src, dst, sem, fs=fx)
            local(stays, src, dst, sem)

    lane2 = lax.broadcasted_iota(jnp.int32, (WINDOW, 2 * WINDOW), 1)
    row2 = lax.broadcasted_iota(jnp.int32, (WINDOW, 2 * WINDOW), 0)
    per = rows // WINDOW
    groups = DK // HD
    sink_row = sm[0, pl.ds(SINK_ROW, 1), pl.ds(0, 128)]
    sink_lane = lax.broadcasted_iota(jnp.int32, (1, 128), 1)
    sinks = [
        jnp.exp(jnp.sum(jnp.where(sink_lane == x * groups + i, sink_row, 0.0), axis=1, keepdims=True))
        for i in range(groups)
    ]

    def attention(b, away):
        aqs = tile(b, A_AT, DK).astype(BF16)
        seen = (lane2 <= row2 + WINDOW) & (lane2 > row2)
        scores, bands = [], []
        for i in range(per):
            n = b * per + i
            band = kvp[pl.ds(pl.multiple_of(n * WINDOW, WINDOW), 2 * WINDOW), :]
            bands.append(band[:, HD:])
            q = aqs[i * WINDOW : (i + 1) * WINDOW]
            stacked = jnp.concatenate([q[:, g * HD : (g + 1) * HD] for g in range(groups)], axis=0)
            scores.append(dot_t(stacked, band[:, :HD]))
        weights = []
        for i in range(per):
            visible = seen & (lane2 + (b * per + i) * WINDOW + zh * 2 * rows >= WINDOW)
            probs = []
            for g in range(groups):
                part_score = scores[i][g * WINDOW : (g + 1) * WINDOW] * HD ** (-0.5)
                e = jnp.exp(jnp.where(visible, part_score, -1e30))
                probs.append((e * (1.0 / (jnp.sum(e, axis=-1, keepdims=True) + sinks[g]))).astype(BF16))
            weights.append(jnp.concatenate(probs, axis=0))
        for i in range(per):
            res = dot(weights[i], bands[i])
            heads_out = [res[g * WINDOW : (g + 1) * WINDOW] for g in range(groups)]
            hid[1, b, pl.ds(i * WINDOW, WINDOW), :] = jnp.concatenate(heads_out, axis=1).astype(BF16)
        hand_on(1, b, away)

    spread(3)
    complete(3)
    pl.when(second)(functools.partial(arrived, kvp.at[pl.ds(0, WINDOW)], halosem))
    attention(other, True)
    take(4)
    attention(own, False)
    complete(4)

    @pl.loop(0, 2)
    def _(b):
        at = block_at(b)
        q = turn(tile(b, Q_AT, DK).astype(BF16).astype(F32), b, 1.0)
        qbuf[at, :] = (q.astype(F32) * since[at, :]).astype(BF16)
        scores = (dot_t(q, kbuf[at, :]) * fade[b]).astype(BF16)
        inner[at, :] = dot(scores, vbuf[at, :])

    @pl.when(second)
    def _():
        arrived(states.at[0], stsem)
        states[1] = (states[0].astype(F32) * decay_of(0) + local_state[0]).astype(BF16)

    gain_at = pl.ds(pl.multiple_of(x * DV, DV), DV)
    for b in (other, own):
        at = block_at(b)
        o = inner[at, :] + dot(qbuf[at, :], states[b])
        centred = o - jnp.mean(o, axis=-1, keepdims=True)
        var = jnp.mean(centred * centred, axis=-1, keepdims=True)
        hid[0, b] = (centred * lax.rsqrt(var + epsilon) * sm[0, pl.ds(GAIN_ROW, 1), gain_at]).astype(BF16)

    for part_at in range(2):
        hand_on(0, other, True, part_at)
        hand_on(0, own, False, part_at)

    pass_out(2)
    others = (2 * zb + 1 - x, 2 * (1 - zb) + x, 2 * (1 - zb) + 1 - x)
    home = c == x

    def mixed_tile(kind, at, t):
        cols = pl.ds(t % 2 * 256, 256)
        acc = None
        for n in range(4):
            term = dot(hin[kind, n, at, :], wo[kind, t // 2, pl.ds(n * DV, DV), cols])
            acc = term if acc is None else acc + term
        return acc

    for n in (head,) + others:
        arrived(hin.at[1, n], hsem.at[2, n])
    wait_out(1)
    wait_out(0)
    for t in range(4):
        total[:, pl.ds(t * 256, 256)] = mixed_tile(1, pl.ds(0, rows), t)

    def finish(part_at):
        at = pl.ds(part_at * (rows // 2), rows // 2)
        for t in range(4):
            ob[t, at, :] = (total[at, pl.ds(t * 256, 256)] + mixed_tile(0, at, t)).astype(BF16)
            src = ob.at[t, at]
            dst = out.at[at, pl.ds(pl.multiple_of(x * out_cols + t % 2 * 256, 256), 256)]
            local(both(home, c == t // 2), src, dst, outsem)
            remote(both(home, c != t // 2), src, dst, outsem, tp=peer)
            remote(jnp.logical_not(home), src, dst, outsem, fs=fx, tp=jnp.int32(t // 2))

    def wait_ret(part_at):
        at = pl.ds(part_at * (rows // 2), rows // 2)
        for n in (head,) + others:
            arrived(hin.at[0, n, at], hsem.at[part_at, n])

    wait_ret(0)
    finish(0)
    wait_ret(1)
    finish(1)

    arrived(out, outsem)
    for cond, copy in sent:
        if copy is ahead:
            continue
        if cond is None:
            copy.wait_send()
        else:
            pl.when(cond)(copy.wait_send)


def layer(mesh, *args):
    (tokens, norm_gain, ret_query, ret_key, ret_value, att_query, att_key, att_value,
     log_decay, start_state, ret_gain, sink_logits, ret_out, att_out) = args
    n_sp, n_fs, n_tp = mesh.shape["sp"], mesh.shape["fs"], mesh.shape["tp"]
    heads = ret_query.shape[1] // DK
    kv_heads = att_key.shape[1] // HD
    rows, half = tokens.shape[1:]
    depth = ret_query.shape[0]
    square = (
        n_tp == 2 and n_fs == 4 and n_sp == 4 and heads == 2 and kv_heads == 2
        and att_query.shape[1] == ret_query.shape[1] and rows == DK and tokens.shape[0] == 1
        and 2 * half == n_sp * depth and ret_out.shape == att_out.shape
        and ret_out.shape == (heads * DV, half // 2) and half == 4 * DK
    )
    if not square:
        return shards(*args)
    h = DK // 2
    length = n_sp * rows
    inverse = np.float32(1.0) / np.float32(10000.0) ** (np.arange(h, dtype=np.float32) / np.float32(h))
    angles = np.arange(length, dtype=np.float32)[:, None] * inverse[None, :]
    cos = jnp.asarray(np.cos(angles), F32)
    sin = jnp.asarray(np.sin(angles), F32)
    wide = heads * rows
    hbm = pl.BlockSpec(memory_space=pl.ANY)
    dma = pltpu.SemaphoreType.DMA
    v = pltpu.VMEM
    res = pl.pallas_call(
        fused,
        out_shape=jax.ShapeDtypeStruct((rows, half), BF16),
        in_specs=[hbm] * 16,
        out_specs=hbm,
        scratch_shapes=[
            v((1, norm_gain.shape[0]), F32),
            v((1, ret_gain.shape[0]), F32),
            v((heads, rows), F32),
            v((1, sink_logits.shape[0]), F32),
            v(att_key.shape, BF16),
            v(att_value.shape, BF16),
            v((2 * rows, h), F32),
            v((2 * rows, h), F32),
            dma((8,)),
            v((8, wide), F32),
            v((2, 8, wide), F32),
            v((2, 2, rows, half), BF16),
            v((2 * rows, 2 * half), BF16),
            v((depth, 128), BF16),
            v((n_sp * depth, A_AT + DK), BF16),
            v((2, 2, 2 * ret_out.shape[0], ret_out.shape[1]), BF16),
            v((DK, DV), F32),
            v((2, DK, DV), F32),
            v((DK, DV), BF16),
            v((2, DK, DV), BF16),
            v((2 * rows, DK), BF16),
            v((2 * rows, DV), BF16),
            v((2 * rows, DK), BF16),
            v((WINDOW + 2 * rows, 128), BF16),
            v((2 * rows, DV), F32),
            v((2, 2, rows, DV), BF16),
            v((2, 4, rows, DV), BF16),
            v((rows, half), F32),
            v((4, rows, 256), BF16),
            v((2, rows, rows), F32),
            v((2 * rows, 1), F32),
            v((2 * rows, 1), F32),
            dma((160,)),
            dma((2,)),
            dma((2, 2)),
            dma((5,)),
            dma((5, n_sp)),
            dma((5, n_sp)),
            dma((5,)),
            dma((3, 2, 2)),
            dma,
            dma,
            dma,
            dma((3, 4)),
            dma,
        ],
        compiler_params=pltpu.CompilerParams(
            collective_id=0, has_side_effects=True, vmem_limit_bytes=67043328
        ),
    )(
        tokens[0], norm_gain[None], ret_query, ret_key, ret_value, att_query, att_key, att_value,
        ret_gain[None], log_decay[0], sink_logits[None], start_state[0], ret_out, att_out, cos, sin,
    )
    return res[None]


def solution(mesh):
    placed = (
        P("fs", "sp", "tp"),
        P(),
        P("sp", "tp"),
        P("sp", "tp"),
        P("sp", "tp"),
        P("sp", "tp"),
        P("sp", "tp"),
        P("sp", "tp"),
        P("fs", "tp", "sp"),
        P("fs", "tp", None, None),
        P("tp"),
        P("tp"),
        P("tp", "fs"),
        P("tp", "fs"),
    )
    return jax.shard_map(
        functools.partial(layer, mesh), mesh=mesh, in_specs=placed, out_specs=P("fs", "sp", "tp"), check_vma=False
    )
```

```python
import functools

import jax
import jax.numpy as jnp
import numpy as np
from jax import lax
from jax.experimental import pallas as pl
from jax.experimental.pallas import tpu as pltpu
from jax.sharding import PartitionSpec as P

DK = 256
DV = 256
HD = 64
WINDOW = 128
BLOCK = 128


epsilon = 1e-06
exact_result = lax.Precision.HIGHEST


def carried_in(array, axis, combine, identity):
    peers, mine = (lax.axis_size(axis), lax.axis_index(axis))
    everything = jax.tree.map(
        lambda part, kind: lax.all_gather(part.astype(kind), axis),
        array,
        (jnp.bfloat16, jnp.bfloat16),
    )
    start = jax.tree.map(
        lambda part, zero: jnp.broadcast_to(jnp.asarray(zero, part.dtype), part.shape),
        array,
        identity,
    )

    def hop(k, before):
        reached = k < mine
        new = combine(
            before, jax.tree.map(lambda part, own: part[k].astype(own.dtype), everything, array)
        )
        return jax.tree.map(lambda a, b: jnp.where(reached, a, b), new, before)

    return lax.fori_loop(0, peers, hop, start)


def passed_along(block, axis, distance):
    devices = range(lax.axis_size(axis))
    route = [(i - distance, i) for i in devices if i - distance in devices]
    return lax.ppermute(block, axis, route)


def rotate(values, positions):
    half_dim = values.shape[-1] // 2
    inverse = 1.0 / 10000.0 ** (jnp.arange(half_dim, dtype=jnp.float32) / half_dim)
    angles = positions.astype(jnp.float32)[:, None] * inverse[None, :]
    cosine = jnp.cos(angles)[:, None, :]
    sine_table = jnp.sin(angles)[:, None, :]
    front_half = values[..., :half_dim]
    back_half = values[..., half_dim:]
    return jnp.concatenate(
        [
            front_half * cosine - back_half * sine_table,
            front_half * sine_table + back_half * cosine,
        ],
        axis=-1,
    )


def block_step(memory_state, inputs):
    queries, key_matrix_rows, value_matrix_rows, log_rates = inputs
    length_here = log_rates.shape[-1]
    causal = jnp.arange(length_here)[:, None] >= jnp.arange(length_here)[None, :]
    running_totals = jnp.cumsum(log_rates, axis=-1)
    relative = running_totals[:, :, None] - running_totals[:, None, :]
    weight = jnp.where(causal[None], jnp.exp(jnp.where(causal[None], relative, 0.0)), 0.0)
    score_matrix = (
        jnp.einsum("hqd,hkd->hqk", queries, key_matrix_rows, precision=exact_result) * weight
    )
    carried_state = jnp.einsum(
        "hqd,hdv->hqv",
        queries * jnp.exp(running_totals)[:, :, None],
        memory_state,
        precision=exact_result,
    )
    output_rows = (
        jnp.einsum("arf,afu->aru", score_matrix, value_matrix_rows, precision=exact_result)
        + carried_state
    )
    decay_factors = jnp.exp(running_totals[:, -1:] - running_totals)
    memory_state = memory_state * jnp.exp(running_totals[:, -1])[:, None, None] + jnp.einsum(
        "iwj,iwe->ije",
        key_matrix_rows * decay_factors[:, :, None],
        value_matrix_rows,
        precision=exact_result,
    )
    return (memory_state, output_rows)


def chain(earlier, later):
    return (earlier[0] * later[0], earlier[1] * later[0][:, None, None] + later[1])


def shards(
    tokens,
    norm_gain,
    ret_query,
    ret_key,
    ret_value,
    att_query,
    att_key,
    att_value,
    log_decay,
    start_state,
    ret_gain,
    sink_logits,
    ret_out,
    att_out,
):
    gathered = lax.all_gather(tokens[0], "tp", axis=1, tiled=True)
    row_count = gathered.shape[0]
    as_float = gathered.astype(jnp.float32)
    normed = (
        as_float
        * lax.rsqrt(jnp.mean(as_float * as_float, axis=-1, keepdims=True) + epsilon)
        * norm_gain
    ).astype(jnp.bfloat16)
    offset = lax.axis_index("sp") * row_count
    positions = offset + jnp.arange(row_count, dtype=jnp.int32)
    weights = (ret_query, ret_key, ret_value, att_query, att_key, att_value)
    pieces = (
        lax.all_gather(weights[0], "sp", axis=0, tiled=True),
        lax.all_gather(weights[1], "sp", axis=0, tiled=True),
        lax.all_gather(weights[2], "sp", axis=0, tiled=True),
        lax.all_gather(weights[3], "sp", axis=0, tiled=True),
        lax.all_gather(weights[4], "sp", axis=0, tiled=True),
        lax.all_gather(weights[5], "sp", axis=0, tiled=True),
    )
    projected = tuple(
        (jnp.dot(normed, piece, preferred_element_type=jnp.float32) for piece in pieces)
    )
    rounded = tuple((product_f.astype(jnp.bfloat16) for product_f in projected))
    projected = rounded[:3]
    head_count = projected[0].shape[1] // DK
    queries = rotate(projected[0].astype(jnp.float32).reshape(row_count, head_count, DK), positions)
    keys_rot = rotate(
        projected[1].astype(jnp.float32).reshape(row_count, head_count, DK), positions
    ) * DK ** (-0.5)
    values_f = projected[2].astype(jnp.float32).reshape(row_count, head_count, DV)
    log_rates = log_decay[0]
    count = row_count // BLOCK

    def blocked(array):
        return array.reshape(count, BLOCK, head_count, array.shape[-1]).transpose(0, 2, 1, 3)

    rates_blocked = log_rates.reshape(head_count, count, BLOCK).transpose(1, 0, 2)
    local_state, pieces = lax.scan(
        block_step,
        jnp.zeros((head_count, DK, DV), jnp.float32),
        (blocked(queries), blocked(keys_rot), blocked(values_f), rates_blocked),
    )
    local_out = pieces.transpose(0, 2, 1, 3).reshape(row_count, head_count, DV)
    running_totals = jnp.cumsum(log_rates, axis=-1)
    device_decay = jnp.exp(running_totals[:, -1])
    identity = (jnp.ones((head_count,), jnp.float32), jnp.zeros((head_count, DK, DV), jnp.float32))
    prior_decay, prior_state = carried_in((device_decay, local_state), "sp", chain, identity)
    incoming = prior_state + prior_decay[:, None, None] * start_state[0]
    retained = local_out + jnp.einsum(
        "thd,hdv->thv",
        queries * jnp.exp(running_totals).T[:, :, None],
        incoming,
        precision=exact_result,
    )
    centred = retained - jnp.mean(retained, axis=-1, keepdims=True)
    variance = jnp.mean(centred * centred, axis=-1, keepdims=True)
    ret_hidden = (
        (centred * lax.rsqrt(variance + epsilon)).reshape(row_count, head_count * DV) * ret_gain
    ).astype(jnp.bfloat16)
    att_queries, att_keys, att_values = rounded[3:]
    kv_heads = att_keys.shape[1] // HD
    groups = att_queries.shape[1] // HD // kv_heads
    earlier_keys, earlier_values = passed_along(
        (att_keys[row_count - WINDOW :], att_values[row_count - WINDOW :]), "sp", 1
    )
    extended_keys = jnp.concatenate([earlier_keys, att_keys], axis=0)
    extended_values = jnp.concatenate([earlier_values, att_values], axis=0)
    windows = row_count // WINDOW

    def banded(array):
        earlier = array[:row_count].reshape(windows, WINDOW, kv_heads, HD)
        current = array[WINDOW:].reshape(windows, WINDOW, kv_heads, HD)
        return jnp.concatenate([earlier, current], axis=1)

    key_band = banded(extended_keys)
    value_band = banded(extended_values)
    grouped_q = att_queries.reshape(windows, WINDOW, kv_heads, groups, HD)
    score_matrix = jnp.einsum(
        "nqhgd,nkhd->nhgqk", grouped_q, key_band, preferred_element_type=jnp.float32
    ) * HD ** (-0.5)
    query_index = WINDOW + jnp.arange(WINDOW)
    key_index = jnp.arange(2 * WINDOW)
    allowed = (key_index[None, :] <= query_index[:, None]) & (
        query_index[:, None] - key_index[None, :] < WINDOW
    )
    key_place = offset - WINDOW + jnp.arange(windows)[:, None] * WINDOW + key_index[None, :]
    visible = (allowed[None] & (key_place >= 0)[:, None, :])[:, None, None]
    expo = jnp.exp(jnp.where(visible, score_matrix, -1e30))
    summed = jnp.sum(expo, axis=-1, keepdims=True) + jnp.exp(sink_logits).reshape(
        1, kv_heads, groups, 1, 1
    )
    probs = (expo / summed).astype(jnp.bfloat16)
    attended = jnp.einsum(
        "nhgqk,nkhd->nqhgd", probs, value_band, preferred_element_type=jnp.float32
    )
    att_hidden = attended.astype(jnp.bfloat16).reshape(row_count, kv_heads * groups * HD)
    ret_width = ret_hidden.shape[1]
    joined = jnp.concatenate([ret_hidden, att_hidden], axis=1)[None]
    piece = lax.all_gather(joined, "fs", axis=0, tiled=True)
    product = jnp.einsum(
        "srh,hd->srd", piece[:, :, :ret_width], ret_out, preferred_element_type=jnp.float32
    )
    product = product + jnp.einsum(
        "srh,hd->srd", piece[:, :, ret_width:], att_out, preferred_element_type=jnp.float32
    )
    partial_rows = product.astype(jnp.bfloat16)
    regrouped = lax.all_to_all(partial_rows, "fs", split_axis=0, concat_axis=2, tiled=True)
    mixed = lax.psum_scatter(
        regrouped[0].astype(jnp.float32).astype(jnp.bfloat16), "tp", scatter_dimension=1, tiled=True
    )
    return mixed[None]


MESH = pl.DeviceIdType.MESH
F32 = jnp.float32
BF16 = jnp.bfloat16
GAIN_ROW = 0
DECAY_ROW = 1
SINK_ROW = 2
K_AT, V_AT, KV_AT, Q_AT, A_AT = 0, 256, 512, 640, 896


def dot(a, b):
    return jnp.dot(a, b, preferred_element_type=F32)


def dot_t(a, b):
    return lax.dot_general(a, b, (((1,), (1,)), ((), ())), preferred_element_type=F32)


def dot_l(a, b):
    return lax.dot_general(a, b, (((0,), (0,)), ((), ())), preferred_element_type=F32)


def fused(
    tok_in, ngain_in, rq, rk, rv, aq, ak, av, gain_in, decay_in, sink_in, start, ro, ao, cos_in, sin_in, out,
    ngain, gain_v, decay_v, sink_v, ak_v, av_v, cos, sin, insem,
    small, sm, traw, xn, akp, w, wo, s0, local_state, sbuf, states, kbuf, vbuf, qbuf, kvp, inner, hid, hin,
    total, ob, fade, since, until,
    send, smsem, tsem, ownsem, zsem, ysem, psem, wosem, ssem, stsem, halosem, hsem, outsem,
):
    z, f, c = lax.axis_index("sp"), lax.axis_index("fs"), lax.axis_index("tp")
    y, x = f // 2, lax.rem(f, 2)
    zh, zb = z // 2, lax.rem(z, 2)
    peer = 1 - c
    fx, fy = 2 * y + 1 - x, 2 * (1 - y) + x
    zp, z2, z3 = z + 1 - 2 * zb, lax.rem(z + 2, 4), 3 - z
    head = 2 * zb + x
    rows, half = tok_in.shape
    depth = rq.shape[0]
    part = depth // 4
    mid = jnp.logical_or(z == 1, z == 2)
    near, far = jnp.where(mid, z3, z2), jnp.where(mid, z2, z3)
    order = (zp, near, far)
    first, second = zh == 0, zh == 1

    loads = [
        (ngain_in, ngain), (gain_in, gain_v), (decay_in, decay_v), (sink_in, sink_v), (ak, ak_v), (av, av_v),
        (cos_in.at[pl.ds(pl.multiple_of(zh * 2 * rows, 2 * rows), 2 * rows)], cos),
        (sin_in.at[pl.ds(pl.multiple_of(zh * 2 * rows, 2 * rows), 2 * rows)], sin),
    ]
    inputs = [pltpu.make_async_copy(src, dst, insem.at[i]) for i, (src, dst) in enumerate(loads)]
    for copy in inputs:
        copy.start()

    barrier = pltpu.get_barrier_semaphore()
    greeted = [{"tp": peer}, {"fs": fy}]
    for t in range(2):
        core = jnp.int32(t)
        greeted += [{"sp": zs, "tp": core} for zs in order]
        greeted += [{"fs": fx, "tp": core}, {"sp": zp, "fs": fx, "tp": core}]
    for where in greeted:
        pl.semaphore_signal(barrier, inc=1, device_id=where, device_id_type=MESH)
    pl.semaphore_wait(barrier, len(greeted))

    sent = []
    slots = iter(range(send.shape[0]))

    def both(a, b):
        if a is None:
            return b
        return a if b is None else jnp.logical_and(a, b)

    def remote(cond, src, dst, rsem, **where):
        copy = pltpu.make_async_remote_copy(
            src_ref=src, dst_ref=dst, send_sem=send.at[next(slots)], recv_sem=rsem,
            device_id=where, device_id_type=MESH,
        )
        sent.append((cond, copy))
        if cond is None:
            copy.start()
        else:
            pl.when(cond)(copy.start)
        return copy

    def local(cond, src, dst, sem):
        copy = pltpu.make_async_copy(src, dst, sem)
        if cond is None:
            copy.start()
        else:
            pl.when(cond)(copy.start)

    def arrived(dst, sem):
        pltpu.make_async_copy(dst, dst, sem).wait()

    mine = traw.at[zb, c]
    local(c == x, tok_in, mine, tsem.at[zb, c])
    remote(c != x, tok_in, mine, tsem.at[zb, c], tp=peer)
    ahead = remote(None, tok_in, mine, tsem.at[zb, c], sp=zp, tp=x)
    remote(None, tok_in, mine, tsem.at[zb, c], fs=fx, tp=x)

    pieces = ((K_AT, DK), (V_AT, DV), (KV_AT, 128), (A_AT, DK), (Q_AT, DK))
    sources = (rk, rv, akp, aq, rq)
    whole = (4,)

    def rows_of(zs, ys, cs):
        return pl.ds(pl.multiple_of(zs * depth + ys * 2 * part + cs * part, part), part)

    def rows_whole(zs, cs):
        return pl.ds(pl.multiple_of(zs * depth + cs * 2 * part, 2 * part), 2 * part)

    def weight(p):
        a, (at, width) = sources[p], pieces[p]
        return a, pl.ds(0, width) if a is akp else pl.ds(pl.multiple_of(x * DK, DK), width), pl.ds(at, width)

    def send_weights(p, cond, to):
        a, cols, at = weight(p)
        for t in range(2):
            if p in whole:
                src = a.at[pl.ds(t * 2 * part, 2 * part), cols]
                dst = w.at[rows_whole(z, t), at]
            else:
                src = a.at[pl.ds(pl.multiple_of(y * 2 * part + t * part, part), part), cols]
                dst = w.at[rows_of(z, y, t), at]
            remote(cond, src, dst, zsem.at[p, z], sp=to, tp=jnp.int32(t))

    def keep_weights(p):
        a, cols, at = weight(p)
        dst = w.at[pl.ds(pl.multiple_of(z * depth, depth), depth), at]
        local(c == zb, a.at[:, cols], dst, ownsem.at[p])
        remote(c == zb, a.at[:, cols], dst, ownsem.at[p], tp=peer)

    to_a = jnp.where(zb == c, z2, zp)
    early = jnp.logical_and(zb != c, mid)
    late = jnp.logical_and(zb != c, jnp.logical_not(mid))
    for p in (0, 1, 3, 4):
        send_weights(p, early, z3)
    for p in (0, 1, 3, 4):
        keep_weights(p)

    out_rows, out_cols = ro.shape

    shares = ((0, 0, out_rows), (1, 0, out_rows // 2), (1, out_rows // 2, out_rows // 2))

    def out_block(share, ys, cs):
        kind, at, n = shares[share]
        rows_at = pl.ds(pl.multiple_of(cs * out_rows + at, n), n)
        return wo.at[kind, ys, rows_at], wosem.at[share, ys, cs]

    def send_out(share):
        kind, at, n = shares[share]
        a = (ro, ao)[kind].at[pl.ds(at, n)]
        block, sem = out_block(share, y, c)
        remote(None, a, block, sem, fs=fy)
        remote(None, a, block, sem, tp=peer)
        local(None, a, block, sem)

    def pass_out(share):
        block, sem = out_block(share, 1 - y, c)
        arrived(block, sem)
        remote(None, block, block, sem, tp=peer)

    def wait_out(kind):
        for share in ((0,), (1, 2))[kind]:
            for ys, cs in ((y, c), (y, peer), (1 - y, peer)):
                arrived(*out_block(share, ys, cs))

    send_out(0)
    send_out(1)

    for i in (1, 2, 3):
        inputs[i].wait()
    small[...] = jnp.zeros_like(small)
    small[pl.ds(GAIN_ROW, 1), :] = gain_v[...]
    for j in range(2):
        small[pl.ds(DECAY_ROW, 1), pl.ds(j * rows, rows)] = decay_v[pl.ds(j, 1), :]
    small[pl.ds(SINK_ROW, 1), pl.ds(0, sink_v.shape[1])] = sink_v[...]
    inputs[4].wait()
    inputs[5].wait()
    packed = [
        jnp.concatenate([ak_v[:, j * HD : (j + 1) * HD], av_v[:, j * HD : (j + 1) * HD]], axis=1) for j in range(2)
    ]
    akp[...] = jnp.where(x == 0, packed[0], packed[1])

    send_weights(2, early, z3)
    keep_weights(2)
    here = jnp.logical_and(zb == c, c == x)
    to_square = 2 * zh + c
    local(here, small, sm.at[zb], smsem.at[zb])
    remote(jnp.logical_not(here), small, sm.at[zb], smsem.at[zb], sp=to_square, tp=x)
    remote(None, small, sm.at[zb], smsem.at[zb], sp=to_square, fs=fx, tp=x)
    gives = jnp.logical_and(first, zb == c)
    local(both(gives, c == x), start.at[x], s0, ssem)
    remote(both(gives, c != x), start.at[x], s0, ssem, tp=peer)

    ahead.wait_send()

    def send_rest(p):
        send_weights(p, None, to_a)
        send_weights(p, late, z3)

    for p in (2, 0, 1):
        send_rest(p)

    for t in range(2):
        block = traw.at[1 - zb, t]

        @pl.when(c == x)
        def _():
            arrived(block, tsem.at[1 - zb, t])

        remote(c == x, block, block, tsem.at[1 - zb, t], fs=fx)

    remote(gives, start.at[1 - x], s0, ssem, fs=fx, tp=x)

    def take(p):
        at, width = pieces[p]
        cols = pl.ds(at, width)
        for zs in order:
            block = w.at[rows_whole(zs, c) if p in whole else rows_of(zs, y, c), cols]
            arrived(block, zsem.at[p, zs])
            if p not in whole:
                remote(None, block, block, ysem.at[p, zs], fs=fy)
            remote(None, block, block, psem.at[p], tp=peer)

    def spread(p):
        at, width = pieces[p]
        cols = pl.ds(at, width)
        for zs in order:
            block = w.at[rows_of(zs, 1 - y, c), cols]
            arrived(block, ysem.at[p, zs])
            remote(None, block, block, psem.at[p], tp=peer)

    def complete(p):
        at, width = pieces[p]
        cols = pl.ds(at, width)
        arrived(w.at[pl.ds(0, depth), cols], ownsem.at[p])
        arrived(w.at[pl.ds(0, 6 * part), cols], psem.at[p])

    inputs[0].wait()

    def normalize(b):
        @pl.loop(0, rows // 32)
        def _(i):
            at = pl.ds(pl.multiple_of(i * 32, 32), 32)
            to = pl.ds(pl.multiple_of(b * rows + i * 32, 32), 32)
            h0, h1 = traw[b, 0, at, :].astype(F32), traw[b, 1, at, :].astype(F32)
            squares = jnp.sum(h0 * h0, axis=-1, keepdims=True) + jnp.sum(h1 * h1, axis=-1, keepdims=True)
            scale = lax.rsqrt(squares / (2 * half) + epsilon)
            xn[to, pl.ds(0, half)] = (h0 * scale * ngain[:, pl.ds(0, half)]).astype(BF16)
            xn[to, pl.ds(half, half)] = (h1 * scale * ngain[:, pl.ds(half, half)]).astype(BF16)

    def token_wait(b):
        for t in range(2):
            block, sem = traw.at[b, t], tsem.at[b, t]
            if b is other:
                pl.when(c != x)(functools.partial(arrived, block, sem))
            else:
                arrived(block, sem)

    own, other = zb, 1 - zb
    token_wait(own)
    normalize(own)
    pl.when(c == x)(functools.partial(normalize, other))
    for b in range(2):
        arrived(sm.at[b], smsem.at[b])
    lane = lax.broadcasted_iota(jnp.int32, (rows, rows), 1)
    row = lax.broadcasted_iota(jnp.int32, (rows, rows), 0)

    def rates(b):
        return sm[b, pl.ds(DECAY_ROW, 1), pl.ds(pl.multiple_of(x * rows, rows), rows)]

    @pl.loop(0, 2)
    def _(b):
        at = pl.ds(pl.multiple_of(b * rows, rows), rows)
        l = rates(b)
        cum = jnp.sum(jnp.where(lane <= row, l, 0.0), axis=1, keepdims=True)
        cum_row = jnp.sum(jnp.where(lane == row, cum, 0.0), axis=0, keepdims=True)
        fade[b] = jnp.where(lane <= row, jnp.exp(jnp.where(lane <= row, cum - cum_row, 0.0)), 0.0)
        since[at, :] = jnp.exp(cum)
        until[at, :] = jnp.exp(jnp.sum(l, axis=1, keepdims=True) - cum)

    pass_out(0)
    take(2)
    take(0)
    send_rest(3)
    spread(2)
    take(1)
    send_rest(4)
    pass_out(1)
    spread(0)
    take(3)
    spread(1)
    send_out(2)
    token_wait(other)
    pl.when(c != x)(functools.partial(normalize, other))
    inputs[6].wait()
    inputs[7].wait()
    complete(2)

    def block_at(b):
        return pl.ds(pl.multiple_of(b * rows, rows), rows)

    def tile(b, at, width):
        return dot(xn[block_at(b), :], w[:, pl.ds(at, width)])

    h = DK // 2

    def turn(a, b, factor):
        co, si = cos[block_at(b), :], sin[block_at(b), :]
        lo, hi = a[:, :h], a[:, h:]
        return jnp.concatenate([(lo * co - hi * si) * factor, (lo * si + hi * co) * factor], axis=1).astype(BF16)

    @pl.when(first)
    def _():
        kvp[pl.ds(0, WINDOW), :] = jnp.zeros((WINDOW, kvp.shape[1]), BF16)

    @pl.loop(0, 2, unroll=True)
    def _(b):
        to = pl.ds(pl.multiple_of(WINDOW + b * rows, WINDOW), rows)
        kvp[to, :] = tile(b, KV_AT, 128).astype(BF16)

    remote(first, kvp.at[pl.ds(2 * rows, WINDOW)], kvp.at[pl.ds(0, WINDOW)], halosem, sp=z2)
    complete(0)
    complete(1)
    @pl.loop(0, 2, unroll=True)
    def _(b):
        at = block_at(b)
        k = turn(tile(b, K_AT, DK).astype(BF16).astype(F32), b, DK ** (-0.5))
        kbuf[at, :] = k
        v = tile(b, V_AT, DV).astype(BF16)
        vbuf[at, :] = v
        kd = (k.astype(F32) * until[at, :]).astype(BF16)
        local_state[b] = dot_l(kd, v)

    def decay_of(b):
        return jnp.exp(jnp.sum(rates(b), axis=1, keepdims=True))

    @pl.when(first)
    def _():
        arrived(s0, ssem)
        states[0] = s0[...].astype(BF16)
        after = s0[...] * decay_of(0) + local_state[0]
        states[1] = after.astype(BF16)
        sbuf[...] = (after * decay_of(1) + local_state[1]).astype(BF16)

    remote(first, sbuf, states.at[0], stsem, sp=z2)

    def hand_on(kind, b, away=None, part_at=None):
        at = pl.ds(0, rows) if part_at is None else pl.ds(part_at * (rows // 2), rows // 2)
        sem = hsem.at[2 if kind else part_at, head]
        src, dst = hid.at[kind, b, at], hin.at[kind, head, at]
        leaves, stays = (zb != b, zb == b) if away is None else (None, None)
        if away is not False:
            remote(leaves, src, dst, sem, sp=zp)
            remote(leaves, src, dst, sem, sp=zp, fs=fx)
        if away is not True:
            remote(stays, src, dst, sem, fs=fx)
            local(stays, src, dst, sem)

    lane2 = lax.broadcasted_iota(jnp.int32, (WINDOW, 2 * WINDOW), 1)
    row2 = lax.broadcasted_iota(jnp.int32, (WINDOW, 2 * WINDOW), 0)
    per = rows // WINDOW
    groups = DK // HD
    sink_row = sm[0, pl.ds(SINK_ROW, 1), pl.ds(0, 128)]
    sink_lane = lax.broadcasted_iota(jnp.int32, (1, 128), 1)
    sinks = [
        jnp.exp(jnp.sum(jnp.where(sink_lane == x * groups + i, sink_row, 0.0), axis=1, keepdims=True))
        for i in range(groups)
    ]

    def attention(b, away):
        aqs = tile(b, A_AT, DK).astype(BF16)
        seen = (lane2 <= row2 + WINDOW) & (lane2 > row2)
        scores, bands = [], []
        for i in range(per):
            n = b * per + i
            band = kvp[pl.ds(pl.multiple_of(n * WINDOW, WINDOW), 2 * WINDOW), :]
            bands.append(band[:, HD:])
            q = aqs[i * WINDOW : (i + 1) * WINDOW]
            stacked = jnp.concatenate([q[:, g * HD : (g + 1) * HD] for g in range(groups)], axis=0)
            scores.append(dot_t(stacked, band[:, :HD]))
        weights = []
        for i in range(per):
            visible = seen & (lane2 + (b * per + i) * WINDOW + zh * 2 * rows >= WINDOW)
            probs = []
            for g in range(groups):
                part_score = scores[i][g * WINDOW : (g + 1) * WINDOW] * HD ** (-0.5)
                e = jnp.exp(jnp.where(visible, part_score, -1e30))
                probs.append((e * (1.0 / (jnp.sum(e, axis=-1, keepdims=True) + sinks[g]))).astype(BF16))
            weights.append(jnp.concatenate(probs, axis=0))
        for i in range(per):
            res = dot(weights[i], bands[i])
            heads_out = [res[g * WINDOW : (g + 1) * WINDOW] for g in range(groups)]
            hid[1, b, pl.ds(i * WINDOW, WINDOW), :] = jnp.concatenate(heads_out, axis=1).astype(BF16)
        hand_on(1, b, away)

    spread(3)
    complete(3)
    pl.when(second)(functools.partial(arrived, kvp.at[pl.ds(0, WINDOW)], halosem))
    attention(other, True)
    take(4)
    attention(own, False)
    complete(4)

    @pl.loop(0, 2, unroll=True)
    def _(b):
        at = block_at(b)
        q = turn(tile(b, Q_AT, DK).astype(BF16).astype(F32), b, 1.0)
        qbuf[at, :] = (q.astype(F32) * since[at, :]).astype(BF16)
        scores = (dot_t(q, kbuf[at, :]) * fade[b]).astype(BF16)
        inner[at, :] = dot(scores, vbuf[at, :])

    @pl.when(second)
    def _():
        arrived(states.at[0], stsem)
        states[1] = (states[0].astype(F32) * decay_of(0) + local_state[0]).astype(BF16)

    gain_at = pl.ds(pl.multiple_of(x * DV, DV), DV)
    for b in (other, own):
        at = block_at(b)
        o = inner[at, :] + dot(qbuf[at, :], states[b])
        centred = o - jnp.mean(o, axis=-1, keepdims=True)
        var = jnp.mean(centred * centred, axis=-1, keepdims=True)
        hid[0, b] = (centred * lax.rsqrt(var + epsilon) * sm[0, pl.ds(GAIN_ROW, 1), gain_at]).astype(BF16)

    for part_at in range(2):
        hand_on(0, other, True, part_at)
        hand_on(0, own, False, part_at)

    pass_out(2)
    others = (2 * zb + 1 - x, 2 * (1 - zb) + x, 2 * (1 - zb) + 1 - x)
    home = c == x

    def mixed_tile(kind, at, t):
        cols = pl.ds(t % 2 * 256, 256)
        acc = None
        for n in range(4):
            term = dot(hin[kind, n, at, :], wo[kind, t // 2, pl.ds(n * DV, DV), cols])
            acc = term if acc is None else acc + term
        return acc

    for n in (head,) + others:
        arrived(hin.at[1, n], hsem.at[2, n])
    wait_out(1)
    wait_out(0)
    for t in range(4):
        total[:, pl.ds(t * 256, 256)] = mixed_tile(1, pl.ds(0, rows), t)

    def finish(part_at):
        at = pl.ds(part_at * (rows // 2), rows // 2)
        for t in range(4):
            ob[t, at, :] = (total[at, pl.ds(t * 256, 256)] + mixed_tile(0, at, t)).astype(BF16)
            src = ob.at[t, at]
            dst = out.at[at, pl.ds(pl.multiple_of(x * out_cols + t % 2 * 256, 256), 256)]
            local(both(home, c == t // 2), src, dst, outsem)
            remote(both(home, c != t // 2), src, dst, outsem, tp=peer)
            remote(jnp.logical_not(home), src, dst, outsem, fs=fx, tp=jnp.int32(t // 2))

    def wait_ret(part_at):
        at = pl.ds(part_at * (rows // 2), rows // 2)
        for n in (head,) + others:
            arrived(hin.at[0, n, at], hsem.at[part_at, n])

    wait_ret(0)
    finish(0)
    wait_ret(1)
    finish(1)

    arrived(out, outsem)
    for cond, copy in sent:
        if copy is ahead:
            continue
        if cond is None:
            copy.wait_send()
        else:
            pl.when(cond)(copy.wait_send)


def layer(mesh, *args):
    (tokens, norm_gain, ret_query, ret_key, ret_value, att_query, att_key, att_value,
     log_decay, start_state, ret_gain, sink_logits, ret_out, att_out) = args
    n_sp, n_fs, n_tp = mesh.shape["sp"], mesh.shape["fs"], mesh.shape["tp"]
    heads = ret_query.shape[1] // DK
    kv_heads = att_key.shape[1] // HD
    rows, half = tokens.shape[1:]
    depth = ret_query.shape[0]
    square = (
        n_tp == 2 and n_fs == 4 and n_sp == 4 and heads == 2 and kv_heads == 2
        and att_query.shape[1] == ret_query.shape[1] and rows == DK and tokens.shape[0] == 1
        and 2 * half == n_sp * depth and ret_out.shape == att_out.shape
        and ret_out.shape == (heads * DV, half // 2) and half == 4 * DK
    )
    if not square:
        return shards(*args)
    h = DK // 2
    length = n_sp * rows
    inverse = np.float32(1.0) / np.float32(10000.0) ** (np.arange(h, dtype=np.float32) / np.float32(h))
    angles = np.arange(length, dtype=np.float32)[:, None] * inverse[None, :]
    cos = jnp.asarray(np.cos(angles), F32)
    sin = jnp.asarray(np.sin(angles), F32)
    wide = heads * rows
    hbm = pl.BlockSpec(memory_space=pl.ANY)
    dma = pltpu.SemaphoreType.DMA
    v = pltpu.VMEM
    res = pl.pallas_call(
        fused,
        out_shape=jax.ShapeDtypeStruct((rows, half), BF16),
        in_specs=[hbm] * 16,
        out_specs=hbm,
        scratch_shapes=[
            v((1, norm_gain.shape[0]), F32),
            v((1, ret_gain.shape[0]), F32),
            v((heads, rows), F32),
            v((1, sink_logits.shape[0]), F32),
            v(att_key.shape, BF16),
            v(att_value.shape, BF16),
            v((2 * rows, h), F32),
            v((2 * rows, h), F32),
            dma((8,)),
            v((8, wide), F32),
            v((2, 8, wide), F32),
            v((2, 2, rows, half), BF16),
            v((2 * rows, 2 * half), BF16),
            v((depth, 128), BF16),
            v((n_sp * depth, A_AT + DK), BF16),
            v((2, 2, 2 * ret_out.shape[0], ret_out.shape[1]), BF16),
            v((DK, DV), F32),
            v((2, DK, DV), F32),
            v((DK, DV), BF16),
            v((2, DK, DV), BF16),
            v((2 * rows, DK), BF16),
            v((2 * rows, DV), BF16),
            v((2 * rows, DK), BF16),
            v((WINDOW + 2 * rows, 128), BF16),
            v((2 * rows, DV), F32),
            v((2, 2, rows, DV), BF16),
            v((2, 4, rows, DV), BF16),
            v((rows, half), F32),
            v((4, rows, 256), BF16),
            v((2, rows, rows), F32),
            v((2 * rows, 1), F32),
            v((2 * rows, 1), F32),
            dma((160,)),
            dma((2,)),
            dma((2, 2)),
            dma((5,)),
            dma((5, n_sp)),
            dma((5, n_sp)),
            dma((5,)),
            dma((3, 2, 2)),
            dma,
            dma,
            dma,
            dma((3, 4)),
            dma,
        ],
        compiler_params=pltpu.CompilerParams(
            collective_id=0, has_side_effects=True, vmem_limit_bytes=67043328
        ),
    )(
        tokens[0], norm_gain[None], ret_query, ret_key, ret_value, att_query, att_key, att_value,
        ret_gain[None], log_decay[0], sink_logits[None], start_state[0], ret_out, att_out, cos, sin,
    )
    return res[None]


def solution(mesh):
    placed = (
        P("fs", "sp", "tp"),
        P(),
        P("sp", "tp"),
        P("sp", "tp"),
        P("sp", "tp"),
        P("sp", "tp"),
        P("sp", "tp"),
        P("sp", "tp"),
        P("fs", "tp", "sp"),
        P("fs", "tp", None, None),
        P("tp"),
        P("tp"),
        P("tp", "fs"),
        P("tp", "fs"),
    )
    return jax.shard_map(
        functools.partial(layer, mesh), mesh=mesh, in_specs=placed, out_specs=P("fs", "sp", "tp"), check_vma=False
    )
```

```python
import functools

import jax
import jax.numpy as jnp
import numpy as np
from jax import lax
from jax.experimental import pallas as pl
from jax.experimental.pallas import tpu as pltpu
from jax.sharding import PartitionSpec as P

DK = 256
DV = 256
HD = 64
WINDOW = 128
BLOCK = 128


epsilon = 1e-06
exact_result = lax.Precision.HIGHEST


def carried_in(array, axis, combine, identity):
    peers, mine = (lax.axis_size(axis), lax.axis_index(axis))
    everything = jax.tree.map(
        lambda part, kind: lax.all_gather(part.astype(kind), axis),
        array,
        (jnp.bfloat16, jnp.bfloat16),
    )
    start = jax.tree.map(
        lambda part, zero: jnp.broadcast_to(jnp.asarray(zero, part.dtype), part.shape),
        array,
        identity,
    )

    def hop(k, before):
        reached = k < mine
        new = combine(
            before, jax.tree.map(lambda part, own: part[k].astype(own.dtype), everything, array)
        )
        return jax.tree.map(lambda a, b: jnp.where(reached, a, b), new, before)

    return lax.fori_loop(0, peers, hop, start)


def passed_along(block, axis, distance):
    devices = range(lax.axis_size(axis))
    route = [(i - distance, i) for i in devices if i - distance in devices]
    return lax.ppermute(block, axis, route)


def rotate(values, positions):
    half_dim = values.shape[-1] // 2
    inverse = 1.0 / 10000.0 ** (jnp.arange(half_dim, dtype=jnp.float32) / half_dim)
    angles = positions.astype(jnp.float32)[:, None] * inverse[None, :]
    cosine = jnp.cos(angles)[:, None, :]
    sine_table = jnp.sin(angles)[:, None, :]
    front_half = values[..., :half_dim]
    back_half = values[..., half_dim:]
    return jnp.concatenate(
        [
            front_half * cosine - back_half * sine_table,
            front_half * sine_table + back_half * cosine,
        ],
        axis=-1,
    )


def block_step(memory_state, inputs):
    queries, key_matrix_rows, value_matrix_rows, log_rates = inputs
    length_here = log_rates.shape[-1]
    causal = jnp.arange(length_here)[:, None] >= jnp.arange(length_here)[None, :]
    running_totals = jnp.cumsum(log_rates, axis=-1)
    relative = running_totals[:, :, None] - running_totals[:, None, :]
    weight = jnp.where(causal[None], jnp.exp(jnp.where(causal[None], relative, 0.0)), 0.0)
    score_matrix = (
        jnp.einsum("hqd,hkd->hqk", queries, key_matrix_rows, precision=exact_result) * weight
    )
    carried_state = jnp.einsum(
        "hqd,hdv->hqv",
        queries * jnp.exp(running_totals)[:, :, None],
        memory_state,
        precision=exact_result,
    )
    output_rows = (
        jnp.einsum("arf,afu->aru", score_matrix, value_matrix_rows, precision=exact_result)
        + carried_state
    )
    decay_factors = jnp.exp(running_totals[:, -1:] - running_totals)
    memory_state = memory_state * jnp.exp(running_totals[:, -1])[:, None, None] + jnp.einsum(
        "iwj,iwe->ije",
        key_matrix_rows * decay_factors[:, :, None],
        value_matrix_rows,
        precision=exact_result,
    )
    return (memory_state, output_rows)


def chain(earlier, later):
    return (earlier[0] * later[0], earlier[1] * later[0][:, None, None] + later[1])


def shards(
    tokens,
    norm_gain,
    ret_query,
    ret_key,
    ret_value,
    att_query,
    att_key,
    att_value,
    log_decay,
    start_state,
    ret_gain,
    sink_logits,
    ret_out,
    att_out,
):
    gathered = lax.all_gather(tokens[0], "tp", axis=1, tiled=True)
    row_count = gathered.shape[0]
    as_float = gathered.astype(jnp.float32)
    normed = (
        as_float
        * lax.rsqrt(jnp.mean(as_float * as_float, axis=-1, keepdims=True) + epsilon)
        * norm_gain
    ).astype(jnp.bfloat16)
    offset = lax.axis_index("sp") * row_count
    positions = offset + jnp.arange(row_count, dtype=jnp.int32)
    weights = (ret_query, ret_key, ret_value, att_query, att_key, att_value)
    pieces = (
        lax.all_gather(weights[0], "sp", axis=0, tiled=True),
        lax.all_gather(weights[1], "sp", axis=0, tiled=True),
        lax.all_gather(weights[2], "sp", axis=0, tiled=True),
        lax.all_gather(weights[3], "sp", axis=0, tiled=True),
        lax.all_gather(weights[4], "sp", axis=0, tiled=True),
        lax.all_gather(weights[5], "sp", axis=0, tiled=True),
    )
    projected = tuple(
        (jnp.dot(normed, piece, preferred_element_type=jnp.float32) for piece in pieces)
    )
    rounded = tuple((product_f.astype(jnp.bfloat16) for product_f in projected))
    projected = rounded[:3]
    head_count = projected[0].shape[1] // DK
    queries = rotate(projected[0].astype(jnp.float32).reshape(row_count, head_count, DK), positions)
    keys_rot = rotate(
        projected[1].astype(jnp.float32).reshape(row_count, head_count, DK), positions
    ) * DK ** (-0.5)
    values_f = projected[2].astype(jnp.float32).reshape(row_count, head_count, DV)
    log_rates = log_decay[0]
    count = row_count // BLOCK

    def blocked(array):
        return array.reshape(count, BLOCK, head_count, array.shape[-1]).transpose(0, 2, 1, 3)

    rates_blocked = log_rates.reshape(head_count, count, BLOCK).transpose(1, 0, 2)
    local_state, pieces = lax.scan(
        block_step,
        jnp.zeros((head_count, DK, DV), jnp.float32),
        (blocked(queries), blocked(keys_rot), blocked(values_f), rates_blocked),
    )
    local_out = pieces.transpose(0, 2, 1, 3).reshape(row_count, head_count, DV)
    running_totals = jnp.cumsum(log_rates, axis=-1)
    device_decay = jnp.exp(running_totals[:, -1])
    identity = (jnp.ones((head_count,), jnp.float32), jnp.zeros((head_count, DK, DV), jnp.float32))
    prior_decay, prior_state = carried_in((device_decay, local_state), "sp", chain, identity)
    incoming = prior_state + prior_decay[:, None, None] * start_state[0]
    retained = local_out + jnp.einsum(
        "thd,hdv->thv",
        queries * jnp.exp(running_totals).T[:, :, None],
        incoming,
        precision=exact_result,
    )
    centred = retained - jnp.mean(retained, axis=-1, keepdims=True)
    variance = jnp.mean(centred * centred, axis=-1, keepdims=True)
    ret_hidden = (
        (centred * lax.rsqrt(variance + epsilon)).reshape(row_count, head_count * DV) * ret_gain
    ).astype(jnp.bfloat16)
    att_queries, att_keys, att_values = rounded[3:]
    kv_heads = att_keys.shape[1] // HD
    groups = att_queries.shape[1] // HD // kv_heads
    earlier_keys, earlier_values = passed_along(
        (att_keys[row_count - WINDOW :], att_values[row_count - WINDOW :]), "sp", 1
    )
    extended_keys = jnp.concatenate([earlier_keys, att_keys], axis=0)
    extended_values = jnp.concatenate([earlier_values, att_values], axis=0)
    windows = row_count // WINDOW

    def banded(array):
        earlier = array[:row_count].reshape(windows, WINDOW, kv_heads, HD)
        current = array[WINDOW:].reshape(windows, WINDOW, kv_heads, HD)
        return jnp.concatenate([earlier, current], axis=1)

    key_band = banded(extended_keys)
    value_band = banded(extended_values)
    grouped_q = att_queries.reshape(windows, WINDOW, kv_heads, groups, HD)
    score_matrix = jnp.einsum(
        "nqhgd,nkhd->nhgqk", grouped_q, key_band, preferred_element_type=jnp.float32
    ) * HD ** (-0.5)
    query_index = WINDOW + jnp.arange(WINDOW)
    key_index = jnp.arange(2 * WINDOW)
    allowed = (key_index[None, :] <= query_index[:, None]) & (
        query_index[:, None] - key_index[None, :] < WINDOW
    )
    key_place = offset - WINDOW + jnp.arange(windows)[:, None] * WINDOW + key_index[None, :]
    visible = (allowed[None] & (key_place >= 0)[:, None, :])[:, None, None]
    expo = jnp.exp(jnp.where(visible, score_matrix, -1e30))
    summed = jnp.sum(expo, axis=-1, keepdims=True) + jnp.exp(sink_logits).reshape(
        1, kv_heads, groups, 1, 1
    )
    probs = (expo / summed).astype(jnp.bfloat16)
    attended = jnp.einsum(
        "nhgqk,nkhd->nqhgd", probs, value_band, preferred_element_type=jnp.float32
    )
    att_hidden = attended.astype(jnp.bfloat16).reshape(row_count, kv_heads * groups * HD)
    ret_width = ret_hidden.shape[1]
    joined = jnp.concatenate([ret_hidden, att_hidden], axis=1)[None]
    piece = lax.all_gather(joined, "fs", axis=0, tiled=True)
    product = jnp.einsum(
        "srh,hd->srd", piece[:, :, :ret_width], ret_out, preferred_element_type=jnp.float32
    )
    product = product + jnp.einsum(
        "srh,hd->srd", piece[:, :, ret_width:], att_out, preferred_element_type=jnp.float32
    )
    partial_rows = product.astype(jnp.bfloat16)
    regrouped = lax.all_to_all(partial_rows, "fs", split_axis=0, concat_axis=2, tiled=True)
    mixed = lax.psum_scatter(
        regrouped[0].astype(jnp.float32).astype(jnp.bfloat16), "tp", scatter_dimension=1, tiled=True
    )
    return mixed[None]


MESH = pl.DeviceIdType.MESH
F32 = jnp.float32
BF16 = jnp.bfloat16
GAIN_ROW = 0
DECAY_ROW = 1
SINK_ROW = 2
K_AT, V_AT, KV_AT, Q_AT, A_AT = 0, 256, 512, 640, 896


def dot(a, b):
    return jnp.dot(a, b, preferred_element_type=F32)


def dot_t(a, b):
    return lax.dot_general(a, b, (((1,), (1,)), ((), ())), preferred_element_type=F32)


def dot_l(a, b):
    return lax.dot_general(a, b, (((0,), (0,)), ((), ())), preferred_element_type=F32)


def fused(
    tok_in, ngain_in, rq, rk, rv, aq, ak, av, gain_in, decay_in, sink_in, start, ro, ao, cos_in, sin_in, out,
    ngain, gain_v, decay_v, sink_v, ak_v, av_v, cos, sin, insem,
    small, sm, traw, xn, akp, w, wo, s0, local_state, sbuf, states, kbuf, vbuf, qbuf, kvp, inner, hid, hin,
    total, ob, fade, since, until, wx,
    send, smsem, tsem, ownsem, zsem, ysem, psem, wosem, ssem, stsem, halosem, hsem, outsem, xsem,
):
    z, f, c = lax.axis_index("sp"), lax.axis_index("fs"), lax.axis_index("tp")
    y, x = f // 2, lax.rem(f, 2)
    zh, zb = z // 2, lax.rem(z, 2)
    peer = 1 - c
    fx, fy = 2 * y + 1 - x, 2 * (1 - y) + x
    zp, z2, z3 = z + 1 - 2 * zb, lax.rem(z + 2, 4), 3 - z
    head = 2 * zb + x
    rows, half = tok_in.shape
    depth = rq.shape[0]
    part = depth // 4
    mid = jnp.logical_or(z == 1, z == 2)
    near, far = jnp.where(mid, z3, z2), jnp.where(mid, z2, z3)
    order = (zp, near, far)
    first, second = zh == 0, zh == 1

    loads = [
        (ngain_in, ngain), (gain_in, gain_v), (decay_in, decay_v), (sink_in, sink_v), (ak, ak_v), (av, av_v),
        (cos_in.at[pl.ds(pl.multiple_of(zh * 2 * rows, 2 * rows), 2 * rows)], cos),
        (sin_in.at[pl.ds(pl.multiple_of(zh * 2 * rows, 2 * rows), 2 * rows)], sin),
    ]
    inputs = [pltpu.make_async_copy(src, dst, insem.at[i]) for i, (src, dst) in enumerate(loads)]
    for copy in inputs:
        copy.start()

    barrier = pltpu.get_barrier_semaphore()
    greeted = [{"tp": peer}, {"fs": fy}]
    for t in range(2):
        core = jnp.int32(t)
        greeted += [{"sp": zs, "tp": core} for zs in order]
        greeted += [{"fs": fx, "tp": core}, {"sp": zp, "fs": fx, "tp": core}]
    for where in greeted:
        pl.semaphore_signal(barrier, inc=1, device_id=where, device_id_type=MESH)
    pl.semaphore_wait(barrier, len(greeted))

    sent = []
    slots = iter(range(send.shape[0]))

    def both(a, b):
        if a is None:
            return b
        return a if b is None else jnp.logical_and(a, b)

    def remote(cond, src, dst, rsem, **where):
        copy = pltpu.make_async_remote_copy(
            src_ref=src, dst_ref=dst, send_sem=send.at[next(slots)], recv_sem=rsem,
            device_id=where, device_id_type=MESH,
        )
        sent.append((cond, copy))
        if cond is None:
            copy.start()
        else:
            pl.when(cond)(copy.start)
        return copy

    def local(cond, src, dst, sem):
        copy = pltpu.make_async_copy(src, dst, sem)
        if cond is None:
            copy.start()
        else:
            pl.when(cond)(copy.start)

    def arrived(dst, sem):
        pltpu.make_async_copy(dst, dst, sem).wait()

    mine = traw.at[zb, c]
    local(c == x, tok_in, mine, tsem.at[zb, c])
    remote(c != x, tok_in, mine, tsem.at[zb, c], tp=peer)
    ahead = remote(None, tok_in, mine, tsem.at[zb, c], sp=zp, tp=x)
    remote(None, tok_in, mine, tsem.at[zb, c], fs=fx, tp=x)

    pieces = ((K_AT, DK), (V_AT, DV), (KV_AT, 128), (A_AT, DK), (Q_AT, DK))
    sources = (rk, rv, akp, aq, rq)
    whole = (4,)

    def rows_of(zs, ys, cs):
        return pl.ds(pl.multiple_of(zs * depth + ys * 2 * part + cs * part, part), part)

    def rows_whole(zs, cs):
        return pl.ds(pl.multiple_of(zs * depth + cs * 2 * part, 2 * part), 2 * part)

    def weight(p):
        a, (at, width) = sources[p], pieces[p]
        return a, pl.ds(0, width) if a is akp else pl.ds(pl.multiple_of(x * DK, DK), width), pl.ds(at, width)

    def send_weights(p, cond, to):
        a, cols, at = weight(p)
        for t in range(2):
            if p in whole:
                src = a.at[pl.ds(t * 2 * part, 2 * part), cols]
                dst = w.at[rows_whole(z, t), at]
            else:
                src = a.at[pl.ds(pl.multiple_of(y * 2 * part + t * part, part), part), cols]
                dst = w.at[rows_of(z, y, t), at]
            remote(cond, src, dst, zsem.at[p, z], sp=to, tp=jnp.int32(t))

    def keep_weights(p):
        a, cols, at = weight(p)
        dst = w.at[pl.ds(pl.multiple_of(z * depth, depth), depth), at]
        local(c == zb, a.at[:, cols], dst, ownsem.at[p])
        remote(c == zb, a.at[:, cols], dst, ownsem.at[p], tp=peer)

    to_a = jnp.where(zb == c, z2, zp)
    early = jnp.logical_and(zb != c, mid)
    late = jnp.logical_and(zb != c, jnp.logical_not(mid))
    for p in (0, 1, 3, 4):
        send_weights(p, early, z3)
    for p in (0, 1, 3, 4):
        keep_weights(p)

    out_rows, out_cols = ro.shape

    shares = ((0, 0, out_rows), (1, 0, out_rows // 2), (1, out_rows // 2, out_rows // 2))

    def out_block(share, ys, cs):
        kind, at, n = shares[share]
        rows_at = pl.ds(pl.multiple_of(cs * out_rows + at, n), n)
        return wo.at[kind, ys, rows_at], wosem.at[share, ys, cs]

    def send_out(share):
        kind, at, n = shares[share]
        a = (ro, ao)[kind].at[pl.ds(at, n)]
        block, sem = out_block(share, y, c)
        remote(None, a, block, sem, fs=fy)
        remote(None, a, block, sem, tp=peer)
        local(None, a, block, sem)

    def pass_out(share):
        block, sem = out_block(share, 1 - y, c)
        arrived(block, sem)
        remote(None, block, block, sem, tp=peer)

    def wait_out(kind):
        for share in ((0,), (1, 2))[kind]:
            for ys, cs in ((y, c), (y, peer), (1 - y, peer)):
                arrived(*out_block(share, ys, cs))

    extra_cols = pl.ds(out_cols // 2, out_cols // 2)

    def extra(kind, cs):
        return wx.at[kind, pl.ds(pl.multiple_of(cs * out_rows, out_rows), out_rows)], xsem.at[kind, cs]

    def send_extra(cond):
        for kind, a in ((0, ro), (1, ao)):
            dst, sem = extra(kind, c)
            remote(cond, a.at[:, extra_cols], dst, sem, fs=fx, tp=1 - x)

    send_out(0)
    send_out(1)

    for i in (1, 2, 3):
        inputs[i].wait()
    small[...] = jnp.zeros_like(small)
    small[pl.ds(GAIN_ROW, 1), :] = gain_v[...]
    for j in range(2):
        small[pl.ds(DECAY_ROW, 1), pl.ds(j * rows, rows)] = decay_v[pl.ds(j, 1), :]
    small[pl.ds(SINK_ROW, 1), pl.ds(0, sink_v.shape[1])] = sink_v[...]
    inputs[4].wait()
    inputs[5].wait()
    packed = [
        jnp.concatenate([ak_v[:, j * HD : (j + 1) * HD], av_v[:, j * HD : (j + 1) * HD]], axis=1) for j in range(2)
    ]
    akp[...] = jnp.where(x == 0, packed[0], packed[1])

    send_weights(2, early, z3)
    keep_weights(2)
    here = jnp.logical_and(zb == c, c == x)
    to_square = 2 * zh + c
    local(here, small, sm.at[zb], smsem.at[zb])
    remote(jnp.logical_not(here), small, sm.at[zb], smsem.at[zb], sp=to_square, tp=x)
    remote(None, small, sm.at[zb], smsem.at[zb], sp=to_square, fs=fx, tp=x)
    gives = jnp.logical_and(first, zb == c)
    local(both(gives, c == x), start.at[x], s0, ssem)
    remote(both(gives, c != x), start.at[x], s0, ssem, tp=peer)

    ahead.wait_send()

    def send_rest(p):
        send_weights(p, None, to_a)
        send_weights(p, late, z3)

    for p in (2, 0, 1):
        send_rest(p)

    for t in range(2):
        block = traw.at[1 - zb, t]

        @pl.when(c == x)
        def _():
            arrived(block, tsem.at[1 - zb, t])

        remote(c == x, block, block, tsem.at[1 - zb, t], fs=fx)

    remote(gives, start.at[1 - x], s0, ssem, fs=fx, tp=x)

    def take(p):
        at, width = pieces[p]
        cols = pl.ds(at, width)
        for zs in order:
            block = w.at[rows_whole(zs, c) if p in whole else rows_of(zs, y, c), cols]
            arrived(block, zsem.at[p, zs])
            if p not in whole:
                remote(None, block, block, ysem.at[p, zs], fs=fy)
            remote(None, block, block, psem.at[p], tp=peer)

    def spread(p):
        at, width = pieces[p]
        cols = pl.ds(at, width)
        for zs in order:
            block = w.at[rows_of(zs, 1 - y, c), cols]
            arrived(block, ysem.at[p, zs])
            remote(None, block, block, psem.at[p], tp=peer)

    def complete(p):
        at, width = pieces[p]
        cols = pl.ds(at, width)
        arrived(w.at[pl.ds(0, depth), cols], ownsem.at[p])
        arrived(w.at[pl.ds(0, 6 * part), cols], psem.at[p])

    inputs[0].wait()

    def normalize(b):
        @pl.loop(0, rows // 32)
        def _(i):
            at = pl.ds(pl.multiple_of(i * 32, 32), 32)
            to = pl.ds(pl.multiple_of(b * rows + i * 32, 32), 32)
            h0, h1 = traw[b, 0, at, :].astype(F32), traw[b, 1, at, :].astype(F32)
            squares = jnp.sum(h0 * h0, axis=-1, keepdims=True) + jnp.sum(h1 * h1, axis=-1, keepdims=True)
            scale = lax.rsqrt(squares / (2 * half) + epsilon)
            xn[to, pl.ds(0, half)] = (h0 * scale * ngain[:, pl.ds(0, half)]).astype(BF16)
            xn[to, pl.ds(half, half)] = (h1 * scale * ngain[:, pl.ds(half, half)]).astype(BF16)

    def token_wait(b):
        for t in range(2):
            block, sem = traw.at[b, t], tsem.at[b, t]
            if b is other:
                pl.when(c != x)(functools.partial(arrived, block, sem))
            else:
                arrived(block, sem)

    own, other = zb, 1 - zb
    token_wait(own)
    normalize(own)
    pl.when(c == x)(functools.partial(normalize, other))
    send_extra(c == x)
    for b in range(2):
        arrived(sm.at[b], smsem.at[b])
    lane = lax.broadcasted_iota(jnp.int32, (rows, rows), 1)
    row = lax.broadcasted_iota(jnp.int32, (rows, rows), 0)

    def rates(b):
        return sm[b, pl.ds(DECAY_ROW, 1), pl.ds(pl.multiple_of(x * rows, rows), rows)]

    @pl.loop(0, 2)
    def _(b):
        at = pl.ds(pl.multiple_of(b * rows, rows), rows)
        l = rates(b)
        cum = jnp.sum(jnp.where(lane <= row, l, 0.0), axis=1, keepdims=True)
        cum_row = jnp.sum(jnp.where(lane == row, cum, 0.0), axis=0, keepdims=True)
        fade[b] = jnp.where(lane <= row, jnp.exp(jnp.where(lane <= row, cum - cum_row, 0.0)), 0.0)
        since[at, :] = jnp.exp(cum)
        until[at, :] = jnp.exp(jnp.sum(l, axis=1, keepdims=True) - cum)

    pass_out(0)
    take(2)
    take(0)
    send_rest(3)
    spread(2)
    take(1)
    send_rest(4)
    pass_out(1)
    spread(0)
    take(3)
    spread(1)
    send_out(2)
    token_wait(other)
    pl.when(c != x)(functools.partial(normalize, other))
    send_extra(c != x)
    inputs[6].wait()
    inputs[7].wait()
    complete(2)

    def block_at(b):
        return pl.ds(pl.multiple_of(b * rows, rows), rows)

    def tile(b, at, width):
        return dot(xn[block_at(b), :], w[:, pl.ds(at, width)])

    h = DK // 2

    def turn(a, b, factor):
        co, si = cos[block_at(b), :], sin[block_at(b), :]
        lo, hi = a[:, :h], a[:, h:]
        return jnp.concatenate([(lo * co - hi * si) * factor, (lo * si + hi * co) * factor], axis=1).astype(BF16)

    @pl.when(first)
    def _():
        kvp[pl.ds(0, WINDOW), :] = jnp.zeros((WINDOW, kvp.shape[1]), BF16)

    @pl.loop(0, 2, unroll=True)
    def _(b):
        to = pl.ds(pl.multiple_of(WINDOW + b * rows, WINDOW), rows)
        kvp[to, :] = tile(b, KV_AT, 128).astype(BF16)

    remote(first, kvp.at[pl.ds(2 * rows, WINDOW)], kvp.at[pl.ds(0, WINDOW)], halosem, sp=z2)
    complete(0)
    complete(1)
    @pl.loop(0, 2, unroll=True)
    def _(b):
        at = block_at(b)
        k = turn(tile(b, K_AT, DK).astype(BF16).astype(F32), b, DK ** (-0.5))
        kbuf[at, :] = k
        v = tile(b, V_AT, DV).astype(BF16)
        vbuf[at, :] = v
        kd = (k.astype(F32) * until[at, :]).astype(BF16)
        local_state[b] = dot_l(kd, v)

    def decay_of(b):
        return jnp.exp(jnp.sum(rates(b), axis=1, keepdims=True))

    @pl.when(first)
    def _():
        arrived(s0, ssem)
        states[0] = s0[...].astype(BF16)
        after = s0[...] * decay_of(0) + local_state[0]
        states[1] = after.astype(BF16)
        sbuf[...] = (after * decay_of(1) + local_state[1]).astype(BF16)

    remote(first, sbuf, states.at[0], stsem, sp=z2)

    def hand_on(kind, b, away=None, part_at=None):
        at = pl.ds(0, rows) if part_at is None else pl.ds(part_at * (rows // 2), rows // 2)
        sem = hsem.at[2 if kind else part_at, head]
        src, dst = hid.at[kind, b, at], hin.at[kind, head, at]
        leaves, stays = (zb != b, zb == b) if away is None else (None, None)
        if away is not False:
            remote(leaves, src, dst, sem, sp=zp)
            remote(leaves, src, dst, sem, sp=zp, fs=fx)
        if away is not True:
            remote(stays, src, dst, sem, fs=fx)
            local(stays, src, dst, sem)

    lane2 = lax.broadcasted_iota(jnp.int32, (WINDOW, 2 * WINDOW), 1)
    row2 = lax.broadcasted_iota(jnp.int32, (WINDOW, 2 * WINDOW), 0)
    per = rows // WINDOW
    groups = DK // HD
    sink_row = sm[0, pl.ds(SINK_ROW, 1), pl.ds(0, 128)]
    sink_lane = lax.broadcasted_iota(jnp.int32, (1, 128), 1)
    sinks = [
        jnp.exp(jnp.sum(jnp.where(sink_lane == x * groups + i, sink_row, 0.0), axis=1, keepdims=True))
        for i in range(groups)
    ]

    def attention(b, away):
        aqs = tile(b, A_AT, DK).astype(BF16)
        seen = (lane2 <= row2 + WINDOW) & (lane2 > row2)
        scores, bands = [], []
        for i in range(per):
            n = b * per + i
            band = kvp[pl.ds(pl.multiple_of(n * WINDOW, WINDOW), 2 * WINDOW), :]
            bands.append(band[:, HD:])
            q = aqs[i * WINDOW : (i + 1) * WINDOW]
            stacked = jnp.concatenate([q[:, g * HD : (g + 1) * HD] for g in range(groups)], axis=0)
            scores.append(dot_t(stacked, band[:, :HD]))
        weights = []
        for i in range(per):
            visible = seen & (lane2 + (b * per + i) * WINDOW + zh * 2 * rows >= WINDOW)
            probs = []
            for g in range(groups):
                part_score = scores[i][g * WINDOW : (g + 1) * WINDOW] * HD ** (-0.5)
                e = jnp.exp(jnp.where(visible, part_score, -1e30))
                probs.append((e * (1.0 / (jnp.sum(e, axis=-1, keepdims=True) + sinks[g]))).astype(BF16))
            weights.append(jnp.concatenate(probs, axis=0))
        for i in range(per):
            res = dot(weights[i], bands[i])
            heads_out = [res[g * WINDOW : (g + 1) * WINDOW] for g in range(groups)]
            hid[1, b, pl.ds(i * WINDOW, WINDOW), :] = jnp.concatenate(heads_out, axis=1).astype(BF16)
        hand_on(1, b, away)

    spread(3)
    complete(3)
    pl.when(second)(functools.partial(arrived, kvp.at[pl.ds(0, WINDOW)], halosem))
    attention(other, True)
    take(4)
    attention(own, False)
    complete(4)

    @pl.loop(0, 2, unroll=True)
    def _(b):
        at = block_at(b)
        q = turn(tile(b, Q_AT, DK).astype(BF16).astype(F32), b, 1.0)
        qbuf[at, :] = (q.astype(F32) * since[at, :]).astype(BF16)
        scores = (dot_t(q, kbuf[at, :]) * fade[b]).astype(BF16)
        inner[at, :] = dot(scores, vbuf[at, :])

    @pl.when(second)
    def _():
        arrived(states.at[0], stsem)
        states[1] = (states[0].astype(F32) * decay_of(0) + local_state[0]).astype(BF16)

    gain_at = pl.ds(pl.multiple_of(x * DV, DV), DV)
    for b in (other, own):
        at = block_at(b)
        o = inner[at, :] + dot(qbuf[at, :], states[b])
        centred = o - jnp.mean(o, axis=-1, keepdims=True)
        var = jnp.mean(centred * centred, axis=-1, keepdims=True)
        hid[0, b] = (centred * lax.rsqrt(var + epsilon) * sm[0, pl.ds(GAIN_ROW, 1), gain_at]).astype(BF16)

    for part_at in range(2):
        hand_on(0, other, True, part_at)
        hand_on(0, own, False, part_at)

    pass_out(2)
    others = (2 * zb + 1 - x, 2 * (1 - zb) + x, 2 * (1 - zb) + 1 - x)
    home = c == x

    def mixed_tile(kind, at, t):
        cols = pl.ds(t % 2 * 256, 256)
        acc = None
        for n in range(4):
            term = dot(hin[kind, n, at, :], wo[kind, t // 2, pl.ds(n * DV, DV), cols])
            acc = term if acc is None else acc + term
        return acc

    def extra_tile(kind, at):
        acc = None
        for n in range(4):
            term = dot(hin[kind, n, at, :], wx[kind, pl.ds(n * DV, DV), :])
            acc = term if acc is None else acc + term
        return acc

    for n in (head,) + others:
        arrived(hin.at[1, n], hsem.at[2, n])
    wait_out(1)
    wait_out(0)
    for t in range(4):
        total[:, pl.ds(t * 256, 256)] = mixed_tile(1, pl.ds(0, rows), t)

    @pl.when(home)
    def _():
        for kind in range(2):
            for cs in range(2):
                arrived(*extra(kind, cs))
        total[:, pl.ds(half, 256)] = extra_tile(1, pl.ds(0, rows))

    def finish(part_at):
        at = pl.ds(part_at * (rows // 2), rows // 2)
        for t in range(4):
            ob[t, at, :] = (total[at, pl.ds(t * 256, 256)] + mixed_tile(0, at, t)).astype(BF16)
            src = ob.at[t, at]
            dst = out.at[at, pl.ds(pl.multiple_of(x * out_cols + t % 2 * 256, 256), 256)]
            local(both(home, c == t // 2), src, dst, outsem)
            remote(both(home, c != t // 2), src, dst, outsem, tp=peer)
            leaves = c != x if t % 2 == 0 else jnp.logical_and(c != x, y != t // 2)
            remote(leaves, src, dst, outsem, fs=fx, tp=jnp.int32(t // 2))

        @pl.when(home)
        def _():
            ob[4, at, :] = (total[at, pl.ds(half, 256)] + extra_tile(0, at)).astype(BF16)

        src = ob.at[4, at]
        dst = out.at[at, pl.ds(pl.multiple_of((1 - x) * out_cols + out_cols // 2, 256), 256)]
        local(both(home, c == y), src, dst, outsem)
        remote(both(home, c != y), src, dst, outsem, tp=peer)

    def wait_ret(part_at):
        at = pl.ds(part_at * (rows // 2), rows // 2)
        for n in (head,) + others:
            arrived(hin.at[0, n, at], hsem.at[part_at, n])

    wait_ret(0)
    finish(0)
    wait_ret(1)
    finish(1)

    arrived(out, outsem)
    for cond, copy in sent:
        if copy is ahead:
            continue
        if cond is None:
            copy.wait_send()
        else:
            pl.when(cond)(copy.wait_send)


def layer(mesh, *args):
    (tokens, norm_gain, ret_query, ret_key, ret_value, att_query, att_key, att_value,
     log_decay, start_state, ret_gain, sink_logits, ret_out, att_out) = args
    n_sp, n_fs, n_tp = mesh.shape["sp"], mesh.shape["fs"], mesh.shape["tp"]
    heads = ret_query.shape[1] // DK
    kv_heads = att_key.shape[1] // HD
    rows, half = tokens.shape[1:]
    depth = ret_query.shape[0]
    square = (
        n_tp == 2 and n_fs == 4 and n_sp == 4 and heads == 2 and kv_heads == 2
        and att_query.shape[1] == ret_query.shape[1] and rows == DK and tokens.shape[0] == 1
        and 2 * half == n_sp * depth and ret_out.shape == att_out.shape
        and ret_out.shape == (heads * DV, half // 2) and half == 4 * DK
    )
    if not square:
        return shards(*args)
    h = DK // 2
    length = n_sp * rows
    inverse = np.float32(1.0) / np.float32(10000.0) ** (np.arange(h, dtype=np.float32) / np.float32(h))
    angles = np.arange(length, dtype=np.float32)[:, None] * inverse[None, :]
    cos = jnp.asarray(np.cos(angles), F32)
    sin = jnp.asarray(np.sin(angles), F32)
    wide = heads * rows
    hbm = pl.BlockSpec(memory_space=pl.ANY)
    dma = pltpu.SemaphoreType.DMA
    v = pltpu.VMEM
    res = pl.pallas_call(
        fused,
        out_shape=jax.ShapeDtypeStruct((rows, half), BF16),
        in_specs=[hbm] * 16,
        out_specs=hbm,
        scratch_shapes=[
            v((1, norm_gain.shape[0]), F32),
            v((1, ret_gain.shape[0]), F32),
            v((heads, rows), F32),
            v((1, sink_logits.shape[0]), F32),
            v(att_key.shape, BF16),
            v(att_value.shape, BF16),
            v((2 * rows, h), F32),
            v((2 * rows, h), F32),
            dma((8,)),
            v((8, wide), F32),
            v((2, 8, wide), F32),
            v((2, 2, rows, half), BF16),
            v((2 * rows, 2 * half), BF16),
            v((depth, 128), BF16),
            v((n_sp * depth, A_AT + DK), BF16),
            v((2, 2, 2 * ret_out.shape[0], ret_out.shape[1]), BF16),
            v((DK, DV), F32),
            v((2, DK, DV), F32),
            v((DK, DV), BF16),
            v((2, DK, DV), BF16),
            v((2 * rows, DK), BF16),
            v((2 * rows, DV), BF16),
            v((2 * rows, DK), BF16),
            v((WINDOW + 2 * rows, 128), BF16),
            v((2 * rows, DV), F32),
            v((2, 2, rows, DV), BF16),
            v((2, 4, rows, DV), BF16),
            v((rows, half + 256), F32),
            v((5, rows, 256), BF16),
            v((2, rows, rows), F32),
            v((2 * rows, 1), F32),
            v((2 * rows, 1), F32),
            v((2, 2 * ret_out.shape[0], ret_out.shape[1] // 2), BF16),
            dma((160,)),
            dma((2,)),
            dma((2, 2)),
            dma((5,)),
            dma((5, n_sp)),
            dma((5, n_sp)),
            dma((5,)),
            dma((3, 2, 2)),
            dma,
            dma,
            dma,
            dma((3, 4)),
            dma,
            dma((2, 2)),
        ],
        compiler_params=pltpu.CompilerParams(
            collective_id=0, has_side_effects=True, vmem_limit_bytes=67043328
        ),
    )(
        tokens[0], norm_gain[None], ret_query, ret_key, ret_value, att_query, att_key, att_value,
        ret_gain[None], log_decay[0], sink_logits[None], start_state[0], ret_out, att_out, cos, sin,
    )
    return res[None]


def solution(mesh):
    placed = (
        P("fs", "sp", "tp"),
        P(),
        P("sp", "tp"),
        P("sp", "tp"),
        P("sp", "tp"),
        P("sp", "tp"),
        P("sp", "tp"),
        P("sp", "tp"),
        P("fs", "tp", "sp"),
        P("fs", "tp", None, None),
        P("tp"),
        P("tp"),
        P("tp", "fs"),
        P("tp", "fs"),
    )
    return jax.shard_map(
        functools.partial(layer, mesh), mesh=mesh, in_specs=placed, out_specs=P("fs", "sp", "tp"), check_vma=False
    )
```

```python
import functools

import jax
import jax.numpy as jnp
import numpy as np
from jax import lax
from jax.experimental import pallas as pl
from jax.experimental.pallas import tpu as pltpu
from jax.sharding import PartitionSpec as P

DK = 256
DV = 256
HD = 64
WINDOW = 128
BLOCK = 128


epsilon = 1e-06
exact_result = lax.Precision.HIGHEST


def carried_in(array, axis, combine, identity):
    peers, mine = (lax.axis_size(axis), lax.axis_index(axis))
    everything = jax.tree.map(
        lambda part, kind: lax.all_gather(part.astype(kind), axis),
        array,
        (jnp.bfloat16, jnp.bfloat16),
    )
    start = jax.tree.map(
        lambda part, zero: jnp.broadcast_to(jnp.asarray(zero, part.dtype), part.shape),
        array,
        identity,
    )

    def hop(k, before):
        reached = k < mine
        new = combine(
            before, jax.tree.map(lambda part, own: part[k].astype(own.dtype), everything, array)
        )
        return jax.tree.map(lambda a, b: jnp.where(reached, a, b), new, before)

    return lax.fori_loop(0, peers, hop, start)


def passed_along(block, axis, distance):
    devices = range(lax.axis_size(axis))
    route = [(i - distance, i) for i in devices if i - distance in devices]
    return lax.ppermute(block, axis, route)


def rotate(values, positions):
    half_dim = values.shape[-1] // 2
    inverse = 1.0 / 10000.0 ** (jnp.arange(half_dim, dtype=jnp.float32) / half_dim)
    angles = positions.astype(jnp.float32)[:, None] * inverse[None, :]
    cosine = jnp.cos(angles)[:, None, :]
    sine_table = jnp.sin(angles)[:, None, :]
    front_half = values[..., :half_dim]
    back_half = values[..., half_dim:]
    return jnp.concatenate(
        [
            front_half * cosine - back_half * sine_table,
            front_half * sine_table + back_half * cosine,
        ],
        axis=-1,
    )


def block_step(memory_state, inputs):
    queries, key_matrix_rows, value_matrix_rows, log_rates = inputs
    length_here = log_rates.shape[-1]
    causal = jnp.arange(length_here)[:, None] >= jnp.arange(length_here)[None, :]
    running_totals = jnp.cumsum(log_rates, axis=-1)
    relative = running_totals[:, :, None] - running_totals[:, None, :]
    weight = jnp.where(causal[None], jnp.exp(jnp.where(causal[None], relative, 0.0)), 0.0)
    score_matrix = (
        jnp.einsum("hqd,hkd->hqk", queries, key_matrix_rows, precision=exact_result) * weight
    )
    carried_state = jnp.einsum(
        "hqd,hdv->hqv",
        queries * jnp.exp(running_totals)[:, :, None],
        memory_state,
        precision=exact_result,
    )
    output_rows = (
        jnp.einsum("arf,afu->aru", score_matrix, value_matrix_rows, precision=exact_result)
        + carried_state
    )
    decay_factors = jnp.exp(running_totals[:, -1:] - running_totals)
    memory_state = memory_state * jnp.exp(running_totals[:, -1])[:, None, None] + jnp.einsum(
        "iwj,iwe->ije",
        key_matrix_rows * decay_factors[:, :, None],
        value_matrix_rows,
        precision=exact_result,
    )
    return (memory_state, output_rows)


def chain(earlier, later):
    return (earlier[0] * later[0], earlier[1] * later[0][:, None, None] + later[1])


def shards(
    tokens,
    norm_gain,
    ret_query,
    ret_key,
    ret_value,
    att_query,
    att_key,
    att_value,
    log_decay,
    start_state,
    ret_gain,
    sink_logits,
    ret_out,
    att_out,
):
    gathered = lax.all_gather(tokens[0], "tp", axis=1, tiled=True)
    row_count = gathered.shape[0]
    as_float = gathered.astype(jnp.float32)
    normed = (
        as_float
        * lax.rsqrt(jnp.mean(as_float * as_float, axis=-1, keepdims=True) + epsilon)
        * norm_gain
    ).astype(jnp.bfloat16)
    offset = lax.axis_index("sp") * row_count
    positions = offset + jnp.arange(row_count, dtype=jnp.int32)
    weights = (ret_query, ret_key, ret_value, att_query, att_key, att_value)
    pieces = (
        lax.all_gather(weights[0], "sp", axis=0, tiled=True),
        lax.all_gather(weights[1], "sp", axis=0, tiled=True),
        lax.all_gather(weights[2], "sp", axis=0, tiled=True),
        lax.all_gather(weights[3], "sp", axis=0, tiled=True),
        lax.all_gather(weights[4], "sp", axis=0, tiled=True),
        lax.all_gather(weights[5], "sp", axis=0, tiled=True),
    )
    projected = tuple(
        (jnp.dot(normed, piece, preferred_element_type=jnp.float32) for piece in pieces)
    )
    rounded = tuple((product_f.astype(jnp.bfloat16) for product_f in projected))
    projected = rounded[:3]
    head_count = projected[0].shape[1] // DK
    queries = rotate(projected[0].astype(jnp.float32).reshape(row_count, head_count, DK), positions)
    keys_rot = rotate(
        projected[1].astype(jnp.float32).reshape(row_count, head_count, DK), positions
    ) * DK ** (-0.5)
    values_f = projected[2].astype(jnp.float32).reshape(row_count, head_count, DV)
    log_rates = log_decay[0]
    count = row_count // BLOCK

    def blocked(array):
        return array.reshape(count, BLOCK, head_count, array.shape[-1]).transpose(0, 2, 1, 3)

    rates_blocked = log_rates.reshape(head_count, count, BLOCK).transpose(1, 0, 2)
    local_state, pieces = lax.scan(
        block_step,
        jnp.zeros((head_count, DK, DV), jnp.float32),
        (blocked(queries), blocked(keys_rot), blocked(values_f), rates_blocked),
    )
    local_out = pieces.transpose(0, 2, 1, 3).reshape(row_count, head_count, DV)
    running_totals = jnp.cumsum(log_rates, axis=-1)
    device_decay = jnp.exp(running_totals[:, -1])
    identity = (jnp.ones((head_count,), jnp.float32), jnp.zeros((head_count, DK, DV), jnp.float32))
    prior_decay, prior_state = carried_in((device_decay, local_state), "sp", chain, identity)
    incoming = prior_state + prior_decay[:, None, None] * start_state[0]
    retained = local_out + jnp.einsum(
        "thd,hdv->thv",
        queries * jnp.exp(running_totals).T[:, :, None],
        incoming,
        precision=exact_result,
    )
    centred = retained - jnp.mean(retained, axis=-1, keepdims=True)
    variance = jnp.mean(centred * centred, axis=-1, keepdims=True)
    ret_hidden = (
        (centred * lax.rsqrt(variance + epsilon)).reshape(row_count, head_count * DV) * ret_gain
    ).astype(jnp.bfloat16)
    att_queries, att_keys, att_values = rounded[3:]
    kv_heads = att_keys.shape[1] // HD
    groups = att_queries.shape[1] // HD // kv_heads
    earlier_keys, earlier_values = passed_along(
        (att_keys[row_count - WINDOW :], att_values[row_count - WINDOW :]), "sp", 1
    )
    extended_keys = jnp.concatenate([earlier_keys, att_keys], axis=0)
    extended_values = jnp.concatenate([earlier_values, att_values], axis=0)
    windows = row_count // WINDOW

    def banded(array):
        earlier = array[:row_count].reshape(windows, WINDOW, kv_heads, HD)
        current = array[WINDOW:].reshape(windows, WINDOW, kv_heads, HD)
        return jnp.concatenate([earlier, current], axis=1)

    key_band = banded(extended_keys)
    value_band = banded(extended_values)
    grouped_q = att_queries.reshape(windows, WINDOW, kv_heads, groups, HD)
    score_matrix = jnp.einsum(
        "nqhgd,nkhd->nhgqk", grouped_q, key_band, preferred_element_type=jnp.float32
    ) * HD ** (-0.5)
    query_index = WINDOW + jnp.arange(WINDOW)
    key_index = jnp.arange(2 * WINDOW)
    allowed = (key_index[None, :] <= query_index[:, None]) & (
        query_index[:, None] - key_index[None, :] < WINDOW
    )
    key_place = offset - WINDOW + jnp.arange(windows)[:, None] * WINDOW + key_index[None, :]
    visible = (allowed[None] & (key_place >= 0)[:, None, :])[:, None, None]
    expo = jnp.exp(jnp.where(visible, score_matrix, -1e30))
    summed = jnp.sum(expo, axis=-1, keepdims=True) + jnp.exp(sink_logits).reshape(
        1, kv_heads, groups, 1, 1
    )
    probs = (expo / summed).astype(jnp.bfloat16)
    attended = jnp.einsum(
        "nhgqk,nkhd->nqhgd", probs, value_band, preferred_element_type=jnp.float32
    )
    att_hidden = attended.astype(jnp.bfloat16).reshape(row_count, kv_heads * groups * HD)
    ret_width = ret_hidden.shape[1]
    joined = jnp.concatenate([ret_hidden, att_hidden], axis=1)[None]
    piece = lax.all_gather(joined, "fs", axis=0, tiled=True)
    product = jnp.einsum(
        "srh,hd->srd", piece[:, :, :ret_width], ret_out, preferred_element_type=jnp.float32
    )
    product = product + jnp.einsum(
        "srh,hd->srd", piece[:, :, ret_width:], att_out, preferred_element_type=jnp.float32
    )
    partial_rows = product.astype(jnp.bfloat16)
    regrouped = lax.all_to_all(partial_rows, "fs", split_axis=0, concat_axis=2, tiled=True)
    mixed = lax.psum_scatter(
        regrouped[0].astype(jnp.float32).astype(jnp.bfloat16), "tp", scatter_dimension=1, tiled=True
    )
    return mixed[None]


MESH = pl.DeviceIdType.MESH
F32 = jnp.float32
BF16 = jnp.bfloat16
GAIN_ROW = 0
DECAY_ROW = 1
SINK_ROW = 2
K_AT, V_AT, KV_AT, Q_AT, A_AT = 0, 256, 512, 640, 896


def dot(a, b):
    return jnp.dot(a, b, preferred_element_type=F32)


def dot_t(a, b):
    return lax.dot_general(a, b, (((1,), (1,)), ((), ())), preferred_element_type=F32)


def dot_l(a, b):
    return lax.dot_general(a, b, (((0,), (0,)), ((), ())), preferred_element_type=F32)


def fused(
    tok_in, ngain_in, rq, rk, rv, aq, ak, av, gain_in, decay_in, sink_in, start, ro, ao, cos_in, sin_in, out,
    ngain, gain_v, decay_v, sink_v, ak_v, av_v, cos, sin, start_v, start_b, insem,
    small, sm, traw, xn, akp, w, wo, s0, local_state, sbuf, states, kbuf, vbuf, qbuf, kvp, inner, hid, hin,
    total, ob, fade, since, until, wx,
    send, smsem, tsem, ownsem, zsem, ysem, psem, wosem, ssem, stsem, halosem, hsem, outsem, xsem,
):
    z, f, c = lax.axis_index("sp"), lax.axis_index("fs"), lax.axis_index("tp")
    y, x = f // 2, lax.rem(f, 2)
    zh, zb = z // 2, lax.rem(z, 2)
    peer = 1 - c
    fx, fy = 2 * y + 1 - x, 2 * (1 - y) + x
    zp, z2, z3 = z + 1 - 2 * zb, lax.rem(z + 2, 4), 3 - z
    head = 2 * zb + x
    rows, half = tok_in.shape
    depth = rq.shape[0]
    part = depth // 4
    mid = jnp.logical_or(z == 1, z == 2)
    near, far = jnp.where(mid, z3, z2), jnp.where(mid, z2, z3)
    order = (zp, near, far)
    first, second = zh == 0, zh == 1

    loads = [
        (ngain_in, ngain), (gain_in, gain_v), (decay_in, decay_v), (sink_in, sink_v), (ak, ak_v), (av, av_v),
        (cos_in.at[pl.ds(pl.multiple_of(zh * 2 * rows, 2 * rows), 2 * rows)], cos),
        (sin_in.at[pl.ds(pl.multiple_of(zh * 2 * rows, 2 * rows), 2 * rows)], sin),
        (start, start_v),
    ]
    inputs = [pltpu.make_async_copy(src, dst, insem.at[i]) for i, (src, dst) in enumerate(loads)]
    for copy in inputs:
        copy.start()

    barrier = pltpu.get_barrier_semaphore()
    greeted = [{"tp": peer}, {"fs": fy}]
    for t in range(2):
        core = jnp.int32(t)
        greeted += [{"sp": zs, "tp": core} for zs in order]
        greeted += [{"fs": fx, "tp": core}, {"sp": zp, "fs": fx, "tp": core}]
    for where in greeted:
        pl.semaphore_signal(barrier, inc=1, device_id=where, device_id_type=MESH)
    pl.semaphore_wait(barrier, len(greeted))

    sent = []
    slots = iter(range(send.shape[0]))

    def both(a, b):
        if a is None:
            return b
        return a if b is None else jnp.logical_and(a, b)

    def remote(cond, src, dst, rsem, **where):
        copy = pltpu.make_async_remote_copy(
            src_ref=src, dst_ref=dst, send_sem=send.at[next(slots)], recv_sem=rsem,
            device_id=where, device_id_type=MESH,
        )
        sent.append((cond, copy))
        if cond is None:
            copy.start()
        else:
            pl.when(cond)(copy.start)
        return copy

    def local(cond, src, dst, sem):
        copy = pltpu.make_async_copy(src, dst, sem)
        if cond is None:
            copy.start()
        else:
            pl.when(cond)(copy.start)

    def arrived(dst, sem):
        pltpu.make_async_copy(dst, dst, sem).wait()

    mine = traw.at[zb, c]
    local(c == x, tok_in, mine, tsem.at[zb, c])
    remote(c != x, tok_in, mine, tsem.at[zb, c], tp=peer)
    ahead = remote(None, tok_in, mine, tsem.at[zb, c], sp=zp, tp=x)
    remote(None, tok_in, mine, tsem.at[zb, c], fs=fx, tp=x)

    pieces = ((K_AT, DK), (V_AT, DV), (KV_AT, 128), (A_AT, DK), (Q_AT, DK))
    sources = (rk, rv, akp, aq, rq)
    whole = (4,)

    def rows_of(zs, ys, cs):
        return pl.ds(pl.multiple_of(zs * depth + ys * 2 * part + cs * part, part), part)

    def rows_whole(zs, cs):
        return pl.ds(pl.multiple_of(zs * depth + cs * 2 * part, 2 * part), 2 * part)

    def weight(p):
        a, (at, width) = sources[p], pieces[p]
        return a, pl.ds(0, width) if a is akp else pl.ds(pl.multiple_of(x * DK, DK), width), pl.ds(at, width)

    def send_weights(p, cond, to):
        a, cols, at = weight(p)
        for t in range(2):
            if p in whole:
                src = a.at[pl.ds(t * 2 * part, 2 * part), cols]
                dst = w.at[rows_whole(z, t), at]
            else:
                src = a.at[pl.ds(pl.multiple_of(y * 2 * part + t * part, part), part), cols]
                dst = w.at[rows_of(z, y, t), at]
            remote(cond, src, dst, zsem.at[p, z], sp=to, tp=jnp.int32(t))

    def keep_weights(p):
        a, cols, at = weight(p)
        dst = w.at[pl.ds(pl.multiple_of(z * depth, depth), depth), at]
        local(c == zb, a.at[:, cols], dst, ownsem.at[p])
        remote(c == zb, a.at[:, cols], dst, ownsem.at[p], tp=peer)

    to_a = jnp.where(zb == c, z2, zp)
    early = jnp.logical_and(zb != c, mid)
    late = jnp.logical_and(zb != c, jnp.logical_not(mid))
    for p in (0, 1, 3, 4):
        send_weights(p, early, z3)
    for p in (0, 1, 3, 4):
        keep_weights(p)

    out_rows, out_cols = ro.shape

    shares = ((0, 0, out_rows), (1, 0, out_rows // 2), (1, out_rows // 2, out_rows // 2))

    def out_block(share, ys, cs):
        kind, at, n = shares[share]
        rows_at = pl.ds(pl.multiple_of(cs * out_rows + at, n), n)
        return wo.at[kind, ys, rows_at], wosem.at[share, ys, cs]

    def send_out(share):
        kind, at, n = shares[share]
        a = (ro, ao)[kind].at[pl.ds(at, n)]
        block, sem = out_block(share, y, c)
        remote(None, a, block, sem, fs=fy)
        remote(None, a, block, sem, tp=peer)
        local(None, a, block, sem)

    def pass_out(share):
        block, sem = out_block(share, 1 - y, c)
        arrived(block, sem)
        remote(None, block, block, sem, tp=peer)

    def wait_out(kind):
        for share in ((0,), (1, 2))[kind]:
            for ys, cs in ((y, c), (y, peer), (1 - y, peer)):
                arrived(*out_block(share, ys, cs))

    extra_cols = pl.ds(out_cols // 2, out_cols // 2)

    def extra(kind, cs):
        return wx.at[kind, pl.ds(pl.multiple_of(cs * out_rows, out_rows), out_rows)], xsem.at[kind, cs]

    def send_extra(cond):
        for kind, a in ((0, ro), (1, ao)):
            dst, sem = extra(kind, c)
            remote(cond, a.at[:, extra_cols], dst, sem, fs=fx, tp=1 - x)

    send_out(0)
    send_out(1)

    for i in (1, 2, 3):
        inputs[i].wait()
    small[...] = jnp.zeros_like(small)
    small[pl.ds(GAIN_ROW, 1), :] = gain_v[...]
    for j in range(2):
        small[pl.ds(DECAY_ROW, 1), pl.ds(j * rows, rows)] = decay_v[pl.ds(j, 1), :]
    small[pl.ds(SINK_ROW, 1), pl.ds(0, sink_v.shape[1])] = sink_v[...]
    inputs[4].wait()
    inputs[5].wait()
    packed = [
        jnp.concatenate([ak_v[:, j * HD : (j + 1) * HD], av_v[:, j * HD : (j + 1) * HD]], axis=1) for j in range(2)
    ]
    akp[...] = jnp.where(x == 0, packed[0], packed[1])

    send_weights(2, early, z3)
    keep_weights(2)
    here = jnp.logical_and(zb == c, c == x)
    to_square = 2 * zh + c
    local(here, small, sm.at[zb], smsem.at[zb])
    remote(jnp.logical_not(here), small, sm.at[zb], smsem.at[zb], sp=to_square, tp=x)
    remote(None, small, sm.at[zb], smsem.at[zb], sp=to_square, fs=fx, tp=x)
    gives = jnp.logical_and(first, zb == c)
    inputs[8].wait()
    start_b[...] = start_v[...].astype(BF16)
    local(both(gives, c == x), start_b.at[x], s0, ssem)
    remote(both(gives, c != x), start_b.at[x], s0, ssem, tp=peer)

    ahead.wait_send()

    def send_rest(p):
        send_weights(p, None, to_a)
        send_weights(p, late, z3)

    for p in (2, 0, 1):
        send_rest(p)

    for t in range(2):
        block = traw.at[1 - zb, t]

        @pl.when(c == x)
        def _():
            arrived(block, tsem.at[1 - zb, t])

        remote(c == x, block, block, tsem.at[1 - zb, t], fs=fx)

    remote(gives, start_b.at[1 - x], s0, ssem, fs=fx, tp=x)

    def take(p):
        at, width = pieces[p]
        cols = pl.ds(at, width)
        for zs in order:
            block = w.at[rows_whole(zs, c) if p in whole else rows_of(zs, y, c), cols]
            arrived(block, zsem.at[p, zs])
            if p not in whole:
                remote(None, block, block, ysem.at[p, zs], fs=fy)
            remote(None, block, block, psem.at[p], tp=peer)

    def spread(p):
        at, width = pieces[p]
        cols = pl.ds(at, width)
        for zs in order:
            block = w.at[rows_of(zs, 1 - y, c), cols]
            arrived(block, ysem.at[p, zs])
            remote(None, block, block, psem.at[p], tp=peer)

    def complete(p):
        at, width = pieces[p]
        cols = pl.ds(at, width)
        arrived(w.at[pl.ds(0, depth), cols], ownsem.at[p])
        arrived(w.at[pl.ds(0, 6 * part), cols], psem.at[p])

    inputs[0].wait()

    def normalize(b):
        @pl.loop(0, rows // 32, unroll=2)
        def _(i):
            at = pl.ds(pl.multiple_of(i * 32, 32), 32)
            to = pl.ds(pl.multiple_of(b * rows + i * 32, 32), 32)
            h0, h1 = traw[b, 0, at, :].astype(F32), traw[b, 1, at, :].astype(F32)
            squares = jnp.sum(h0 * h0, axis=-1, keepdims=True) + jnp.sum(h1 * h1, axis=-1, keepdims=True)
            scale = lax.rsqrt(squares / (2 * half) + epsilon)
            xn[to, pl.ds(0, half)] = (h0 * scale * ngain[:, pl.ds(0, half)]).astype(BF16)
            xn[to, pl.ds(half, half)] = (h1 * scale * ngain[:, pl.ds(half, half)]).astype(BF16)

    def token_wait(b):
        for t in range(2):
            block, sem = traw.at[b, t], tsem.at[b, t]
            if b is other:
                pl.when(c != x)(functools.partial(arrived, block, sem))
            else:
                arrived(block, sem)

    own, other = zb, 1 - zb
    token_wait(own)
    normalize(own)
    pl.when(c == x)(functools.partial(normalize, other))
    send_extra(c == x)
    for b in range(2):
        arrived(sm.at[b], smsem.at[b])
    lane = lax.broadcasted_iota(jnp.int32, (rows, rows), 1)
    row = lax.broadcasted_iota(jnp.int32, (rows, rows), 0)

    def rates(b):
        return sm[b, pl.ds(DECAY_ROW, 1), pl.ds(pl.multiple_of(x * rows, rows), rows)]

    @pl.loop(0, 2)
    def _(b):
        at = pl.ds(pl.multiple_of(b * rows, rows), rows)
        l = rates(b)
        cum = jnp.sum(jnp.where(lane <= row, l, 0.0), axis=1, keepdims=True)
        cum_row = jnp.sum(jnp.where(lane == row, cum, 0.0), axis=0, keepdims=True)
        fade[b] = jnp.where(lane <= row, jnp.exp(jnp.where(lane <= row, cum - cum_row, 0.0)), 0.0)
        since[at, :] = jnp.exp(cum)
        until[at, :] = jnp.exp(jnp.sum(l, axis=1, keepdims=True) - cum)

    pass_out(0)
    take(2)
    take(0)
    send_rest(3)
    spread(2)
    take(1)
    send_rest(4)
    pass_out(1)
    spread(0)
    take(3)
    spread(1)
    send_out(2)
    token_wait(other)
    pl.when(c != x)(functools.partial(normalize, other))
    send_extra(c != x)
    inputs[6].wait()
    inputs[7].wait()
    complete(2)

    def block_at(b):
        return pl.ds(pl.multiple_of(b * rows, rows), rows)

    def tile(b, at, width):
        return dot(xn[block_at(b), :], w[:, pl.ds(at, width)])

    h = DK // 2

    def turn(a, b, factor):
        co, si = cos[block_at(b), :], sin[block_at(b), :]
        lo, hi = a[:, :h], a[:, h:]
        return jnp.concatenate([(lo * co - hi * si) * factor, (lo * si + hi * co) * factor], axis=1).astype(BF16)

    @pl.when(first)
    def _():
        kvp[pl.ds(0, WINDOW), :] = jnp.zeros((WINDOW, kvp.shape[1]), BF16)

    @pl.loop(0, 2, unroll=True)
    def _(b):
        to = pl.ds(pl.multiple_of(WINDOW + b * rows, WINDOW), rows)
        kvp[to, :] = tile(b, KV_AT, 128).astype(BF16)

    remote(first, kvp.at[pl.ds(2 * rows, WINDOW)], kvp.at[pl.ds(0, WINDOW)], halosem, sp=z2)
    complete(0)
    complete(1)
    @pl.loop(0, 2, unroll=True)
    def _(b):
        at = block_at(b)
        k = turn(tile(b, K_AT, DK).astype(BF16).astype(F32), b, DK ** (-0.5))
        kbuf[at, :] = k
        v = tile(b, V_AT, DV).astype(BF16)
        vbuf[at, :] = v
        kd = (k.astype(F32) * until[at, :]).astype(BF16)
        local_state[b] = dot_l(kd, v)

    def decay_of(b):
        return jnp.exp(jnp.sum(rates(b), axis=1, keepdims=True))

    @pl.when(first)
    def _():
        arrived(s0, ssem)
        states[0] = s0[...]
        after = s0[...].astype(F32) * decay_of(0) + local_state[0]
        states[1] = after.astype(BF16)
        sbuf[...] = (after * decay_of(1) + local_state[1]).astype(BF16)

    remote(first, sbuf, states.at[0], stsem, sp=z2)

    def hand_on(kind, b, away=None, part_at=None):
        at = pl.ds(0, rows) if part_at is None else pl.ds(part_at * (rows // 2), rows // 2)
        sem = hsem.at[2 if kind else part_at, head]
        src, dst = hid.at[kind, b, at], hin.at[kind, head, at]
        leaves, stays = (zb != b, zb == b) if away is None else (None, None)
        if away is not False:
            remote(leaves, src, dst, sem, sp=zp)
            remote(leaves, src, dst, sem, sp=zp, fs=fx)
        if away is not True:
            remote(stays, src, dst, sem, fs=fx)
            local(stays, src, dst, sem)

    lane2 = lax.broadcasted_iota(jnp.int32, (WINDOW, 2 * WINDOW), 1)
    row2 = lax.broadcasted_iota(jnp.int32, (WINDOW, 2 * WINDOW), 0)
    per = rows // WINDOW
    groups = DK // HD
    sink_row = sm[0, pl.ds(SINK_ROW, 1), pl.ds(0, 128)]
    sink_lane = lax.broadcasted_iota(jnp.int32, (1, 128), 1)
    sinks = [
        jnp.exp(jnp.sum(jnp.where(sink_lane == x * groups + i, sink_row, 0.0), axis=1, keepdims=True))
        for i in range(groups)
    ]

    def attention(b, away):
        aqs = tile(b, A_AT, DK).astype(BF16)
        seen = (lane2 <= row2 + WINDOW) & (lane2 > row2)
        scores, bands = [], []
        for i in range(per):
            n = b * per + i
            band = kvp[pl.ds(pl.multiple_of(n * WINDOW, WINDOW), 2 * WINDOW), :]
            bands.append(band[:, HD:])
            q = aqs[i * WINDOW : (i + 1) * WINDOW]
            stacked = jnp.concatenate([q[:, g * HD : (g + 1) * HD] for g in range(groups)], axis=0)
            scores.append(dot_t(stacked, band[:, :HD]))
        weights = []
        for i in range(per):
            visible = seen & (lane2 + (b * per + i) * WINDOW + zh * 2 * rows >= WINDOW)
            probs = []
            for g in range(groups):
                part_score = scores[i][g * WINDOW : (g + 1) * WINDOW] * HD ** (-0.5)
                e = jnp.exp(jnp.where(visible, part_score, -1e30))
                probs.append((e * (1.0 / (jnp.sum(e, axis=-1, keepdims=True) + sinks[g]))).astype(BF16))
            weights.append(jnp.concatenate(probs, axis=0))
        for i in range(per):
            res = dot(weights[i], bands[i])
            heads_out = [res[g * WINDOW : (g + 1) * WINDOW] for g in range(groups)]
            hid[1, b, pl.ds(i * WINDOW, WINDOW), :] = jnp.concatenate(heads_out, axis=1).astype(BF16)
        hand_on(1, b, away)

    spread(3)
    complete(3)
    pl.when(second)(functools.partial(arrived, kvp.at[pl.ds(0, WINDOW)], halosem))
    attention(own, False)
    attention(other, True)
    take(4)
    complete(4)

    @pl.loop(0, 2, unroll=True)
    def _(b):
        at = block_at(b)
        q = turn(tile(b, Q_AT, DK).astype(BF16).astype(F32), b, 1.0)
        qbuf[at, :] = (q.astype(F32) * since[at, :]).astype(BF16)
        scores = (dot_t(q, kbuf[at, :]) * fade[b]).astype(BF16)
        inner[at, :] = dot(scores, vbuf[at, :])

    @pl.when(second)
    def _():
        arrived(states.at[0], stsem)
        states[1] = (states[0].astype(F32) * decay_of(0) + local_state[0]).astype(BF16)

    gain_at = pl.ds(pl.multiple_of(x * DV, DV), DV)
    for b in (other, own):
        at = block_at(b)
        o = inner[at, :] + dot(qbuf[at, :], states[b])
        centred = o - jnp.mean(o, axis=-1, keepdims=True)
        var = jnp.mean(centred * centred, axis=-1, keepdims=True)
        hid[0, b] = (centred * lax.rsqrt(var + epsilon) * sm[0, pl.ds(GAIN_ROW, 1), gain_at]).astype(BF16)

    for part_at in range(2):
        hand_on(0, other, True, part_at)
        hand_on(0, own, False, part_at)

    pass_out(2)
    others = (2 * zb + 1 - x, 2 * (1 - zb) + x, 2 * (1 - zb) + 1 - x)
    home = c == x

    def mixed_tile(kind, at, t):
        cols = pl.ds(t % 2 * 256, 256)
        acc = None
        for n in range(4):
            term = dot(hin[kind, n, at, :], wo[kind, t // 2, pl.ds(n * DV, DV), cols])
            acc = term if acc is None else acc + term
        return acc

    def extra_tile(kind, at):
        acc = None
        for n in range(4):
            term = dot(hin[kind, n, at, :], wx[kind, pl.ds(n * DV, DV), :])
            acc = term if acc is None else acc + term
        return acc

    for n in (head,) + others:
        arrived(hin.at[1, n], hsem.at[2, n])
    wait_out(1)
    wait_out(0)
    for t in range(4):
        total[:, pl.ds(t * 256, 256)] = mixed_tile(1, pl.ds(0, rows), t)

    @pl.when(home)
    def _():
        for kind in range(2):
            for cs in range(2):
                arrived(*extra(kind, cs))
        total[:, pl.ds(half, 256)] = extra_tile(1, pl.ds(0, rows))

    def finish(part_at):
        at = pl.ds(part_at * (rows // 2), rows // 2)
        for t in range(4):
            ob[t, at, :] = (total[at, pl.ds(t * 256, 256)] + mixed_tile(0, at, t)).astype(BF16)
            src = ob.at[t, at]
            dst = out.at[at, pl.ds(pl.multiple_of(x * out_cols + t % 2 * 256, 256), 256)]
            local(both(home, c == t // 2), src, dst, outsem)
            remote(both(home, c != t // 2), src, dst, outsem, tp=peer)
            leaves = c != x if t % 2 == 0 else jnp.logical_and(c != x, y != t // 2)
            remote(leaves, src, dst, outsem, fs=fx, tp=jnp.int32(t // 2))

        @pl.when(home)
        def _():
            ob[4, at, :] = (total[at, pl.ds(half, 256)] + extra_tile(0, at)).astype(BF16)

        src = ob.at[4, at]
        dst = out.at[at, pl.ds(pl.multiple_of((1 - x) * out_cols + out_cols // 2, 256), 256)]
        local(both(home, c == y), src, dst, outsem)
        remote(both(home, c != y), src, dst, outsem, tp=peer)

    def wait_ret(part_at):
        at = pl.ds(part_at * (rows // 2), rows // 2)
        for n in (head,) + others:
            arrived(hin.at[0, n, at], hsem.at[part_at, n])

    wait_ret(0)
    finish(0)
    wait_ret(1)
    finish(1)

    arrived(out, outsem)
    for cond, copy in sent:
        if copy is ahead:
            continue
        if cond is None:
            copy.wait_send()
        else:
            pl.when(cond)(copy.wait_send)


def layer(mesh, *args):
    (tokens, norm_gain, ret_query, ret_key, ret_value, att_query, att_key, att_value,
     log_decay, start_state, ret_gain, sink_logits, ret_out, att_out) = args
    n_sp, n_fs, n_tp = mesh.shape["sp"], mesh.shape["fs"], mesh.shape["tp"]
    heads = ret_query.shape[1] // DK
    kv_heads = att_key.shape[1] // HD
    rows, half = tokens.shape[1:]
    depth = ret_query.shape[0]
    square = (
        n_tp == 2 and n_fs == 4 and n_sp == 4 and heads == 2 and kv_heads == 2
        and att_query.shape[1] == ret_query.shape[1] and rows == DK and tokens.shape[0] == 1
        and 2 * half == n_sp * depth and ret_out.shape == att_out.shape
        and ret_out.shape == (heads * DV, half // 2) and half == 4 * DK
    )
    if not square:
        return shards(*args)
    h = DK // 2
    length = n_sp * rows
    inverse = np.float32(1.0) / np.float32(10000.0) ** (np.arange(h, dtype=np.float32) / np.float32(h))
    angles = np.arange(length, dtype=np.float32)[:, None] * inverse[None, :]
    cos = jnp.asarray(np.cos(angles), F32)
    sin = jnp.asarray(np.sin(angles), F32)
    wide = heads * rows
    hbm = pl.BlockSpec(memory_space=pl.ANY)
    dma = pltpu.SemaphoreType.DMA
    v = pltpu.VMEM
    res = pl.pallas_call(
        fused,
        out_shape=jax.ShapeDtypeStruct((rows, half), BF16),
        in_specs=[hbm] * 16,
        out_specs=hbm,
        scratch_shapes=[
            v((1, norm_gain.shape[0]), F32),
            v((1, ret_gain.shape[0]), F32),
            v((heads, rows), F32),
            v((1, sink_logits.shape[0]), F32),
            v(att_key.shape, BF16),
            v(att_value.shape, BF16),
            v((2 * rows, h), F32),
            v((2 * rows, h), F32),
            v(start_state.shape[1:], F32),
            v(start_state.shape[1:], BF16),
            dma((9,)),
            v((8, wide), F32),
            v((2, 8, wide), F32),
            v((2, 2, rows, half), BF16),
            v((2 * rows, 2 * half), BF16),
            v((depth, 128), BF16),
            v((n_sp * depth, A_AT + DK), BF16),
            v((2, 2, 2 * ret_out.shape[0], ret_out.shape[1]), BF16),
            v((DK, DV), BF16),
            v((2, DK, DV), F32),
            v((DK, DV), BF16),
            v((2, DK, DV), BF16),
            v((2 * rows, DK), BF16),
            v((2 * rows, DV), BF16),
            v((2 * rows, DK), BF16),
            v((WINDOW + 2 * rows, 128), BF16),
            v((2 * rows, DV), F32),
            v((2, 2, rows, DV), BF16),
            v((2, 4, rows, DV), BF16),
            v((rows, half + 256), F32),
            v((5, rows, 256), BF16),
            v((2, rows, rows), F32),
            v((2 * rows, 1), F32),
            v((2 * rows, 1), F32),
            v((2, 2 * ret_out.shape[0], ret_out.shape[1] // 2), BF16),
            dma((160,)),
            dma((2,)),
            dma((2, 2)),
            dma((5,)),
            dma((5, n_sp)),
            dma((5, n_sp)),
            dma((5,)),
            dma((3, 2, 2)),
            dma,
            dma,
            dma,
            dma((3, 4)),
            dma,
            dma((2, 2)),
        ],
        compiler_params=pltpu.CompilerParams(
            collective_id=0, has_side_effects=True, vmem_limit_bytes=67043328
        ),
    )(
        tokens[0], norm_gain[None], ret_query, ret_key, ret_value, att_query, att_key, att_value,
        ret_gain[None], log_decay[0], sink_logits[None], start_state[0], ret_out, att_out, cos, sin,
    )
    return res[None]


def solution(mesh):
    placed = (
        P("fs", "sp", "tp"),
        P(),
        P("sp", "tp"),
        P("sp", "tp"),
        P("sp", "tp"),
        P("sp", "tp"),
        P("sp", "tp"),
        P("sp", "tp"),
        P("fs", "tp", "sp"),
        P("fs", "tp", None, None),
        P("tp"),
        P("tp"),
        P("tp", "fs"),
        P("tp", "fs"),
    )
    return jax.shard_map(
        functools.partial(layer, mesh), mesh=mesh, in_specs=placed, out_specs=P("fs", "sp", "tp"), check_vma=False
    )
```

```python
import functools

import jax
import jax.numpy as jnp
import numpy as np
from jax import lax
from jax.experimental import pallas as pl
from jax.experimental.pallas import tpu as pltpu
from jax.sharding import PartitionSpec as P

DK = 256
DV = 256
HD = 64
WINDOW = 128
BLOCK = 128


epsilon = 1e-06
exact_result = lax.Precision.HIGHEST


def carried_in(array, axis, combine, identity):
    peers, mine = (lax.axis_size(axis), lax.axis_index(axis))
    everything = jax.tree.map(
        lambda part, kind: lax.all_gather(part.astype(kind), axis),
        array,
        (jnp.bfloat16, jnp.bfloat16),
    )
    start = jax.tree.map(
        lambda part, zero: jnp.broadcast_to(jnp.asarray(zero, part.dtype), part.shape),
        array,
        identity,
    )

    def hop(k, before):
        reached = k < mine
        new = combine(
            before, jax.tree.map(lambda part, own: part[k].astype(own.dtype), everything, array)
        )
        return jax.tree.map(lambda a, b: jnp.where(reached, a, b), new, before)

    return lax.fori_loop(0, peers, hop, start)


def passed_along(block, axis, distance):
    devices = range(lax.axis_size(axis))
    route = [(i - distance, i) for i in devices if i - distance in devices]
    return lax.ppermute(block, axis, route)


def rotate(values, positions):
    half_dim = values.shape[-1] // 2
    inverse = 1.0 / 10000.0 ** (jnp.arange(half_dim, dtype=jnp.float32) / half_dim)
    angles = positions.astype(jnp.float32)[:, None] * inverse[None, :]
    cosine = jnp.cos(angles)[:, None, :]
    sine_table = jnp.sin(angles)[:, None, :]
    front_half = values[..., :half_dim]
    back_half = values[..., half_dim:]
    return jnp.concatenate(
        [
            front_half * cosine - back_half * sine_table,
            front_half * sine_table + back_half * cosine,
        ],
        axis=-1,
    )


def block_step(memory_state, inputs):
    queries, key_matrix_rows, value_matrix_rows, log_rates = inputs
    length_here = log_rates.shape[-1]
    causal = jnp.arange(length_here)[:, None] >= jnp.arange(length_here)[None, :]
    running_totals = jnp.cumsum(log_rates, axis=-1)
    relative = running_totals[:, :, None] - running_totals[:, None, :]
    weight = jnp.where(causal[None], jnp.exp(jnp.where(causal[None], relative, 0.0)), 0.0)
    score_matrix = (
        jnp.einsum("hqd,hkd->hqk", queries, key_matrix_rows, precision=exact_result) * weight
    )
    carried_state = jnp.einsum(
        "hqd,hdv->hqv",
        queries * jnp.exp(running_totals)[:, :, None],
        memory_state,
        precision=exact_result,
    )
    output_rows = (
        jnp.einsum("arf,afu->aru", score_matrix, value_matrix_rows, precision=exact_result)
        + carried_state
    )
    decay_factors = jnp.exp(running_totals[:, -1:] - running_totals)
    memory_state = memory_state * jnp.exp(running_totals[:, -1])[:, None, None] + jnp.einsum(
        "iwj,iwe->ije",
        key_matrix_rows * decay_factors[:, :, None],
        value_matrix_rows,
        precision=exact_result,
    )
    return (memory_state, output_rows)


def chain(earlier, later):
    return (earlier[0] * later[0], earlier[1] * later[0][:, None, None] + later[1])


def shards(
    tokens,
    norm_gain,
    ret_query,
    ret_key,
    ret_value,
    att_query,
    att_key,
    att_value,
    log_decay,
    start_state,
    ret_gain,
    sink_logits,
    ret_out,
    att_out,
):
    gathered = lax.all_gather(tokens[0], "tp", axis=1, tiled=True)
    row_count = gathered.shape[0]
    as_float = gathered.astype(jnp.float32)
    normed = (
        as_float
        * lax.rsqrt(jnp.mean(as_float * as_float, axis=-1, keepdims=True) + epsilon)
        * norm_gain
    ).astype(jnp.bfloat16)
    offset = lax.axis_index("sp") * row_count
    positions = offset + jnp.arange(row_count, dtype=jnp.int32)
    weights = (ret_query, ret_key, ret_value, att_query, att_key, att_value)
    pieces = (
        lax.all_gather(weights[0], "sp", axis=0, tiled=True),
        lax.all_gather(weights[1], "sp", axis=0, tiled=True),
        lax.all_gather(weights[2], "sp", axis=0, tiled=True),
        lax.all_gather(weights[3], "sp", axis=0, tiled=True),
        lax.all_gather(weights[4], "sp", axis=0, tiled=True),
        lax.all_gather(weights[5], "sp", axis=0, tiled=True),
    )
    projected = tuple(
        (jnp.dot(normed, piece, preferred_element_type=jnp.float32) for piece in pieces)
    )
    rounded = tuple((product_f.astype(jnp.bfloat16) for product_f in projected))
    projected = rounded[:3]
    head_count = projected[0].shape[1] // DK
    queries = rotate(projected[0].astype(jnp.float32).reshape(row_count, head_count, DK), positions)
    keys_rot = rotate(
        projected[1].astype(jnp.float32).reshape(row_count, head_count, DK), positions
    ) * DK ** (-0.5)
    values_f = projected[2].astype(jnp.float32).reshape(row_count, head_count, DV)
    log_rates = log_decay[0]
    count = row_count // BLOCK

    def blocked(array):
        return array.reshape(count, BLOCK, head_count, array.shape[-1]).transpose(0, 2, 1, 3)

    rates_blocked = log_rates.reshape(head_count, count, BLOCK).transpose(1, 0, 2)
    local_state, pieces = lax.scan(
        block_step,
        jnp.zeros((head_count, DK, DV), jnp.float32),
        (blocked(queries), blocked(keys_rot), blocked(values_f), rates_blocked),
    )
    local_out = pieces.transpose(0, 2, 1, 3).reshape(row_count, head_count, DV)
    running_totals = jnp.cumsum(log_rates, axis=-1)
    device_decay = jnp.exp(running_totals[:, -1])
    identity = (jnp.ones((head_count,), jnp.float32), jnp.zeros((head_count, DK, DV), jnp.float32))
    prior_decay, prior_state = carried_in((device_decay, local_state), "sp", chain, identity)
    incoming = prior_state + prior_decay[:, None, None] * start_state[0]
    retained = local_out + jnp.einsum(
        "thd,hdv->thv",
        queries * jnp.exp(running_totals).T[:, :, None],
        incoming,
        precision=exact_result,
    )
    centred = retained - jnp.mean(retained, axis=-1, keepdims=True)
    variance = jnp.mean(centred * centred, axis=-1, keepdims=True)
    ret_hidden = (
        (centred * lax.rsqrt(variance + epsilon)).reshape(row_count, head_count * DV) * ret_gain
    ).astype(jnp.bfloat16)
    att_queries, att_keys, att_values = rounded[3:]
    kv_heads = att_keys.shape[1] // HD
    groups = att_queries.shape[1] // HD // kv_heads
    earlier_keys, earlier_values = passed_along(
        (att_keys[row_count - WINDOW :], att_values[row_count - WINDOW :]), "sp", 1
    )
    extended_keys = jnp.concatenate([earlier_keys, att_keys], axis=0)
    extended_values = jnp.concatenate([earlier_values, att_values], axis=0)
    windows = row_count // WINDOW

    def banded(array):
        earlier = array[:row_count].reshape(windows, WINDOW, kv_heads, HD)
        current = array[WINDOW:].reshape(windows, WINDOW, kv_heads, HD)
        return jnp.concatenate([earlier, current], axis=1)

    key_band = banded(extended_keys)
    value_band = banded(extended_values)
    grouped_q = att_queries.reshape(windows, WINDOW, kv_heads, groups, HD)
    score_matrix = jnp.einsum(
        "nqhgd,nkhd->nhgqk", grouped_q, key_band, preferred_element_type=jnp.float32
    ) * HD ** (-0.5)
    query_index = WINDOW + jnp.arange(WINDOW)
    key_index = jnp.arange(2 * WINDOW)
    allowed = (key_index[None, :] <= query_index[:, None]) & (
        query_index[:, None] - key_index[None, :] < WINDOW
    )
    key_place = offset - WINDOW + jnp.arange(windows)[:, None] * WINDOW + key_index[None, :]
    visible = (allowed[None] & (key_place >= 0)[:, None, :])[:, None, None]
    expo = jnp.exp(jnp.where(visible, score_matrix, -1e30))
    summed = jnp.sum(expo, axis=-1, keepdims=True) + jnp.exp(sink_logits).reshape(
        1, kv_heads, groups, 1, 1
    )
    probs = (expo / summed).astype(jnp.bfloat16)
    attended = jnp.einsum(
        "nhgqk,nkhd->nqhgd", probs, value_band, preferred_element_type=jnp.float32
    )
    att_hidden = attended.astype(jnp.bfloat16).reshape(row_count, kv_heads * groups * HD)
    ret_width = ret_hidden.shape[1]
    joined = jnp.concatenate([ret_hidden, att_hidden], axis=1)[None]
    piece = lax.all_gather(joined, "fs", axis=0, tiled=True)
    product = jnp.einsum(
        "srh,hd->srd", piece[:, :, :ret_width], ret_out, preferred_element_type=jnp.float32
    )
    product = product + jnp.einsum(
        "srh,hd->srd", piece[:, :, ret_width:], att_out, preferred_element_type=jnp.float32
    )
    partial_rows = product.astype(jnp.bfloat16)
    regrouped = lax.all_to_all(partial_rows, "fs", split_axis=0, concat_axis=2, tiled=True)
    mixed = lax.psum_scatter(
        regrouped[0].astype(jnp.float32).astype(jnp.bfloat16), "tp", scatter_dimension=1, tiled=True
    )
    return mixed[None]


MESH = pl.DeviceIdType.MESH
F32 = jnp.float32
BF16 = jnp.bfloat16
GAIN_ROW = 0
DECAY_ROW = 1
SINK_ROW = 2
K_AT, V_AT, KV_AT, Q_AT, A_AT = 0, 256, 512, 640, 896


def dot(a, b):
    return jnp.dot(a, b, preferred_element_type=F32)


def dot_t(a, b):
    return lax.dot_general(a, b, (((1,), (1,)), ((), ())), preferred_element_type=F32)


def dot_l(a, b):
    return lax.dot_general(a, b, (((0,), (0,)), ((), ())), preferred_element_type=F32)


def fused(
    tok_in, ngain_in, rq, rk, rv, aq, ak, av, gain_in, decay_in, sink_in, start, ro, ao, cos_in, sin_in, out,
    ngain, gain_v, decay_v, sink_v, ak_v, av_v, cos, sin, start_v, start_b, insem,
    small, sm, traw, xn, akp, w, wo, s0, local_state, sbuf, states, kbuf, vbuf, qbuf, kvp, inner, hid, hin,
    total, ob, fade, since, until, wx,
    send, smsem, tsem, ownsem, zsem, ysem, psem, wosem, ssem, stsem, halosem, hsem, outsem, xsem,
):
    z, f, c = lax.axis_index("sp"), lax.axis_index("fs"), lax.axis_index("tp")
    y, x = f // 2, lax.rem(f, 2)
    zh, zb = z // 2, lax.rem(z, 2)
    peer = 1 - c
    fx, fy = 2 * y + 1 - x, 2 * (1 - y) + x
    zp, z2, z3 = z + 1 - 2 * zb, lax.rem(z + 2, 4), 3 - z
    head = 2 * zb + x
    rows, half = tok_in.shape
    depth = rq.shape[0]
    part = depth // 4
    mid = jnp.logical_or(z == 1, z == 2)
    near, far = jnp.where(mid, z3, z2), jnp.where(mid, z2, z3)
    order = (zp, near, far)
    first, second = zh == 0, zh == 1

    loads = [
        (ngain_in, ngain), (gain_in, gain_v), (decay_in, decay_v), (sink_in, sink_v), (ak, ak_v), (av, av_v),
        (cos_in.at[pl.ds(pl.multiple_of(zh * 2 * rows, 2 * rows), 2 * rows)], cos),
        (sin_in.at[pl.ds(pl.multiple_of(zh * 2 * rows, 2 * rows), 2 * rows)], sin),
        (start, start_v),
    ]
    inputs = [pltpu.make_async_copy(src, dst, insem.at[i]) for i, (src, dst) in enumerate(loads)]
    for copy in inputs:
        copy.start()

    barrier = pltpu.get_barrier_semaphore()
    greeted = [{"tp": peer}, {"fs": fy}]
    for t in range(2):
        core = jnp.int32(t)
        greeted += [{"sp": zs, "tp": core} for zs in order]
        greeted += [{"fs": fx, "tp": core}, {"sp": zp, "fs": fx, "tp": core}]
    for where in greeted:
        pl.semaphore_signal(barrier, inc=1, device_id=where, device_id_type=MESH)
    pl.semaphore_wait(barrier, len(greeted))

    sent = []
    slots = iter(range(send.shape[0]))

    def both(a, b):
        if a is None:
            return b
        return a if b is None else jnp.logical_and(a, b)

    def remote(cond, src, dst, rsem, **where):
        copy = pltpu.make_async_remote_copy(
            src_ref=src, dst_ref=dst, send_sem=send.at[next(slots)], recv_sem=rsem,
            device_id=where, device_id_type=MESH,
        )
        sent.append((cond, copy))
        if cond is None:
            copy.start()
        else:
            pl.when(cond)(copy.start)
        return copy

    def local(cond, src, dst, sem):
        copy = pltpu.make_async_copy(src, dst, sem)
        if cond is None:
            copy.start()
        else:
            pl.when(cond)(copy.start)

    def arrived(dst, sem):
        pltpu.make_async_copy(dst, dst, sem).wait()

    mine = traw.at[zb, c]
    local(c == x, tok_in, mine, tsem.at[zb, c])
    remote(c != x, tok_in, mine, tsem.at[zb, c], tp=peer)
    ahead = remote(None, tok_in, mine, tsem.at[zb, c], sp=zp, tp=x)
    remote(None, tok_in, mine, tsem.at[zb, c], fs=fx, tp=x)

    pieces = ((K_AT, DK), (V_AT, DV), (KV_AT, 128), (A_AT, DK), (Q_AT, DK))
    sources = (rk, rv, akp, aq, rq)
    whole = (4,)

    def rows_of(zs, ys, cs):
        return pl.ds(pl.multiple_of(zs * depth + ys * 2 * part + cs * part, part), part)

    def rows_whole(zs, cs):
        return pl.ds(pl.multiple_of(zs * depth + cs * 2 * part, 2 * part), 2 * part)

    def weight(p):
        a, (at, width) = sources[p], pieces[p]
        return a, pl.ds(0, width) if a is akp else pl.ds(pl.multiple_of(x * DK, DK), width), pl.ds(at, width)

    def send_weights(p, cond, to):
        a, cols, at = weight(p)
        for t in range(2):
            if p in whole:
                src = a.at[pl.ds(t * 2 * part, 2 * part), cols]
                dst = w.at[rows_whole(z, t), at]
            else:
                src = a.at[pl.ds(pl.multiple_of(y * 2 * part + t * part, part), part), cols]
                dst = w.at[rows_of(z, y, t), at]
            remote(cond, src, dst, zsem.at[p, z], sp=to, tp=jnp.int32(t))

    def keep_weights(p):
        a, cols, at = weight(p)
        dst = w.at[pl.ds(pl.multiple_of(z * depth, depth), depth), at]
        local(c == zb, a.at[:, cols], dst, ownsem.at[p])
        remote(c == zb, a.at[:, cols], dst, ownsem.at[p], tp=peer)

    to_a = jnp.where(zb == c, z2, zp)
    early = jnp.logical_and(zb != c, mid)
    late = jnp.logical_and(zb != c, jnp.logical_not(mid))
    for p in (0, 1, 3, 4):
        send_weights(p, early, z3)
    for p in (0, 1, 3, 4):
        keep_weights(p)

    out_rows, out_cols = ro.shape

    shares = ((0, 0, out_rows), (1, 0, out_rows // 2), (1, out_rows // 2, out_rows // 2))

    def out_block(share, ys, cs):
        kind, at, n = shares[share]
        rows_at = pl.ds(pl.multiple_of(cs * out_rows + at, n), n)
        return wo.at[kind, ys, rows_at], wosem.at[share, ys, cs]

    def send_out(share):
        kind, at, n = shares[share]
        a = (ro, ao)[kind].at[pl.ds(at, n)]
        block, sem = out_block(share, y, c)
        remote(None, a, block, sem, fs=fy)
        remote(None, a, block, sem, tp=peer)
        local(None, a, block, sem)

    def pass_out(share):
        block, sem = out_block(share, 1 - y, c)
        arrived(block, sem)
        remote(None, block, block, sem, tp=peer)

    def wait_out(kind):
        for share in ((0,), (1, 2))[kind]:
            for ys, cs in ((y, c), (y, peer), (1 - y, peer)):
                arrived(*out_block(share, ys, cs))

    extra_cols = pl.ds(out_cols // 2, out_cols // 2)

    def extra(kind, cs):
        return wx.at[kind, pl.ds(pl.multiple_of(cs * out_rows, out_rows), out_rows)], xsem.at[kind, cs]

    def send_extra(cond):
        for kind, a in ((0, ro), (1, ao)):
            dst, sem = extra(kind, c)
            remote(cond, a.at[:, extra_cols], dst, sem, fs=fx, tp=1 - x)

    send_out(0)
    send_out(1)

    for i in (1, 2, 3):
        inputs[i].wait()
    small[...] = jnp.zeros_like(small)
    small[pl.ds(GAIN_ROW, 1), :] = gain_v[...]
    for j in range(2):
        small[pl.ds(DECAY_ROW, 1), pl.ds(j * rows, rows)] = decay_v[pl.ds(j, 1), :]
    small[pl.ds(SINK_ROW, 1), pl.ds(0, sink_v.shape[1])] = sink_v[...]
    inputs[4].wait()
    inputs[5].wait()
    packed = [
        jnp.concatenate([ak_v[:, j * HD : (j + 1) * HD], av_v[:, j * HD : (j + 1) * HD]], axis=1) for j in range(2)
    ]
    akp[...] = jnp.where(x == 0, packed[0], packed[1])

    send_weights(2, early, z3)
    keep_weights(2)
    here = jnp.logical_and(zb == c, c == x)
    to_square = 2 * zh + c
    local(here, small, sm.at[zb], smsem.at[zb])
    remote(jnp.logical_not(here), small, sm.at[zb], smsem.at[zb], sp=to_square, tp=x)
    remote(None, small, sm.at[zb], smsem.at[zb], sp=to_square, fs=fx, tp=x)
    gives = jnp.logical_and(first, zb == c)
    inputs[8].wait()
    start_b[...] = start_v[...].astype(BF16)
    local(both(gives, c == x), start_b.at[x], s0, ssem)
    remote(both(gives, c != x), start_b.at[x], s0, ssem, tp=peer)

    ahead.wait_send()

    def send_rest(p):
        send_weights(p, None, to_a)
        send_weights(p, late, z3)

    for p in (2, 0, 1):
        send_rest(p)

    for t in range(2):
        block = traw.at[1 - zb, t]

        @pl.when(c == x)
        def _():
            arrived(block, tsem.at[1 - zb, t])

        remote(c == x, block, block, tsem.at[1 - zb, t], fs=fx)

    remote(gives, start_b.at[1 - x], s0, ssem, fs=fx, tp=x)

    def take(p):
        at, width = pieces[p]
        cols = pl.ds(at, width)
        for zs in order:
            block = w.at[rows_whole(zs, c) if p in whole else rows_of(zs, y, c), cols]
            arrived(block, zsem.at[p, zs])
            if p not in whole:
                remote(None, block, block, ysem.at[p, zs], fs=fy)
            remote(None, block, block, psem.at[p], tp=peer)

    def spread(p):
        at, width = pieces[p]
        cols = pl.ds(at, width)
        for zs in order:
            block = w.at[rows_of(zs, 1 - y, c), cols]
            arrived(block, ysem.at[p, zs])
            remote(None, block, block, psem.at[p], tp=peer)

    def complete(p):
        at, width = pieces[p]
        cols = pl.ds(at, width)
        arrived(w.at[pl.ds(0, depth), cols], ownsem.at[p])
        arrived(w.at[pl.ds(0, 6 * part), cols], psem.at[p])

    inputs[0].wait()

    def normalize(b):
        @pl.loop(0, rows // 32, unroll=2)
        def _(i):
            at = pl.ds(pl.multiple_of(i * 32, 32), 32)
            to = pl.ds(pl.multiple_of(b * rows + i * 32, 32), 32)
            h0, h1 = traw[b, 0, at, :].astype(F32), traw[b, 1, at, :].astype(F32)
            squares = jnp.sum(h0 * h0, axis=-1, keepdims=True) + jnp.sum(h1 * h1, axis=-1, keepdims=True)
            scale = lax.rsqrt(squares / (2 * half) + epsilon)
            xn[to, pl.ds(0, half)] = (h0 * scale * ngain[:, pl.ds(0, half)]).astype(BF16)
            xn[to, pl.ds(half, half)] = (h1 * scale * ngain[:, pl.ds(half, half)]).astype(BF16)

    def token_wait(b):
        for t in range(2):
            block, sem = traw.at[b, t], tsem.at[b, t]
            if b is other:
                pl.when(c != x)(functools.partial(arrived, block, sem))
            else:
                arrived(block, sem)

    own, other = zb, 1 - zb
    token_wait(own)
    normalize(own)
    pl.when(c == x)(functools.partial(normalize, other))
    send_extra(c == x)
    for b in range(2):
        arrived(sm.at[b], smsem.at[b])
    lane = lax.broadcasted_iota(jnp.int32, (rows, rows), 1)
    row = lax.broadcasted_iota(jnp.int32, (rows, rows), 0)

    def rates(b):
        return sm[b, pl.ds(DECAY_ROW, 1), pl.ds(pl.multiple_of(x * rows, rows), rows)]

    @pl.loop(0, 2)
    def _(b):
        at = pl.ds(pl.multiple_of(b * rows, rows), rows)
        l = rates(b)
        cum = jnp.sum(jnp.where(lane <= row, l, 0.0), axis=1, keepdims=True)
        cum_row = jnp.sum(jnp.where(lane == row, cum, 0.0), axis=0, keepdims=True)
        fade[b] = jnp.where(lane <= row, jnp.exp(jnp.where(lane <= row, cum - cum_row, 0.0)), 0.0)
        since[at, :] = jnp.exp(cum)
        until[at, :] = jnp.exp(jnp.sum(l, axis=1, keepdims=True) - cum)

    pass_out(0)
    take(2)
    take(0)
    send_rest(3)
    spread(2)
    take(1)
    send_rest(4)
    pass_out(1)
    spread(0)
    take(3)
    spread(1)
    send_out(2)
    token_wait(other)
    pl.when(c != x)(functools.partial(normalize, other))
    send_extra(c != x)
    inputs[6].wait()
    inputs[7].wait()
    complete(2)

    def block_at(b):
        return pl.ds(pl.multiple_of(b * rows, rows), rows)

    def tile(b, at, width):
        return dot(xn[block_at(b), :], w[:, pl.ds(at, width)])

    h = DK // 2

    def turn(a, b, factor):
        co, si = cos[block_at(b), :], sin[block_at(b), :]
        lo, hi = a[:, :h], a[:, h:]
        return jnp.concatenate([(lo * co - hi * si) * factor, (lo * si + hi * co) * factor], axis=1).astype(BF16)

    @pl.when(first)
    def _():
        kvp[pl.ds(0, WINDOW), :] = jnp.zeros((WINDOW, kvp.shape[1]), BF16)

    @pl.loop(0, 2, unroll=True)
    def _(b):
        to = pl.ds(pl.multiple_of(WINDOW + b * rows, WINDOW), rows)
        kvp[to, :] = tile(b, KV_AT, 128).astype(BF16)

    remote(first, kvp.at[pl.ds(2 * rows, WINDOW)], kvp.at[pl.ds(0, WINDOW)], halosem, sp=z2)
    complete(0)
    complete(1)
    @pl.loop(0, 2, unroll=True)
    def _(b):
        at = block_at(b)
        k = turn(tile(b, K_AT, DK).astype(BF16).astype(F32), b, DK ** (-0.5))
        kbuf[at, :] = k
        v = tile(b, V_AT, DV).astype(BF16)
        vbuf[at, :] = v
        kd = (k.astype(F32) * until[at, :]).astype(BF16)
        local_state[b] = dot_l(kd, v)

    def decay_of(b):
        return jnp.exp(jnp.sum(rates(b), axis=1, keepdims=True))

    @pl.when(first)
    def _():
        arrived(s0, ssem)
        states[0] = s0[...]
        after = s0[...].astype(F32) * decay_of(0) + local_state[0]
        states[1] = after.astype(BF16)
        sbuf[...] = (after * decay_of(1) + local_state[1]).astype(BF16)

    remote(first, sbuf, states.at[0], stsem, sp=z2)

    def hand_on(kind, b, away=None, part_at=None):
        at = pl.ds(0, rows) if part_at is None else pl.ds(part_at * (rows // 2), rows // 2)
        sem = hsem.at[2 if kind else part_at, head]
        src, dst = hid.at[kind, b, at], hin.at[kind, head, at]
        leaves, stays = (zb != b, zb == b) if away is None else (None, None)
        if away is not False:
            remote(leaves, src, dst, sem, sp=zp)
            remote(leaves, src, dst, sem, sp=zp, fs=fx)
        if away is not True:
            remote(stays, src, dst, sem, fs=fx)
            local(stays, src, dst, sem)

    lane2 = lax.broadcasted_iota(jnp.int32, (WINDOW, 2 * WINDOW), 1)
    row2 = lax.broadcasted_iota(jnp.int32, (WINDOW, 2 * WINDOW), 0)
    per = rows // WINDOW
    groups = DK // HD
    sink_row = sm[0, pl.ds(SINK_ROW, 1), pl.ds(0, 128)]
    sink_lane = lax.broadcasted_iota(jnp.int32, (1, 128), 1)
    sinks = [
        jnp.exp(jnp.sum(jnp.where(sink_lane == x * groups + i, sink_row, 0.0), axis=1, keepdims=True))
        for i in range(groups)
    ]

    def attention(b, away):
        aqs = tile(b, A_AT, DK).astype(BF16)
        seen = (lane2 <= row2 + WINDOW) & (lane2 > row2)
        scores, bands = [], []
        for i in range(per):
            n = b * per + i
            band = kvp[pl.ds(pl.multiple_of(n * WINDOW, WINDOW), 2 * WINDOW), :]
            bands.append(band[:, HD:])
            q = aqs[i * WINDOW : (i + 1) * WINDOW]
            stacked = jnp.concatenate([q[:, g * HD : (g + 1) * HD] for g in range(groups)], axis=0)
            scores.append(dot_t(stacked, band[:, :HD]))
        weights = []
        for i in range(per):
            visible = seen & (lane2 + (b * per + i) * WINDOW + zh * 2 * rows >= WINDOW)
            probs = []
            for g in range(groups):
                part_score = scores[i][g * WINDOW : (g + 1) * WINDOW] * HD ** (-0.5)
                e = jnp.exp(jnp.where(visible, part_score, -1e30))
                probs.append((e * (1.0 / (jnp.sum(e, axis=-1, keepdims=True) + sinks[g]))).astype(BF16))
            weights.append(jnp.concatenate(probs, axis=0))
        for i in range(per):
            res = dot(weights[i], bands[i])
            heads_out = [res[g * WINDOW : (g + 1) * WINDOW] for g in range(groups)]
            hid[1, b, pl.ds(i * WINDOW, WINDOW), :] = jnp.concatenate(heads_out, axis=1).astype(BF16)
        hand_on(1, b, away)

    spread(3)
    complete(3)
    pl.when(second)(functools.partial(arrived, kvp.at[pl.ds(0, WINDOW)], halosem))
    attention(own, False)
    attention(other, True)
    take(4)
    complete(4)

    @pl.loop(0, 2, unroll=True)
    def _(b):
        at = block_at(b)
        q = turn(tile(b, Q_AT, DK).astype(BF16).astype(F32), b, 1.0)
        qbuf[at, :] = (q.astype(F32) * since[at, :]).astype(BF16)
        scores = (dot_t(q, kbuf[at, :]) * fade[b]).astype(BF16)
        inner[at, :] = dot(scores, vbuf[at, :])

    @pl.when(second)
    def _():
        arrived(states.at[0], stsem)
        states[1] = (states[0].astype(F32) * decay_of(0) + local_state[0]).astype(BF16)

    gain_at = pl.ds(pl.multiple_of(x * DV, DV), DV)
    for b in (other, own):
        at = block_at(b)
        o = inner[at, :] + dot(qbuf[at, :], states[b])
        centred = o - jnp.mean(o, axis=-1, keepdims=True)
        var = jnp.mean(centred * centred, axis=-1, keepdims=True)
        hid[0, b] = (centred * lax.rsqrt(var + epsilon) * sm[0, pl.ds(GAIN_ROW, 1), gain_at]).astype(BF16)

    for part_at in range(2):
        hand_on(0, other, True, part_at)
        hand_on(0, own, False, part_at)

    pass_out(2)
    others = (2 * zb + 1 - x, 2 * (1 - zb) + x, 2 * (1 - zb) + 1 - x)
    home = c == x

    def mixed_tile(kind, at, t):
        cols = pl.ds(t % 2 * 256, 256)
        acc = None
        for n in range(4):
            term = dot(hin[kind, n, at, :], wo[kind, t // 2, pl.ds(n * DV, DV), cols])
            acc = term if acc is None else acc + term
        return acc

    def extra_tile(kind, at):
        acc = None
        for n in range(4):
            term = dot(hin[kind, n, at, :], wx[kind, pl.ds(n * DV, DV), :])
            acc = term if acc is None else acc + term
        return acc

    for n in (head,) + others:
        arrived(hin.at[1, n], hsem.at[2, n])
    wait_out(1)
    wait_out(0)
    for t in range(4):
        total[:, pl.ds(t * 256, 256)] = mixed_tile(1, pl.ds(0, rows), t)

    @pl.when(home)
    def _():
        for kind in range(2):
            for cs in range(2):
                arrived(*extra(kind, cs))
        total[:, pl.ds(half, 256)] = extra_tile(1, pl.ds(0, rows))

    def finish(part_at):
        at = pl.ds(part_at * (rows // 2), rows // 2)
        for t in range(4):
            needed = True if t % 2 == 0 else jnp.logical_or(home, y != t // 2)

            @pl.when(needed)
            def _():
                ob[t, at, :] = (total[at, pl.ds(t * 256, 256)] + mixed_tile(0, at, t)).astype(BF16)

            src = ob.at[t, at]
            dst = out.at[at, pl.ds(pl.multiple_of(x * out_cols + t % 2 * 256, 256), 256)]
            local(both(home, c == t // 2), src, dst, outsem)
            remote(both(home, c != t // 2), src, dst, outsem, tp=peer)
            leaves = c != x if t % 2 == 0 else jnp.logical_and(c != x, y != t // 2)
            remote(leaves, src, dst, outsem, fs=fx, tp=jnp.int32(t // 2))

        @pl.when(home)
        def _():
            ob[4, at, :] = (total[at, pl.ds(half, 256)] + extra_tile(0, at)).astype(BF16)

        src = ob.at[4, at]
        dst = out.at[at, pl.ds(pl.multiple_of((1 - x) * out_cols + out_cols // 2, 256), 256)]
        local(both(home, c == y), src, dst, outsem)
        remote(both(home, c != y), src, dst, outsem, tp=peer)

    def wait_ret(part_at):
        at = pl.ds(part_at * (rows // 2), rows // 2)
        for n in (head,) + others:
            arrived(hin.at[0, n, at], hsem.at[part_at, n])

    wait_ret(0)
    finish(0)
    wait_ret(1)
    finish(1)

    arrived(out, outsem)
    for cond, copy in sent:
        if copy is ahead:
            continue
        if cond is None:
            copy.wait_send()
        else:
            pl.when(cond)(copy.wait_send)


def layer(mesh, *args):
    (tokens, norm_gain, ret_query, ret_key, ret_value, att_query, att_key, att_value,
     log_decay, start_state, ret_gain, sink_logits, ret_out, att_out) = args
    n_sp, n_fs, n_tp = mesh.shape["sp"], mesh.shape["fs"], mesh.shape["tp"]
    heads = ret_query.shape[1] // DK
    kv_heads = att_key.shape[1] // HD
    rows, half = tokens.shape[1:]
    depth = ret_query.shape[0]
    square = (
        n_tp == 2 and n_fs == 4 and n_sp == 4 and heads == 2 and kv_heads == 2
        and att_query.shape[1] == ret_query.shape[1] and rows == DK and tokens.shape[0] == 1
        and 2 * half == n_sp * depth and ret_out.shape == att_out.shape
        and ret_out.shape == (heads * DV, half // 2) and half == 4 * DK
    )
    if not square:
        return shards(*args)
    h = DK // 2
    length = n_sp * rows
    inverse = np.float32(1.0) / np.float32(10000.0) ** (np.arange(h, dtype=np.float32) / np.float32(h))
    angles = np.arange(length, dtype=np.float32)[:, None] * inverse[None, :]
    cos = jnp.asarray(np.cos(angles), F32)
    sin = jnp.asarray(np.sin(angles), F32)
    wide = heads * rows
    hbm = pl.BlockSpec(memory_space=pl.ANY)
    dma = pltpu.SemaphoreType.DMA
    v = pltpu.VMEM
    res = pl.pallas_call(
        fused,
        out_shape=jax.ShapeDtypeStruct((rows, half), BF16),
        in_specs=[hbm] * 16,
        out_specs=hbm,
        scratch_shapes=[
            v((1, norm_gain.shape[0]), F32),
            v((1, ret_gain.shape[0]), F32),
            v((heads, rows), F32),
            v((1, sink_logits.shape[0]), F32),
            v(att_key.shape, BF16),
            v(att_value.shape, BF16),
            v((2 * rows, h), F32),
            v((2 * rows, h), F32),
            v(start_state.shape[1:], F32),
            v(start_state.shape[1:], BF16),
            dma((9,)),
            v((8, wide), F32),
            v((2, 8, wide), F32),
            v((2, 2, rows, half), BF16),
            v((2 * rows, 2 * half), BF16),
            v((depth, 128), BF16),
            v((n_sp * depth, A_AT + DK), BF16),
            v((2, 2, 2 * ret_out.shape[0], ret_out.shape[1]), BF16),
            v((DK, DV), BF16),
            v((2, DK, DV), F32),
            v((DK, DV), BF16),
            v((2, DK, DV), BF16),
            v((2 * rows, DK), BF16),
            v((2 * rows, DV), BF16),
            v((2 * rows, DK), BF16),
            v((WINDOW + 2 * rows, 128), BF16),
            v((2 * rows, DV), F32),
            v((2, 2, rows, DV), BF16),
            v((2, 4, rows, DV), BF16),
            v((rows, half + 256), F32),
            v((5, rows, 256), BF16),
            v((2, rows, rows), F32),
            v((2 * rows, 1), F32),
            v((2 * rows, 1), F32),
            v((2, 2 * ret_out.shape[0], ret_out.shape[1] // 2), BF16),
            dma((160,)),
            dma((2,)),
            dma((2, 2)),
            dma((5,)),
            dma((5, n_sp)),
            dma((5, n_sp)),
            dma((5,)),
            dma((3, 2, 2)),
            dma,
            dma,
            dma,
            dma((3, 4)),
            dma,
            dma((2, 2)),
        ],
        compiler_params=pltpu.CompilerParams(
            collective_id=0, has_side_effects=True, vmem_limit_bytes=67043328
        ),
    )(
        tokens[0], norm_gain[None], ret_query, ret_key, ret_value, att_query, att_key, att_value,
        ret_gain[None], log_decay[0], sink_logits[None], start_state[0], ret_out, att_out, cos, sin,
    )
    return res[None]


def solution(mesh):
    placed = (
        P("fs", "sp", "tp"),
        P(),
        P("sp", "tp"),
        P("sp", "tp"),
        P("sp", "tp"),
        P("sp", "tp"),
        P("sp", "tp"),
        P("sp", "tp"),
        P("fs", "tp", "sp"),
        P("fs", "tp", None, None),
        P("tp"),
        P("tp"),
        P("tp", "fs"),
        P("tp", "fs"),
    )
    return jax.shard_map(
        functools.partial(layer, mesh), mesh=mesh, in_specs=placed, out_specs=P("fs", "sp", "tp"), check_vma=False
    )
```
